256 devices in a mesh: sp: 64 (over z, x, core), tp: 4 (over y).
Axes of the slice: x: 4, y: 4, z: 8, core: 2. Of those that a mesh axis runs over, the one named last changes fastest.
Arguments:
- hidden_in: bfloat16 [4096, 2048], P(('sp', 'tp')), may hold values from -6 to 6
- pre_gain: float32 [2048], replicated, may hold values from 0.5 to 1.5
- w_query: bfloat16 [2048, 1024], P(None, 'tp'), may hold values from -0.4375 to 0.4375
- w_key: bfloat16 [2048, 1024], P(None, 'tp'), may hold values from -0.125 to 0.125
- w_value: bfloat16 [2048, 1024], P(None, 'tp'), may hold values from -0.125 to 0.125
- stick_offset: float32 [8], P('tp'), may hold values from -15.2 to -14.2
- w_glu_a: bfloat16 [2048, 1024], P(None, 'tp'), may hold values from -0.125 to 0.125
- w_glu_b: bfloat16 [2048, 1024], P(None, 'tp'), may hold values from -0.125 to 0.125
- w_gate_attn: bfloat16 [2048, 2048], P(None, 'tp'), may hold values from -0.125 to 0.125
- w_gate_conv: bfloat16 [2048, 2048], P(None, 'tp'), may hold values from -0.125 to 0.125
- conv_taps: float32 [31, 1024], P(None, 'tp'), may hold values from -1 to 1
- conv_bias: float32 [1024], P('tp'), may hold values from -0.6 to 0.6
- norm_gain: float32 [1024], P('tp'), may hold values from 0.5 to 1.5
- norm_shift: float32 [1024], P('tp'), may hold values from -0.6 to 0.6
- w_attn_out: bfloat16 [1024, 2048], P('tp'), may hold values from -0.4375 to 0.4375
- w_conv_out: bfloat16 [1024, 2048], P('tp'), may hold values from -0.1875 to 0.1875
- post_gain: float32 [2048], P('tp'), may hold values from 0.5 to 1.5
Outputs:
- mixed: bfloat16 [4096, 2048], P('sp', 'tp')
The draws below stay inside these ranges and needn't reach their ends.
All inputs are finite; a program needn't handle non-finite values.
Results may differ from the reference program's by a relative error of at most 0.015.
Values may be sent and summed in bfloat16 or wider, within the bound.
A program may use at most 64 MiB of HBM per device.

```python
import math
import jax
import jax.numpy as jnp
from jax import lax

D = 2048
HEADS = 8
HEAD_DIM = 128
CONV_CH = 1024
WIDTH = 31
TOK_DEV = 64
TOKENS = 4096
N_SP = 64


def block_scale(stream_key, dims, shards, least, top_value):
    gain = 1.0
    for position, blocks in shards:
        steps = jax.random.uniform(jax.random.fold_in(jax.random.fold_in(stream_key, 6), position), (blocks,), jnp.float32, least / len(shards), top_value / len(shards))
        gain = gain * jnp.repeat(jnp.exp(steps), dims[position] // blocks).reshape((-1,) + (1,) * (len(dims) - 1 - position))
    return gain


def centred(rng, extent, deviation, limit, shards=(), held_as=jnp.bfloat16):
    result = jax.random.normal(rng, extent, jnp.float32) * deviation
    if len(shards) > 0:
        result = block_scale(rng, extent, shards, -0.22, 0.18) * result
    return jnp.clip(result, min=-limit, max=limit).astype(held_as)


def setup_inputs(seed: int = 0) -> dict:
    key_of = jax.random.split(jax.random.key(seed), 18)
    return {
        "hidden_in": centred(key_of[0], (TOKENS, D), 1.0, 6.0, ((0, 256),)),
        "pre_gain": jnp.clip(1.0 + 0.1 * jax.random.normal(key_of[1], (D,), jnp.float32), 0.5, 1.5),
        "w_query": centred(key_of[2], (D, HEADS * HEAD_DIM), (D // 12) ** -0.5, 0.4375, ((1, 4),)),
        "w_key": centred(key_of[3], (D, HEADS * HEAD_DIM), D ** -0.5, 0.125, ((1, 4),)),
        "w_value": centred(key_of[4], (D, HEADS * HEAD_DIM), D ** -0.5, 0.125, ((1, 4),)),
        "stick_offset": jnp.clip(-15.2 + 1.0 * jax.random.uniform(key_of[5], (HEADS,), jnp.float32) ** block_scale(key_of[5], (HEADS,), ((0, 4),), -0.2, 0.2), -15.2, -14.2),
        "w_glu_a": centred(key_of[6], (D, CONV_CH), D ** -0.5, 0.125, ((1, 4),)),
        "w_glu_b": centred(key_of[7], (D, CONV_CH), D ** -0.5, 0.125, ((1, 4),)),
        "w_gate_attn": centred(key_of[8], (D, D), D ** -0.5, 0.125, ((1, 4),)),
        "w_gate_conv": centred(key_of[9], (D, D), D ** -0.5, 0.125, ((1, 4),)),
        "conv_taps": centred(key_of[10], (WIDTH, CONV_CH), WIDTH ** -0.5, 1.0, ((1, 4),), jnp.float32),
        "conv_bias": centred(key_of[11], (CONV_CH,), 0.1, 0.6, ((0, 4),), jnp.float32),
        "norm_gain": jnp.clip(1.0 + 0.1 * jax.random.normal(key_of[12], (CONV_CH,), jnp.float32), 0.5, 1.5),
        "norm_shift": centred(key_of[13], (CONV_CH,), 0.1, 0.6, ((0, 4),), jnp.float32),
        "w_attn_out": centred(key_of[14], (HEADS * HEAD_DIM, D), (HEADS * HEAD_DIM // 6) ** -0.5, 0.4375, ((0, 4),)),
        "w_conv_out": centred(key_of[15], (CONV_CH, D), CONV_CH ** -0.5, 0.1875, ((0, 4),)),
        "post_gain": jnp.clip(1.0 + 0.1 * jax.random.normal(key_of[16], (D,), jnp.float32), 0.5, 1.5),
    }


epsilon = 1e-06

def held_bf16(values):
    return lax.optimization_barrier(values.astype(jnp.bfloat16))

def reference(hidden_in, pre_gain, w_query, w_key, w_value, stick_offset, w_glu_a, w_glu_b, w_gate_attn, w_gate_conv, conv_taps, conv_bias, norm_gain, norm_shift, w_attn_out, w_conv_out, post_gain):
    values = hidden_in.astype(jnp.float32)
    inverse = lax.rsqrt(lax.optimization_barrier(jnp.mean(values * values, axis=1, keepdims=True)) + epsilon)
    normed = (values * inverse * pre_gain).astype(jnp.bfloat16)

    def project(weight):
        return held_bf16(jnp.dot(normed, weight, preferred_element_type=jnp.float32))
    queries = project(w_query).astype(jnp.float32).reshape(TOKENS, HEADS, HEAD_DIM)
    key_rows = project(w_key).astype(jnp.float32).reshape(TOKENS, HEADS, HEAD_DIM)
    value_rows = project(w_value).astype(jnp.float32).reshape(TOKENS, HEADS, HEAD_DIM)
    glu_left = project(w_glu_a).astype(jnp.float32)
    glu_right = project(w_glu_b).astype(jnp.float32)
    gate_attn = project(w_gate_attn).astype(jnp.float32)
    gate_conv = project(w_gate_conv).astype(jnp.float32)
    positions = jnp.arange(TOKENS, dtype=jnp.int32)

    def attend_block(block_start):
        query_block = lax.dynamic_slice_in_dim(queries, block_start, TOK_DEV, 0)
        scores = jnp.einsum('thd,shd->hts', query_block, key_rows, precision=lax.Precision.HIGHEST)
        scores = scores / math.sqrt(HEAD_DIM) + stick_offset[:, None, None]
        query_pos = block_start + jnp.arange(TOK_DEV, dtype=jnp.int32)
        causal = (positions[None, :] < query_pos[:, None])[None]
        log_rest = jnp.where(causal, jax.nn.log_sigmoid(-scores), 0.0)
        suffix = lax.cumsum(log_rest, axis=2, reverse=True) - log_rest
        weights = jnp.where(causal, jnp.exp(jax.nn.log_sigmoid(scores) + suffix), 0.0)
        return jnp.einsum('hts,shd->thd', weights, value_rows, precision=lax.Precision.HIGHEST)
    starts = jnp.arange(N_SP, dtype=jnp.int32) * TOK_DEV
    attended = lax.map(attend_block, starts).reshape(TOKENS, HEADS * HEAD_DIM).astype(jnp.bfloat16)
    attn_branch = held_bf16(jnp.dot(attended, w_attn_out, preferred_element_type=jnp.float32)).astype(jnp.float32)
    gated_in = held_bf16(glu_left * jax.nn.sigmoid(glu_right)).astype(jnp.float32)
    padded = jnp.pad(gated_in, ((WIDTH - 1, 0), (0, 0)))
    convolved = lax.conv_general_dilated(padded[None], conv_taps.reshape(WIDTH, 1, CONV_CH), (1,), 'VALID', dimension_numbers=('NWC', 'WIO', 'NWC'), feature_group_count=CONV_CH, precision=lax.Precision.HIGHEST)[0] + conv_bias
    mean_row = lax.optimization_barrier(jnp.mean(convolved, axis=1, keepdims=True))
    centered = convolved - mean_row
    spread = lax.optimization_barrier(jnp.mean(centered * centered, axis=1, keepdims=True))
    conv_normed = jax.nn.silu(centered * lax.rsqrt(spread + epsilon) * norm_gain + norm_shift).astype(jnp.bfloat16)
    conv_branch = held_bf16(jnp.dot(conv_normed, w_conv_out, preferred_element_type=jnp.float32)).astype(jnp.float32)
    merged = jax.nn.sigmoid(gate_attn) * attn_branch + jax.nn.sigmoid(gate_conv) * conv_branch
    squares = lax.optimization_barrier(jnp.mean(merged * merged, axis=1, keepdims=True))
    return (merged * lax.rsqrt(squares + epsilon) * post_gain).astype(jnp.bfloat16)
```

```python
import functools
import math

import jax
import jax.numpy as jnp
from jax import lax
from jax.experimental import pallas as pl
from jax.experimental.pallas import tpu as pltpu
from jax.sharding import Mesh
from jax.sharding import PartitionSpec as P

D = 2048
HD = 128
CONV_CH = 1024
WIDTH = 31
EPS = 1e-06
MESH = pl.DeviceIdType.MESH
F32 = jnp.float32
BF16 = jnp.bfloat16
NX = 4
NZ = 8
NY = 4
NCHIP = NX * NZ


def dot(a, b):
    return jnp.dot(a, b, preferred_element_type=F32)


def dot_nt(a, b):
    return lax.dot_general(a, b, (((1,), (1,)), ((), ())), preferred_element_type=F32)


def sigmoid(v):
    return jax.nn.sigmoid(v)


(C_K0, C_V0, C_K1, C_V1, C_Q0, C_Q1, C_A, C_B, C_GA, C_GC, C_CO, C_AO) = range(12)


def kernel(
    hidden, pre_gain, w_query, w_key, w_value, offset, w_a, w_b, w_ga, w_gc,
    taps, bias, ngain, nshift, w_ao, w_co, post_gain,
    out,
    hbuf, wkv_own, wkv_oth, wq, wa, wb, wga, wgc, wco, wo,
    kvbuf, kvst, qbuf, qst, obuf, tbuf, tri,
    gst, halo, gbuf, cst, crx, stx, srx, convb, gateb, att, abuf, ssx, ssr,
    lsem, h_s, h_r, p_s, p_r, kx_s, kz_s, k_r, halo_s, halo_r,
    w_s, w_r, st_s, st_r, c_s, c_r, a_s, a_r, ss_s, ss_r,
):
    z = lax.axis_index("z")
    x = lax.axis_index("x")
    c = lax.axis_index("c")
    y = lax.axis_index("y")
    chip = z * NX + x
    oc = 1 - c

    def dev(zz=z, xx=x, cc=c, yy=y):
        return (zz, xx, cc, yy)

    def ypeer(d):
        return lax.rem(y + d, NY)

    def xpeer(d):
        return lax.rem(x + d, NX)

    def zpeer(d):
        return lax.rem(z + d + NZ, NZ)

    def rc(src, dst, ss, rs, to):
        return pltpu.make_async_remote_copy(
            src_ref=src, dst_ref=dst, send_sem=ss, recv_sem=rs, device_id=to, device_id_type=MESH
        )

    sends = []

    def start(copy):
        copy.start()
        sends.append(copy)

    own_cols = pl.ds(pl.multiple_of(c * HD, HD), HD)
    oth_cols = pl.ds(pl.multiple_of(oc * HD, HD), HD)
    lo, hi = pl.ds(0, HD), pl.ds(HD, HD)
    ycols = pl.ds(pl.multiple_of(y * 512, 512), 512)
    yrows = pl.ds(pl.multiple_of(y * 256, 256), 256)
    local = {
        C_K1: (w_key.at[:, oth_cols], wkv_oth.at[:, lo]),
        C_V1: (w_value.at[:, oth_cols], wkv_oth.at[:, hi]),
        C_K0: (w_key.at[:, own_cols], wkv_own.at[:, lo]),
        C_V0: (w_value.at[:, own_cols], wkv_own.at[:, hi]),
        C_Q1: (w_query.at[:, oth_cols], wq.at[:, hi]),
        C_Q0: (w_query.at[:, own_cols], wq.at[:, lo]),
        C_A: (w_a, wa),
        C_B: (w_b, wb),
        C_GA: (w_ga, wga),
        C_GC: (w_gc, wgc),
        C_CO: (w_co, wco),
        C_AO: (w_ao.at[:, ycols], wo.at[yrows, :]),
    }
    local = {k: pltpu.make_async_copy(s, d, lsem.at[k]) for k, (s, d) in local.items()}
    for copy in local.values():
        copy.start()

    barrier = pltpu.get_barrier_semaphore()
    next_chip = lax.rem(chip + 1, NCHIP)
    prev_chip = lax.rem(chip + NCHIP - 1, NCHIP)
    pair_chip = c * next_chip + oc * prev_chip
    pz, px = pair_chip // NX, lax.rem(pair_chip, NX)
    greet = [dev(yy=ypeer(d)) for d in (1, 2, 3)]
    greet += [dev(cc=oc, yy=ypeer(d)) for d in (0, 1, 2, 3)]
    greet += [dev(xx=xpeer(d)) for d in (1, 2, 3)]
    greet += [dev(zz=zpeer(1)), dev(zz=zpeer(-1))]
    greet += [(pz, px, oc, y)]
    for peer in greet:
        pl.semaphore_signal(barrier, inc=1, device_id=peer, device_id_type=MESH)

    hv = hidden[...].astype(F32)
    inv = lax.rsqrt(jnp.mean(hv * hv, axis=1, keepdims=True) + EPS)
    my16 = pl.ds(pl.multiple_of(y * 16, 16), 16)
    hbuf[my16, :] = (hv * inv * pre_gain[...]).astype(BF16)

    r2 = lax.broadcasted_iota(jnp.int32, (HD, 2 * HD), 0)
    c2 = lax.broadcasted_iota(jnp.int32, (HD, 2 * HD), 1)
    tri[...] = jnp.where((r2 > c2) | (c2 >= HD), 1.0, 0.0).astype(BF16)

    pl.semaphore_wait(barrier, len(greet))

    for d in (1, 3, 2):
        start(rc(hbuf.at[my16, :], hbuf.at[my16, :], h_s.at[d], h_r.at[y], dev(yy=ypeer(d))))
    for d in (1, 3, 2):
        yy = ypeer(d)
        rows = pl.ds(pl.multiple_of(yy * 16, 16), 16)
        rc(hbuf.at[rows, :], hbuf.at[rows, :], h_s.at[d], h_r.at[yy], dev(yy=yy)).wait_recv()

    my64 = pl.ds(pl.multiple_of(c * 64, 64), 64)
    oth64 = pl.ds(pl.multiple_of(oc * 64, 64), 64)
    partner = dev(cc=oc)
    local[C_K1].wait()
    local[C_V1].wait()
    kvst[...] = dot(hbuf[...], wkv_oth[...]).astype(BF16)
    start(rc(kvst, kvbuf.at[chip, my64, :], p_s.at[0], p_r.at[0], partner))
    local[C_K0].wait()
    local[C_V0].wait()
    kvbuf[chip, my64, :] = dot(hbuf[...], wkv_own[...]).astype(BF16)
    rc(kvst, kvbuf.at[chip, oth64, :], p_s.at[0], p_r.at[0], partner).wait_recv()

    def chunk_copy(idx, ss, to):
        return rc(kvbuf.at[idx], kvbuf.at[idx], ss, k_r.at[idx], to)

    for d in (1, 3, 2):
        start(chunk_copy(chip, kx_s.at[d], dev(xx=xpeer(d))))

    def z_send(idx, k, dx, up):
        to = dev(zz=zpeer(1)) if up else dev(zz=zpeer(-1))
        start(chunk_copy(idx, kz_s.at[(k * 4 + dx) * 2 + int(up)], to))

    for up in (True, False):
        z_send(chip, 0, 0, up)

    local[C_Q0].wait()
    local[C_Q1].wait()
    qv = dot(hbuf[...], wq[...]).astype(BF16)
    qst[...] = qv[:, HD:]
    start(rc(qst, qbuf.at[my64, :], p_s.at[1], p_r.at[1], partner))
    qbuf[my64, :] = qv[:, :HD]

    def wait_chunk(idx):
        rc(kvbuf.at[idx], kvbuf.at[idx], kx_s.at[0], k_r.at[idx], partner).wait_recv()

    for dx in (1, 3, 2):
        idx = z * NX + xpeer(dx)
        wait_chunk(idx)
        for up in (True, False):
            z_send(idx, 0, dx, up)

    for d in (1, 3, 2):
        yy = ypeer(d)
        cols = pl.ds(pl.multiple_of(yy * 512, 512), 512)
        start(rc(w_ao.at[:, cols], wo.at[yrows, :], w_s.at[d], w_r.at[y], dev(yy=yy)))

    local[C_A].wait()
    local[C_B].wait()
    left = dot(hbuf[...], wa[...]).astype(BF16).astype(F32)
    right = dot(hbuf[...], wb[...]).astype(BF16).astype(F32)
    gated = (left * sigmoid(right)).astype(BF16)
    gst[...] = gated[32:, :]
    gbuf[32:, :] = gated.astype(F32)
    halo_to = ((next_chip // NX) * c + z * oc, lax.rem(next_chip, NX) * c + x * oc, oc, y)
    start(rc(gst, halo, halo_s, halo_r, halo_to))

    depth_up = (4, 4, 3, 3)
    depth_down = (3, 3, 4, 4)

    def forward(k):
        for dx in (0, 1, 3, 2):
            for up in (True, False):
                depth = (depth_up if up else depth_down)[dx]
                if k > depth:
                    continue
                idx = (zpeer(-k) if up else zpeer(k)) * NX + xpeer(dx)
                wait_chunk(idx)
                if k < depth:
                    z_send(idx, k, dx, up)

    off = offset[c]
    scale = 1.0 / math.sqrt(HD)

    def block(idx):
        kb = kvbuf[idx, :, 0:HD]
        vb = kvbuf[idx, :, HD:]
        s = dot_nt(qbuf[...], kb) * scale + off
        u = jnp.exp(-jnp.abs(s))
        one = 1.0 + u
        tail = jnp.log(one) + (u - (one - 1.0))
        soft = jnp.maximum(s, 0.0) + tail
        rows = lax.broadcasted_iota(jnp.int32, (HD, HD), 0) + chip * HD
        cols = lax.broadcasted_iota(jnp.int32, (HD, HD), 1) + idx * HD
        causal = cols < rows
        logit = s - soft
        soft = jnp.where(causal, soft, 0.0)
        top = soft.astype(BF16)
        rest = (soft - top.astype(F32)).astype(BF16)
        sums = dot(top, tri[...]) + dot(rest, tri[...])
        stick = jnp.where(causal, jnp.exp(logit - sums[:, :HD]), 0.0)
        obuf[idx] = dot(stick.astype(BF16), vb)
        tbuf[idx] = sums[:, HD:]

    def row_blocks(zz):
        @pl.when(zz <= z)
        def _():
            def body(xx, carry):
                idx = zz * NX + xx

                @pl.when(idx <= chip)
                def _():
                    block(idx)

                return carry

            lax.fori_loop(0, NX, body, 0)

    forward(1)
    local[C_GA].wait()
    local[C_GC].wait()
    gateb[0] = sigmoid(dot(hbuf[...], wga[...]).astype(BF16).astype(F32))
    gateb[1] = sigmoid(dot(hbuf[...], wgc[...]).astype(BF16).astype(F32))

    rc(qst, qbuf.at[oth64, :], p_s.at[1], p_r.at[1], partner).wait_recv()
    row_blocks(z)
    row_blocks(zpeer(-1))

    rc(gst, halo, halo_s, halo_r, halo_to).wait_recv()
    first = (chip * 2 + c) == 0
    gbuf[0:32, :] = jnp.where(first, 0.0, halo[...].astype(F32))
    conv = jnp.broadcast_to(bias[...], (64, 256))
    for i in range(WIDTH):
        conv = conv + taps[i : i + 1, :] * gbuf[2 + i : 66 + i, :]
    local_mean = jnp.mean(conv, axis=1, keepdims=True)
    dev_local = conv - local_mean
    local_m2 = jnp.sum(dev_local * dev_local, axis=1, keepdims=True)
    lane = lax.broadcasted_iota(jnp.int32, (64, HD), 1)
    stx[...] = jnp.where(lane < 64, local_mean, local_m2)
    for d in (1, 3, 2):
        start(rc(stx, srx.at[y], st_s.at[d], st_r.at[y], dev(yy=ypeer(d))))
    convb[...] = conv

    forward(2)
    row_blocks(zpeer(-2))

    srx[y] = stx[...]
    for d in (1, 3, 2):
        yy = ypeer(d)
        rc(stx, srx.at[yy], st_s.at[d], st_r.at[yy], dev(yy=yy)).wait_recv()
    stats = [srx[i] for i in range(NY)]
    means = [t[:, 0:1] for t in stats]
    mean = (means[0] + means[1] + means[2] + means[3]) * 0.25
    m2 = stats[0][:, 64:65] + stats[1][:, 64:65] + stats[2][:, 64:65] + stats[3][:, 64:65]
    for t in means:
        m2 = m2 + 256.0 * (t - mean) * (t - mean)
    cn = (convb[...] - mean) * lax.rsqrt(m2 / CONV_CH + EPS) * ngain[...] + nshift[...]
    cn = (cn * sigmoid(cn)).astype(BF16)
    local[C_CO].wait()
    for i in range(NY):
        cst[i] = dot(cn, wco[:, i * 512 : (i + 1) * 512]).astype(BF16)
    for d in (1, 3, 2):
        yy = ypeer(d)
        start(rc(cst.at[yy], crx.at[y], c_s.at[d], c_r.at[y], dev(yy=yy)))

    forward(3)
    row_blocks(zpeer(-3))
    row_blocks(zpeer(1))

    csum = cst[y].astype(F32)
    for d in (1, 3, 2):
        yy = ypeer(d)
        rc(cst.at[yy], crx.at[yy], c_s.at[d], c_r.at[yy], dev(yy=yy)).wait_recv()
        csum = csum + crx[yy].astype(F32)
    gateb[1] = gateb[1] * csum.astype(BF16).astype(F32)

    forward(4)
    row_blocks(zpeer(2))
    row_blocks(zpeer(3))
    row_blocks(zpeer(4))

    def combine(j, state):
        acc, carry = state
        idx = chip - j
        return (acc + obuf[idx] * jnp.exp(-carry), carry + tbuf[idx])

    zero = jnp.zeros((HD, HD), F32)
    acc, _ = lax.fori_loop(0, chip + 1, combine, (zero, zero))
    att[...] = acc.astype(BF16)

    head = pl.ds(pl.multiple_of((y * 2 + c) * HD, HD), HD)
    n = 0
    for d in (0, 1, 3, 2):
        for cc, rows in ((c, my64), (oc, oth64)):
            if d == 0 and cc is c:
                continue
            start(rc(att.at[rows, :], abuf.at[:, head], a_s.at[n], a_r.at[y * 2 + c], dev(cc=cc, yy=ypeer(d))))
            n += 1
    abuf[:, head] = att[my64, :]
    local[C_AO].wait()
    for d in (1, 3, 2):
        yy = ypeer(d)
        rows = pl.ds(pl.multiple_of(yy * 256, 256), 256)
        rc(w_ao.at[:, ycols], wo.at[rows, :], w_s.at[d], w_r.at[yy], dev(yy=yy)).wait_recv()
    for d in (0, 1, 3, 2):
        for cc in (c, oc):
            if d == 0 and cc is c:
                continue
            yy = ypeer(d)
            h = yy * 2 + cc
            cols = pl.ds(pl.multiple_of(h * HD, HD), HD)
            rc(att.at[my64, :], abuf.at[:, cols], a_s.at[0], a_r.at[h], dev(cc=oc, yy=yy)).wait_recv()
    branch = dot(abuf[...], wo[...]).astype(BF16).astype(F32)
    merged = gateb[0] * branch + gateb[1]
    sq = merged * merged
    part = sq[:, 0:128] + sq[:, 128:256] + sq[:, 256:384] + sq[:, 384:512]
    part = jnp.concatenate([part, jnp.zeros((64, HD), F32)], axis=0).T
    ssx[...] = jnp.sum(part.reshape(16, 8, HD), axis=0)
    for d in (1, 3, 2):
        start(rc(ssx, ssr.at[y], ss_s.at[d], ss_r.at[y], dev(yy=ypeer(d))))
    total = ssx[...]
    for d in (1, 3, 2):
        yy = ypeer(d)
        rc(ssx, ssr.at[yy], ss_s.at[d], ss_r.at[yy], dev(yy=yy)).wait_recv()
        total = total + ssr[yy]
    total = jnp.broadcast_to(jnp.sum(total, axis=0, keepdims=True), (HD, HD)).T[:64, 0:1]
    out[...] = (merged * lax.rsqrt(total / D + EPS) * post_gain[...]).astype(BF16)

    for copy in sends:
        copy.wait_send()


def on_device(
    hidden_in, pre_gain, w_query, w_key, w_value, stick_offset, w_glu_a, w_glu_b, w_gate_attn,
    w_gate_conv, conv_taps, conv_bias, norm_gain, norm_shift, w_attn_out, w_conv_out, post_gain,
):
    vm = pl.BlockSpec(memory_space=pltpu.VMEM)
    hb = pl.BlockSpec(memory_space=pl.ANY)
    sm = pl.BlockSpec(memory_space=pltpu.SMEM)
    dma = pltpu.SemaphoreType.DMA
    return pl.pallas_call(
        kernel,
        out_shape=jax.ShapeDtypeStruct((64, 512), BF16),
        in_specs=[vm, vm, hb, hb, hb, sm, hb, hb, hb, hb, vm, vm, vm, vm, hb, hb, vm],
        out_specs=vm,
        scratch_shapes=[
            pltpu.VMEM((64, D), BF16),
            pltpu.VMEM((D, 256), BF16),
            pltpu.VMEM((D, 256), BF16),
            pltpu.VMEM((D, 256), BF16),
            pltpu.VMEM((D, 256), BF16),
            pltpu.VMEM((D, 256), BF16),
            pltpu.VMEM((D, 512), BF16),
            pltpu.VMEM((D, 512), BF16),
            pltpu.VMEM((256, D), BF16),
            pltpu.VMEM((1024, 512), BF16),
            pltpu.VMEM((NCHIP, 128, 256), BF16),
            pltpu.VMEM((64, 256), BF16),
            pltpu.VMEM((128, 128), BF16),
            pltpu.VMEM((64, 128), BF16),
            pltpu.VMEM((NCHIP, 128, 128), F32),
            pltpu.VMEM((NCHIP, 128, 128), F32),
            pltpu.VMEM((128, 256), BF16),
            pltpu.VMEM((32, 256), BF16),
            pltpu.VMEM((32, 256), BF16),
            pltpu.VMEM((96, 256), F32),
            pltpu.VMEM((NY, 64, 512), BF16),
            pltpu.VMEM((NY, 64, 512), BF16),
            pltpu.VMEM((64, 128), F32),
            pltpu.VMEM((NY, 64, 128), F32),
            pltpu.VMEM((64, 256), F32),
            pltpu.VMEM((2, 64, 512), F32),
            pltpu.VMEM((128, 128), BF16),
            pltpu.VMEM((64, 1024), BF16),
            pltpu.VMEM((8, 128), F32),
            pltpu.VMEM((NY, 8, 128), F32),
            dma((12,)),
            dma((4,)), dma((4,)),
            dma((2,)), dma((2,)),
            dma((4,)), dma((40,)), dma((NCHIP,)),
            dma, dma,
            dma((4,)), dma((4,)),
            dma((4,)), dma((4,)),
            dma((4,)), dma((4,)),
            dma((7,)), dma((8,)),
            dma((4,)), dma((4,)),
        ],
        compiler_params=pltpu.CompilerParams(
            collective_id=0, has_side_effects=True, vmem_limit_bytes=56 * 1024 * 1024
        ),
    )(
        hidden_in, pre_gain.reshape(1, -1), w_query, w_key, w_value, stick_offset, w_glu_a,
        w_glu_b, w_gate_attn, w_gate_conv, conv_taps, conv_bias.reshape(1, -1),
        norm_gain.reshape(1, -1), norm_shift.reshape(1, -1), w_attn_out, w_conv_out,
        post_gain.reshape(1, -1),
    )


def solution(mesh):
    torus = Mesh(mesh.devices.reshape(NZ, NX, 2, NY), ("z", "x", "c", "y"))
    every = ("z", "x", "c", "y")
    cols = P(None, "y")
    return jax.shard_map(
        on_device,
        mesh=torus,
        in_specs=(
            P(every, None), P(), cols, cols, cols, P("y"), cols, cols, cols, cols, cols,
            P("y"), P("y"), P("y"), P("y", None), P("y", None), P("y"),
        ),
        out_specs=P(("z", "x", "c"), "y"),
        check_vma=False,
    )
```

```python
import functools
import math

import jax
import jax.numpy as jnp
from jax import lax
from jax.experimental import pallas as pl
from jax.experimental.pallas import tpu as pltpu
from jax.sharding import Mesh
from jax.sharding import PartitionSpec as P

D = 2048
HD = 128
CONV_CH = 1024
WIDTH = 31
EPS = 1e-06
MESH = pl.DeviceIdType.MESH
F32 = jnp.float32
BF16 = jnp.bfloat16
NX = 4
NZ = 8
NY = 4
NCHIP = NX * NZ


ORDER0 = (
    (0, 0), (-1, 0), (0, 1), (0, 3), (1, 0), (0, 2), (-2, 0), (1, 1),
    (-1, 1), (1, 3), (-1, 3), (2, 0), (-1, 2), (1, 2), (-3, 0), (2, 1),
    (-2, 1), (2, 3), (3, 0), (-2, 3), (2, 2), (-2, 2), (3, 1), (-4, 0),
    (3, 3), (-3, 1), (-3, 3), (3, 2), (-3, 2), (4, 3), (-4, 1), (4, 2),
)
ORDER1 = (
    (0, 0), (-1, 0), (0, 1), (0, 3), (1, 0), (-1, 1), (-1, 3), (-2, 0),
    (2, 0), (0, 2), (1, 1), (1, 3), (-1, 2), (-2, 3), (-2, 1), (-3, 0),
    (3, 0), (2, 3), (2, 1), (1, 2), (-2, 2), (-3, 1), (-3, 3), (-4, 0),
    (3, 1), (3, 3), (2, 2), (-3, 2), (-4, 3), (-4, 1), (3, 2), (-4, 2),
)
UP0, DOWN0 = (4, 4, 3, 3), (3, 3, 4, 4)
UP1, DOWN1 = 4, 3


def hops(core, dz, dx):
    if core == 0:
        if dz == 0:
            return [("z", 1), ("z", -1)] + ([("x", 1), ("x", 3), ("x", 2)] if dx == 0 else [])
        if dz < 0:
            return [("z", 1)] if -dz < UP0[dx] else []
        return [("z", -1)] if dz < DOWN0[dx] else []
    if dx == 0:
        along = [("z", 1)] * (-UP1 < dz <= 0) + [("z", -1)] * (0 <= dz < DOWN1)
        return along + [("x", 1), ("x", 3)]
    if dx == 3:
        return [("x", 1)] if dz % 2 == 0 else []
    return [("x", 3)] if dx == 1 and dz % 2 == 1 else []


SENDS = [sum(len(hops(core, *t)) for t in order) for core, order in ((0, ORDER0), (1, ORDER1))]


def dot(a, b):
    return jnp.dot(a, b, preferred_element_type=F32)


def dot_nt(a, b):
    return lax.dot_general(a, b, (((1,), (1,)), ((), ())), preferred_element_type=F32)


def sigmoid(v):
    return jax.nn.sigmoid(v)


(C_K0, C_V0, C_K1, C_V1, C_Q0, C_Q1, C_A, C_B, C_GA, C_GC, C_CO, C_AO) = range(12)


def kernel(
    hidden, pre_gain, w_query, w_key, w_value, offset, w_a, w_b, w_ga, w_gc,
    taps, bias, ngain, nshift, w_ao, w_co, post_gain,
    out,
    hbuf, wkv_own, wkv_oth, wq, wa, wb, wga, wgc, wco, wo,
    kvbuf, kvst, qbuf, qst, obuf, tbuf, tri,
    gst, halo, gbuf, cst, crx, stx, srx, convb, gateb, att, abuf, ssx, ssr,
    lsem, h_s, h_r, p_s, p_r, k_s, k_r, halo_s, halo_r,
    w_s, w_r, st_s, st_r, c_s, c_r, a_s, a_r, ss_s, ss_r,
):
    z = lax.axis_index("z")
    x = lax.axis_index("x")
    c = lax.axis_index("c")
    y = lax.axis_index("y")
    chip = z * NX + x
    oc = 1 - c

    def dev(zz=z, xx=x, cc=c, yy=y):
        return (zz, xx, cc, yy)

    def ypeer(d):
        return lax.rem(y + d, NY)

    def xpeer(d):
        return lax.rem(x + d, NX)

    def zpeer(d):
        return lax.rem(z + d + NZ, NZ)

    def rc(src, dst, ss, rs, to):
        return pltpu.make_async_remote_copy(
            src_ref=src, dst_ref=dst, send_sem=ss, recv_sem=rs, device_id=to, device_id_type=MESH
        )

    sends = []

    def start(copy):
        copy.start()
        sends.append(copy)

    own_cols = pl.ds(pl.multiple_of(c * HD, HD), HD)
    oth_cols = pl.ds(pl.multiple_of(oc * HD, HD), HD)
    lo, hi = pl.ds(0, HD), pl.ds(HD, HD)
    ycols = pl.ds(pl.multiple_of(y * 512, 512), 512)
    yrows = pl.ds(pl.multiple_of(y * 256, 256), 256)
    local = {
        C_K1: (w_key.at[:, oth_cols], wkv_oth.at[:, lo]),
        C_V1: (w_value.at[:, oth_cols], wkv_oth.at[:, hi]),
        C_K0: (w_key.at[:, own_cols], wkv_own.at[:, lo]),
        C_V0: (w_value.at[:, own_cols], wkv_own.at[:, hi]),
        C_Q1: (w_query.at[:, oth_cols], wq.at[:, hi]),
        C_Q0: (w_query.at[:, own_cols], wq.at[:, lo]),
        C_A: (w_a, wa),
        C_B: (w_b, wb),
        C_GA: (w_ga, wga),
        C_GC: (w_gc, wgc),
        C_CO: (w_co, wco),
        C_AO: (w_ao.at[:, ycols], wo.at[yrows, :]),
    }
    local = {k: pltpu.make_async_copy(s, d, lsem.at[k]) for k, (s, d) in local.items()}
    for copy in local.values():
        copy.start()

    barrier = pltpu.get_barrier_semaphore()
    next_chip = lax.rem(chip + 1, NCHIP)
    prev_chip = lax.rem(chip + NCHIP - 1, NCHIP)
    pair_chip = c * next_chip + oc * prev_chip
    pz, px = pair_chip // NX, lax.rem(pair_chip, NX)
    greet = [dev(yy=ypeer(d)) for d in (1, 2, 3)]
    greet += [dev(cc=oc, yy=ypeer(d)) for d in (0, 1, 2, 3)]
    greet += [dev(xx=xpeer(d)) for d in (1, 2, 3)]
    greet += [dev(zz=zpeer(1)), dev(zz=zpeer(-1))]
    greet += [(pz, px, oc, y)]
    for peer in greet:
        pl.semaphore_signal(barrier, inc=1, device_id=peer, device_id_type=MESH)

    hv = hidden[...].astype(F32)
    inv = lax.rsqrt(jnp.mean(hv * hv, axis=1, keepdims=True) + EPS)
    my16 = pl.ds(pl.multiple_of(y * 16, 16), 16)
    hbuf[my16, :] = (hv * inv * pre_gain[...]).astype(BF16)

    r2 = lax.broadcasted_iota(jnp.int32, (2 * HD, 2 * HD), 0) % HD
    c2 = lax.broadcasted_iota(jnp.int32, (2 * HD, 2 * HD), 1)
    tri[...] = jnp.where((r2 > c2) | (c2 >= HD), 1.0, 0.0).astype(BF16)

    pl.semaphore_wait(barrier, len(greet))

    for d in (1, 3, 2):
        start(rc(hbuf.at[my16, :], hbuf.at[my16, :], h_s.at[d], h_r.at[y], dev(yy=ypeer(d))))
    for d in (1, 3, 2):
        yy = ypeer(d)
        rows = pl.ds(pl.multiple_of(yy * 16, 16), 16)
        rc(hbuf.at[rows, :], hbuf.at[rows, :], h_s.at[d], h_r.at[yy], dev(yy=yy)).wait_recv()

    my64 = pl.ds(pl.multiple_of(c * 64, 64), 64)
    oth64 = pl.ds(pl.multiple_of(oc * 64, 64), 64)
    partner = dev(cc=oc)
    local[C_K1].wait()
    local[C_V1].wait()
    kvst[...] = dot(hbuf[...], wkv_oth[...]).astype(BF16)
    start(rc(kvst, kvbuf.at[chip, my64, :], p_s.at[0], p_r.at[0], partner))
    local[C_K0].wait()
    local[C_V0].wait()
    kvbuf[chip, my64, :] = dot(hbuf[...], wkv_own[...]).astype(BF16)
    rc(kvst, kvbuf.at[chip, oth64, :], p_s.at[0], p_r.at[0], partner).wait_recv()

    def chunk_copy(idx, ss, to):
        return rc(kvbuf.at[idx], kvbuf.at[idx], ss, k_r.at[idx], to)

    counts = [0, 0]

    def send_on(core, dz, dx):
        copies = hops(core, dz, dx)
        if not copies:
            return
        first = counts[core]
        counts[core] += len(copies)

        @pl.when(c == core)
        def _():
            idx = zpeer(dz) * NX + xpeer(dx)
            for i, (axis, step) in enumerate(copies):
                to = dev(zz=zpeer(step)) if axis == "z" else dev(xx=xpeer(step))
                chunk_copy(idx, k_s.at[first + i], to).start()

    def chunk(n):
        (z0, x0), (z1, x1) = ORDER0[n], ORDER1[n]
        dz = z0 * oc + z1 * c
        dx = x0 * oc + x1 * c
        return zpeer(dz) * NX + xpeer(dx)

    def arrivals(first, last):
        for n in range(first, last):
            if n > 0:
                idx = chunk(n)
                rc(kvbuf.at[idx], kvbuf.at[idx], k_s.at[0], k_r.at[idx], partner).wait_recv()
            send_on(0, *ORDER0[n])
            send_on(1, *ORDER1[n])

    arrivals(0, 1)
    local[C_Q0].wait()
    local[C_Q1].wait()
    qv = dot(hbuf[...], wq[...]).astype(BF16)
    qst[...] = qv[:, HD:]
    start(rc(qst, qbuf.at[my64, :], p_s.at[1], p_r.at[1], partner))
    qbuf[my64, :] = qv[:, :HD]

    for d in (1, 3, 2):
        yy = ypeer(d)
        cols = pl.ds(pl.multiple_of(yy * 512, 512), 512)
        start(rc(w_ao.at[:, cols], wo.at[yrows, :], w_s.at[d], w_r.at[y], dev(yy=yy)))

    local[C_A].wait()
    local[C_B].wait()
    left = dot(hbuf[...], wa[...]).astype(BF16).astype(F32)
    right = dot(hbuf[...], wb[...]).astype(BF16).astype(F32)
    gated = (left * sigmoid(right)).astype(BF16)
    gst[...] = gated[32:, :]
    gbuf[32:, :] = gated.astype(F32)
    halo_to = ((next_chip // NX) * c + z * oc, lax.rem(next_chip, NX) * c + x * oc, oc, y)
    start(rc(gst, halo, halo_s, halo_r, halo_to))

    local[C_GA].wait()
    local[C_GC].wait()
    gateb[0] = sigmoid(dot(hbuf[...], wga[...]).astype(BF16).astype(F32))
    gateb[1] = sigmoid(dot(hbuf[...], wgc[...]).astype(BF16).astype(F32))
    rc(qst, qbuf.at[oth64, :], p_s.at[1], p_r.at[1], partner).wait_recv()

    off = offset[c]
    scale = 1.0 / math.sqrt(HD)

    def blocks(first, last):
        chunks = [chunk(n) for n in range(first, last)]
        needed = chunks[0] <= chip
        for idx in chunks[1:]:
            needed = needed | (idx <= chip)

        @pl.when(needed)
        def _():
            fronts = []
            for n, idx in enumerate(chunks, first):
                s = dot_nt(qbuf[...], kvbuf[idx, :, 0:HD]) * scale + off
                u = jnp.exp(-jnp.abs(s))
                one = 1.0 + u
                tail = jnp.log(one) + (u - (one - 1.0))
                soft = jnp.maximum(s, 0.0) + tail
                logit = s - soft
                if n == 0:
                    rows = lax.broadcasted_iota(jnp.int32, (HD, HD), 0)
                    causal = lax.broadcasted_iota(jnp.int32, (HD, HD), 1) < rows
                    soft = jnp.where(causal, soft, 0.0)
                    logit = jnp.where(causal, logit, -jnp.inf)
                top = soft.astype(BF16)
                rest = (soft - top.astype(F32)).astype(BF16)
                fronts.append((logit, jnp.concatenate([top, rest], axis=1)))
            sums = [dot(pair, tri[...]) for _, pair in fronts]
            for idx, t in zip(chunks, sums):
                tbuf[idx] = t[:, HD:]
            sticks = [jnp.exp(f[0] - t[:, :HD]).astype(BF16) for f, t in zip(fronts, sums)]
            for idx, stick in zip(chunks, sticks):
                obuf[idx] = dot(stick, kvbuf[idx, :, HD:])

    arrivals(1, 4)
    blocks(0, 4)
    arrivals(4, 8)
    blocks(4, 8)

    rc(gst, halo, halo_s, halo_r, halo_to).wait_recv()
    first = (chip * 2 + c) == 0
    gbuf[0:32, :] = jnp.where(first, 0.0, halo[...].astype(F32))
    conv = jnp.broadcast_to(bias[...], (64, 256))
    for i in range(WIDTH):
        conv = conv + taps[i : i + 1, :] * gbuf[2 + i : 66 + i, :]
    local_mean = jnp.mean(conv, axis=1, keepdims=True)
    dev_local = conv - local_mean
    local_m2 = jnp.sum(dev_local * dev_local, axis=1, keepdims=True)
    lane = lax.broadcasted_iota(jnp.int32, (64, HD), 1)
    stx[...] = jnp.where(lane < 64, local_mean, local_m2)
    for d in (1, 3, 2):
        start(rc(stx, srx.at[y], st_s.at[d], st_r.at[y], dev(yy=ypeer(d))))
    convb[...] = conv

    arrivals(8, 12)
    blocks(8, 12)
    arrivals(12, 16)
    blocks(12, 16)

    srx[y] = stx[...]
    for d in (1, 3, 2):
        yy = ypeer(d)
        rc(stx, srx.at[yy], st_s.at[d], st_r.at[yy], dev(yy=yy)).wait_recv()
    stats = [srx[i] for i in range(NY)]
    means = [t[:, 0:1] for t in stats]
    mean = (means[0] + means[1] + means[2] + means[3]) * 0.25
    m2 = stats[0][:, 64:65] + stats[1][:, 64:65] + stats[2][:, 64:65] + stats[3][:, 64:65]
    for t in means:
        m2 = m2 + 256.0 * (t - mean) * (t - mean)
    cn = (convb[...] - mean) * lax.rsqrt(m2 / CONV_CH + EPS) * ngain[...] + nshift[...]
    cn = (cn * sigmoid(cn)).astype(BF16)
    local[C_CO].wait()
    for i in range(NY):
        cst[i] = dot(cn, wco[:, i * 512 : (i + 1) * 512]).astype(BF16)
    for d in (1, 3, 2):
        yy = ypeer(d)
        start(rc(cst.at[yy], crx.at[y], c_s.at[d], c_r.at[y], dev(yy=yy)))

    arrivals(16, 20)
    blocks(16, 20)
    arrivals(20, 24)
    blocks(20, 24)

    csum = cst[y].astype(F32)
    for d in (1, 3, 2):
        yy = ypeer(d)
        rc(cst.at[yy], crx.at[yy], c_s.at[d], c_r.at[yy], dev(yy=yy)).wait_recv()
        csum = csum + crx[yy].astype(F32)
    gateb[1] = gateb[1] * csum.astype(BF16).astype(F32)

    arrivals(24, 28)
    blocks(24, 28)
    arrivals(28, 32)
    blocks(28, 32)

    def combine(j, state):
        acc, carry = state
        idx = chip - j
        return (acc + obuf[idx] * jnp.exp(-carry), carry + tbuf[idx])

    zero = jnp.zeros((HD, HD), F32)
    acc, _ = lax.fori_loop(0, chip + 1, combine, (zero, zero))
    att[...] = acc.astype(BF16)

    head = pl.ds(pl.multiple_of((y * 2 + c) * HD, HD), HD)
    n = 0
    for d in (0, 1, 3, 2):
        for cc, rows in ((c, my64), (oc, oth64)):
            if d == 0 and cc is c:
                continue
            start(rc(att.at[rows, :], abuf.at[:, head], a_s.at[n], a_r.at[y * 2 + c], dev(cc=cc, yy=ypeer(d))))
            n += 1
    abuf[:, head] = att[my64, :]
    local[C_AO].wait()
    for d in (1, 3, 2):
        yy = ypeer(d)
        rows = pl.ds(pl.multiple_of(yy * 256, 256), 256)
        rc(w_ao.at[:, ycols], wo.at[rows, :], w_s.at[d], w_r.at[yy], dev(yy=yy)).wait_recv()
    for d in (0, 1, 3, 2):
        for cc in (c, oc):
            if d == 0 and cc is c:
                continue
            yy = ypeer(d)
            h = yy * 2 + cc
            cols = pl.ds(pl.multiple_of(h * HD, HD), HD)
            rc(att.at[my64, :], abuf.at[:, cols], a_s.at[0], a_r.at[h], dev(cc=oc, yy=yy)).wait_recv()
    branch = dot(abuf[...], wo[...]).astype(BF16).astype(F32)
    merged = gateb[0] * branch + gateb[1]
    sq = merged * merged
    part = sq[:, 0:128] + sq[:, 128:256] + sq[:, 256:384] + sq[:, 384:512]
    part = jnp.concatenate([part, jnp.zeros((64, HD), F32)], axis=0).T
    ssx[...] = jnp.sum(part.reshape(16, 8, HD), axis=0)
    for d in (1, 3, 2):
        start(rc(ssx, ssr.at[y], ss_s.at[d], ss_r.at[y], dev(yy=ypeer(d))))
    total = ssx[...]
    for d in (1, 3, 2):
        yy = ypeer(d)
        rc(ssx, ssr.at[yy], ss_s.at[d], ss_r.at[yy], dev(yy=yy)).wait_recv()
        total = total + ssr[yy]
    total = jnp.broadcast_to(jnp.sum(total, axis=0, keepdims=True), (HD, HD)).T[:64, 0:1]
    out[...] = (merged * lax.rsqrt(total / D + EPS) * post_gain[...]).astype(BF16)

    for copy in sends:
        copy.wait_send()
    for i in range(max(SENDS)):
        ended = rc(kvbuf.at[chip], kvbuf.at[chip], k_s.at[i], k_r.at[chip], partner).wait_send
        if i < min(SENDS):
            ended()
        else:
            pl.when(c == SENDS.index(max(SENDS)))(ended)


def on_device(
    hidden_in, pre_gain, w_query, w_key, w_value, stick_offset, w_glu_a, w_glu_b, w_gate_attn,
    w_gate_conv, conv_taps, conv_bias, norm_gain, norm_shift, w_attn_out, w_conv_out, post_gain,
):
    vm = pl.BlockSpec(memory_space=pltpu.VMEM)
    hb = pl.BlockSpec(memory_space=pl.ANY)
    sm = pl.BlockSpec(memory_space=pltpu.SMEM)
    dma = pltpu.SemaphoreType.DMA
    return pl.pallas_call(
        kernel,
        out_shape=jax.ShapeDtypeStruct((64, 512), BF16),
        in_specs=[vm, vm, hb, hb, hb, sm, hb, hb, hb, hb, vm, vm, vm, vm, hb, hb, vm],
        out_specs=vm,
        scratch_shapes=[
            pltpu.VMEM((64, D), BF16),
            pltpu.VMEM((D, 256), BF16),
            pltpu.VMEM((D, 256), BF16),
            pltpu.VMEM((D, 256), BF16),
            pltpu.VMEM((D, 256), BF16),
            pltpu.VMEM((D, 256), BF16),
            pltpu.VMEM((D, 512), BF16),
            pltpu.VMEM((D, 512), BF16),
            pltpu.VMEM((256, D), BF16),
            pltpu.VMEM((1024, 512), BF16),
            pltpu.VMEM((NCHIP, 128, 256), BF16),
            pltpu.VMEM((64, 256), BF16),
            pltpu.VMEM((128, 128), BF16),
            pltpu.VMEM((64, 128), BF16),
            pltpu.VMEM((NCHIP, 128, 128), F32),
            pltpu.VMEM((NCHIP, 128, 128), F32),
            pltpu.VMEM((256, 256), BF16),
            pltpu.VMEM((32, 256), BF16),
            pltpu.VMEM((32, 256), BF16),
            pltpu.VMEM((96, 256), F32),
            pltpu.VMEM((NY, 64, 512), BF16),
            pltpu.VMEM((NY, 64, 512), BF16),
            pltpu.VMEM((64, 128), F32),
            pltpu.VMEM((NY, 64, 128), F32),
            pltpu.VMEM((64, 256), F32),
            pltpu.VMEM((2, 64, 512), F32),
            pltpu.VMEM((128, 128), BF16),
            pltpu.VMEM((64, 1024), BF16),
            pltpu.VMEM((8, 128), F32),
            pltpu.VMEM((NY, 8, 128), F32),
            dma((12,)),
            dma((4,)), dma((4,)),
            dma((2,)), dma((2,)),
            dma((max(SENDS),)), dma((NCHIP,)),
            dma, dma,
            dma((4,)), dma((4,)),
            dma((4,)), dma((4,)),
            dma((4,)), dma((4,)),
            dma((7,)), dma((8,)),
            dma((4,)), dma((4,)),
        ],
        compiler_params=pltpu.CompilerParams(
            collective_id=0, has_side_effects=True, vmem_limit_bytes=56 * 1024 * 1024
        ),
    )(
        hidden_in, pre_gain.reshape(1, -1), w_query, w_key, w_value, stick_offset, w_glu_a,
        w_glu_b, w_gate_attn, w_gate_conv, conv_taps, conv_bias.reshape(1, -1),
        norm_gain.reshape(1, -1), norm_shift.reshape(1, -1), w_attn_out, w_conv_out,
        post_gain.reshape(1, -1),
    )


def solution(mesh):
    torus = Mesh(mesh.devices.reshape(NZ, NX, 2, NY), ("z", "x", "c", "y"))
    every = ("z", "x", "c", "y")
    cols = P(None, "y")
    return jax.shard_map(
        on_device,
        mesh=torus,
        in_specs=(
            P(every, None), P(), cols, cols, cols, P("y"), cols, cols, cols, cols, cols,
            P("y"), P("y"), P("y"), P("y", None), P("y", None), P("y"),
        ),
        out_specs=P(("z", "x", "c"), "y"),
        check_vma=False,
    )
```

```python
import functools
import math

import jax
import jax.numpy as jnp
from jax import lax
from jax.experimental import pallas as pl
from jax.experimental.pallas import tpu as pltpu
from jax.sharding import Mesh
from jax.sharding import PartitionSpec as P

D = 2048
HD = 128
CONV_CH = 1024
WIDTH = 31
EPS = 1e-06
MESH = pl.DeviceIdType.MESH
F32 = jnp.float32
BF16 = jnp.bfloat16
NX = 4
NZ = 8
NY = 4
NCHIP = NX * NZ


ORDER = (
    (0, 0), (7, 0), (1, 0), (6, 0), (0, 1), (0, 3), (2, 0), (5, 0),
    (7, 1), (7, 3), (3, 0), (1, 1), (1, 3), (6, 1), (6, 3), (4, 0),
    (2, 1), (0, 2), (5, 1), (2, 3), (7, 2), (5, 3), (3, 1), (3, 3),
    (6, 2), (1, 2), (4, 1), (4, 3), (5, 2), (2, 2), (3, 2), (4, 2),
)
UP = 4
WRAPS = (7, 6, 5)


def hops(k, dx):
    if dx == 0:
        return [("x", 1), ("x", 3)] + [("z", 1)] * (k < UP)
    if dx == 3:
        return [("x", 1)] if k % 2 == 0 else []
    return [("x", 3)] if dx == 1 and k % 2 == 1 else []


SENDS = sum(len(hops(*t)) for t in ORDER)


def dot(a, b):
    return jnp.dot(a, b, preferred_element_type=F32)


def dot_nt(a, b):
    return lax.dot_general(a, b, (((1,), (1,)), ((), ())), preferred_element_type=F32)


def sigmoid(v):
    return jax.nn.sigmoid(v)


(C_K0, C_V0, C_K1, C_V1, C_Q0, C_Q1, C_A, C_B, C_GA, C_GC, C_CO, C_AO) = range(12)


def kernel(
    hidden, pre_gain, w_query, w_key, w_value, offset, w_a, w_b, w_ga, w_gc,
    taps, bias, ngain, nshift, w_ao, w_co, post_gain,
    out,
    hbuf, wkv_own, wkv_oth, wq, wa, wb, wga, wgc, wco, wo,
    kvbuf, kvst, qbuf, qst, obuf, tbuf, tri,
    gst, halo, gbuf, cst, crx, stx, srx, convb, gateb, att, abuf, ssx, ssr,
    lsem, h_s, h_r, p_s, p_r, k_s, wrap_s, k_r, ready, halo_s, halo_r,
    w_s, w_r, v_s, v_r, st_s, st_r, c_s, c_r, a_s, a_r, ss_s, ss_r,
):
    z = lax.axis_index("z")
    x = lax.axis_index("x")
    c = lax.axis_index("c")
    y = lax.axis_index("y")
    chip = z * NX + x
    oc = 1 - c

    def dev(zz=z, xx=x, cc=c, yy=y):
        return (zz, xx, cc, yy)

    def ypeer(d):
        return lax.rem(y + d, NY)

    def xpeer(d):
        return lax.rem(x + d, NX)

    def zpeer(d):
        return lax.rem(z + d + NZ, NZ)

    def rc(src, dst, ss, rs, to):
        return pltpu.make_async_remote_copy(
            src_ref=src, dst_ref=dst, send_sem=ss, recv_sem=rs, device_id=to, device_id_type=MESH
        )

    half = pl.ds(pl.multiple_of(c * HD, HD), HD)

    def whalf(yy, cc):
        return pl.ds(pl.multiple_of(yy * 256 + cc * HD, HD), HD)

    sends = []

    def start(copy):
        copy.start()
        sends.append(copy)

    own_cols = pl.ds(pl.multiple_of(c * HD, HD), HD)
    oth_cols = pl.ds(pl.multiple_of(oc * HD, HD), HD)
    lo, hi = pl.ds(0, HD), pl.ds(HD, HD)
    ycols = pl.ds(pl.multiple_of(y * 512, 512), 512)
    yrows = pl.ds(pl.multiple_of(y * 256, 256), 256)
    local = {
        C_K1: (w_key.at[:, oth_cols], wkv_oth.at[:, lo]),
        C_V1: (w_value.at[:, oth_cols], wkv_oth.at[:, hi]),
        C_K0: (w_key.at[:, own_cols], wkv_own.at[:, lo]),
        C_V0: (w_value.at[:, own_cols], wkv_own.at[:, hi]),
        C_Q1: (w_query.at[:, oth_cols], wq.at[:, hi]),
        C_Q0: (w_query.at[:, own_cols], wq.at[:, lo]),
        C_A: (w_a, wa),
        C_B: (w_b, wb),
        C_GA: (w_ga, wga),
        C_GC: (w_gc, wgc),
        C_CO: (w_co, wco),
        C_AO: (w_ao.at[:, ycols], wo.at[yrows, :]),
    }
    local = {k: pltpu.make_async_copy(s, d, lsem.at[k]) for k, (s, d) in local.items()}
    for copy in local.values():
        copy.start()

    barrier = pltpu.get_barrier_semaphore()
    next_chip = lax.rem(chip + 1, NCHIP)
    prev_chip = lax.rem(chip + NCHIP - 1, NCHIP)
    pair_chip = c * next_chip + oc * prev_chip
    pz, px = pair_chip // NX, lax.rem(pair_chip, NX)
    greet = [dev(yy=ypeer(d)) for d in (1, 2, 3)]
    greet += [dev(cc=oc, yy=ypeer(d)) for d in (0, 1, 2, 3)]
    greet += [dev(xx=xpeer(d)) for d in (1, 3)]
    for peer in greet:
        pl.semaphore_signal(barrier, inc=1, device_id=peer, device_id_type=MESH)
    greeted = len(greet)
    for k in (1,) + WRAPS:
        @pl.when(z + k < NZ)
        def _():
            pl.semaphore_signal(barrier, inc=1, device_id=dev(zz=zpeer(k)), device_id_type=MESH)

        greeted = greeted + jnp.where(z >= k, 1, 0)
    next_core = (pz, px, oc, y)
    has_next = (c == 1) & (chip < NCHIP - 1)
    has_prev = (c == 0) & (chip > 0)

    @pl.when(has_next)
    def _():
        pl.semaphore_signal(barrier, inc=1, device_id=next_core, device_id_type=MESH)

    greeted = greeted + jnp.where(has_prev, 1, 0)

    hv = hidden[...].astype(F32)
    inv = lax.rsqrt(jnp.mean(hv * hv, axis=1, keepdims=True) + EPS)
    my16 = pl.ds(pl.multiple_of(y * 16, 16), 16)
    hbuf[my16, :] = (hv * inv * pre_gain[...]).astype(BF16)

    r2 = lax.broadcasted_iota(jnp.int32, (2 * HD, 2 * HD), 0) % HD
    c2 = lax.broadcasted_iota(jnp.int32, (2 * HD, 2 * HD), 1)
    tri[...] = jnp.where((r2 > c2) | (c2 >= HD), 1.0, 0.0).astype(BF16)

    pl.semaphore_wait(barrier, greeted)
    for k in (1,) + WRAPS:
        @pl.when(z >= k)
        def _():
            pl.semaphore_signal(ready.at[k], inc=1, device_id=dev(zz=zpeer(-k)), device_id_type=MESH)

    @pl.when(has_prev)
    def _():
        pl.semaphore_signal(ready.at[0], inc=1, device_id=next_core, device_id_type=MESH)


    for d in (1, 3, 2):
        start(rc(hbuf.at[my16, :], hbuf.at[my16, :], h_s.at[d], h_r.at[y], dev(yy=ypeer(d))))
    for d in (1, 3, 2):
        yy = ypeer(d)
        rows = pl.ds(pl.multiple_of(yy * 16, 16), 16)
        rc(hbuf.at[rows, :], hbuf.at[rows, :], h_s.at[d], h_r.at[yy], dev(yy=yy)).wait_recv()

    my64 = pl.ds(pl.multiple_of(c * 64, 64), 64)
    oth64 = pl.ds(pl.multiple_of(oc * 64, 64), 64)
    partner = dev(cc=oc)
    local[C_K1].wait()
    local[C_V1].wait()
    kvst[...] = dot(hbuf[...], wkv_oth[...]).astype(BF16)
    start(rc(kvst, kvbuf.at[chip, my64, :], p_s.at[0], p_r.at[0], partner))
    local[C_K0].wait()
    local[C_V0].wait()
    kvbuf[chip, my64, :] = dot(hbuf[...], wkv_own[...]).astype(BF16)
    rc(kvst, kvbuf.at[chip, oth64, :], p_s.at[0], p_r.at[0], partner).wait_recv()

    def chunk_copy(idx, ss, to):
        return rc(kvbuf.at[idx], kvbuf.at[idx], ss, k_r.at[idx], to)

    def chunk(n):
        k, dx = ORDER[n]
        return zpeer(-k) * NX + xpeer(dx)

    sent = []

    def send_on(n):
        k, dx = ORDER[n]
        idx = chunk(n)
        for axis, step in hops(k, dx):
            i = len(sent)
            if axis == "x":
                sent.append((k, NZ))
                chunk_copy(idx, k_s.at[i], dev(xx=xpeer(step))).start()
            else:
                sent.append((k, NZ - 1))

                @pl.when(z < NZ - 1)
                def _():
                    if k == 0:
                        pl.semaphore_wait(ready.at[1], 1)
                    chunk_copy(idx, k_s.at[i], dev(zz=zpeer(step))).start()

    def arrivals(first, last):
        for n in range(first, last):
            k, dx = ORDER[n]
            if n == 0:
                send_on(n)
                continue

            @pl.when(z >= k)
            def _():
                idx = chunk(n)
                rc(kvbuf.at[idx], kvbuf.at[idx], k_s.at[0], k_r.at[idx], partner).wait_recv()
                send_on(n)

    arrivals(0, 1)
    local[C_Q0].wait()
    local[C_Q1].wait()
    qv = dot(hbuf[...], wq[...]).astype(BF16)
    qst[...] = qv[:, HD:]
    start(rc(qst, qbuf.at[my64, :], p_s.at[1], p_r.at[1], partner))
    qbuf[my64, :] = qv[:, :HD]

    local[C_A].wait()
    local[C_B].wait()
    left = dot(hbuf[...], wa[...]).astype(BF16).astype(F32)
    right = dot(hbuf[...], wb[...]).astype(BF16).astype(F32)
    gated = (left * sigmoid(right)).astype(BF16)
    gst[...] = gated[32:, :]
    gbuf[32:, :] = gated.astype(F32)
    halo_to = ((next_chip // NX) * c + z * oc, lax.rem(next_chip, NX) * c + x * oc, oc, y)

    @pl.when(has_next)
    def _():
        pl.semaphore_wait(ready.at[0], 1)

    has_halo = (c == 1) | (chip > 0)
    sends_halo = (c == 0) | (chip < NCHIP - 1)

    @pl.when(sends_halo)
    def _():
        rc(gst, halo, halo_s, halo_r, halo_to).start()

    for i, k in enumerate(WRAPS):
        @pl.when(z + k < NZ)
        def _():
            pl.semaphore_wait(ready.at[k], 1)
            chunk_copy(chip, wrap_s.at[i], dev(zz=zpeer(k))).start()


    local[C_GA].wait()
    local[C_GC].wait()
    gateb[0] = sigmoid(dot(hbuf[...], wga[...]).astype(BF16).astype(F32))
    gateb[1] = sigmoid(dot(hbuf[...], wgc[...]).astype(BF16).astype(F32))
    rc(qst, qbuf.at[oth64, :], p_s.at[1], p_r.at[1], partner).wait_recv()

    off = offset[c]
    scale = 1.0 / math.sqrt(HD)

    def blocks(first, last):
        chunks = [chunk(n) for n in range(first, last)]

        @pl.when(z >= min(ORDER[n][0] for n in range(first, last)))
        def _():
            fronts = []
            for n, idx in enumerate(chunks, first):
                s = dot_nt(qbuf[...], kvbuf[idx, :, 0:HD]) * scale + off
                u = jnp.exp(-jnp.abs(s))
                one = 1.0 + u
                tail = jnp.log(one) + (u - (one - 1.0))
                soft = jnp.maximum(s, 0.0) + tail
                logit = s - soft
                if n == 0:
                    rows = lax.broadcasted_iota(jnp.int32, (HD, HD), 0)
                    causal = lax.broadcasted_iota(jnp.int32, (HD, HD), 1) < rows
                    soft = jnp.where(causal, soft, 0.0)
                    logit = jnp.where(causal, logit, -jnp.inf)
                top = soft.astype(BF16)
                rest = (soft - top.astype(F32)).astype(BF16)
                fronts.append((logit, jnp.concatenate([top, rest], axis=1)))
            sums = [dot(pair, tri[...]) for _, pair in fronts]
            for idx, t in zip(chunks, sums):
                tbuf[idx] = t[:, HD:]
            sticks = [jnp.exp(f[0] - t[:, :HD]).astype(BF16) for f, t in zip(fronts, sums)]
            for idx, stick in zip(chunks, sticks):
                obuf[idx] = dot(stick, kvbuf[idx, :, HD:])

    @pl.when(has_halo)
    def _():
        rc(gst, halo, halo_s, halo_r, halo_to).wait_recv()
        gbuf[0:32, :] = halo[...].astype(F32)

    @pl.when(jnp.logical_not(has_halo))
    def _():
        gbuf[0:32, :] = jnp.zeros((32, 256), F32)

    conv = jnp.broadcast_to(bias[...], (64, 256))
    for i in range(WIDTH):
        conv = conv + taps[i : i + 1, :] * gbuf[2 + i : 66 + i, :]
    local_mean = jnp.mean(conv, axis=1, keepdims=True)
    dev_local = conv - local_mean
    local_m2 = jnp.sum(dev_local * dev_local, axis=1, keepdims=True)
    lane = lax.broadcasted_iota(jnp.int32, (64, HD), 1)
    stx[...] = jnp.where(lane < 64, local_mean, local_m2)
    for d in (1, 3, 2):
        start(rc(stx, srx.at[y], st_s.at[d], st_r.at[y], dev(yy=ypeer(d))))
    convb[...] = conv

    arrivals(1, 4)
    blocks(0, 4)
    srx[y] = stx[...]
    for d in (1, 3, 2):
        yy = ypeer(d)
        rc(stx, srx.at[yy], st_s.at[d], st_r.at[yy], dev(yy=yy)).wait_recv()
    stats = [srx[i] for i in range(NY)]
    means = [t[:, 0:1] for t in stats]
    mean = (means[0] + means[1] + means[2] + means[3]) * 0.25
    m2 = stats[0][:, 64:65] + stats[1][:, 64:65] + stats[2][:, 64:65] + stats[3][:, 64:65]
    for t in means:
        m2 = m2 + 256.0 * (t - mean) * (t - mean)
    cn = (convb[...] - mean) * lax.rsqrt(m2 / CONV_CH + EPS) * ngain[...] + nshift[...]
    cn = (cn * sigmoid(cn)).astype(BF16)
    local[C_CO].wait()
    for i in range(NY):
        cst[i] = dot(cn, wco[:, i * 512 : (i + 1) * 512]).astype(BF16)
    for d in (1, 3, 2):
        yy = ypeer(d)
        start(rc(cst.at[yy], crx.at[y], c_s.at[d], c_r.at[y], dev(yy=yy)))

    for d in (1, 3, 2):
        yy = ypeer(d)
        cols = pl.ds(pl.multiple_of(yy * 512, 512), 512)
        start(rc(w_ao.at[half, cols], wo.at[whalf(y, c), :], w_s.at[d], w_r.at[y], dev(yy=yy)))

    arrivals(4, 8)
    blocks(4, 8)

    arrivals(8, 12)
    blocks(8, 12)
    arrivals(12, 16)
    blocks(12, 16)

    arrivals(16, 20)
    blocks(16, 20)

    csum = cst[y].astype(F32)
    for d in (1, 3, 2):
        yy = ypeer(d)
        rc(cst.at[yy], crx.at[yy], c_s.at[d], c_r.at[yy], dev(yy=yy)).wait_recv()
        csum = csum + crx[yy].astype(F32)
    gateb[1] = gateb[1] * csum.astype(BF16).astype(F32)

    arrivals(20, 24)
    blocks(20, 24)
    arrivals(24, 28)
    blocks(24, 28)
    for d in (1, 3, 2):
        yy = ypeer(d)
        got = wo.at[whalf(yy, c), :]
        rc(got, got, w_s.at[d], w_r.at[yy], dev(yy=yy)).wait_recv()
        start(rc(got, got, v_s.at[d], v_r.at[yy], partner))

    arrivals(28, 32)
    blocks(28, 32)

    def combine(j, state):
        acc, carry = state
        idx = chip - j
        return (acc + obuf[idx] * jnp.exp(-carry), carry + tbuf[idx])

    zero = jnp.zeros((HD, HD), F32)
    acc, _ = lax.fori_loop(0, chip + 1, combine, (zero, zero))
    att[...] = acc.astype(BF16)

    head = pl.ds(pl.multiple_of((y * 2 + c) * HD, HD), HD)
    n = 0
    for d in (0, 1, 3, 2):
        for cc, rows in ((c, my64), (oc, oth64)):
            if d == 0 and cc is c:
                continue
            start(rc(att.at[rows, :], abuf.at[:, head], a_s.at[n], a_r.at[y * 2 + c], dev(cc=cc, yy=ypeer(d))))
            n += 1
    abuf[:, head] = att[my64, :]
    local[C_AO].wait()
    for d in (1, 3, 2):
        yy = ypeer(d)
        came = wo.at[whalf(yy, oc), :]
        rc(came, came, v_s.at[d], v_r.at[yy], partner).wait_recv()
    for d in (0, 1, 3, 2):
        for cc in (c, oc):
            if d == 0 and cc is c:
                continue
            yy = ypeer(d)
            h = yy * 2 + cc
            cols = pl.ds(pl.multiple_of(h * HD, HD), HD)
            rc(att.at[my64, :], abuf.at[:, cols], a_s.at[0], a_r.at[h], dev(cc=oc, yy=yy)).wait_recv()
    branch = dot(abuf[...], wo[...]).astype(BF16).astype(F32)
    merged = gateb[0] * branch + gateb[1]
    sq = merged * merged
    part = sq[:, 0:128] + sq[:, 128:256] + sq[:, 256:384] + sq[:, 384:512]
    part = jnp.concatenate([part, jnp.zeros((64, HD), F32)], axis=0).T
    ssx[...] = jnp.sum(part.reshape(16, 8, HD), axis=0)
    for d in (1, 3, 2):
        start(rc(ssx, ssr.at[y], ss_s.at[d], ss_r.at[y], dev(yy=ypeer(d))))
    total = ssx[...]
    for d in (1, 3, 2):
        yy = ypeer(d)
        rc(ssx, ssr.at[yy], ss_s.at[d], ss_r.at[yy], dev(yy=yy)).wait_recv()
        total = total + ssr[yy]
    total = jnp.broadcast_to(jnp.sum(total, axis=0, keepdims=True), (HD, HD)).T[:64, 0:1]
    out[...] = (merged * lax.rsqrt(total / D + EPS) * post_gain[...]).astype(BF16)

    for copy in sends:
        copy.wait_send()
    for i, (k, end) in enumerate(sent):
        @pl.when((z >= k) & (z < end))
        def _():
            rc(kvbuf.at[chip], kvbuf.at[chip], k_s.at[i], k_r.at[chip], partner).wait_send()

    for i, k in enumerate(WRAPS):
        @pl.when(z + k < NZ)
        def _():
            rc(kvbuf.at[chip], kvbuf.at[chip], wrap_s.at[i], k_r.at[chip], partner).wait_send()

    @pl.when(sends_halo)
    def _():
        rc(gst, halo, halo_s, halo_r, halo_to).wait_send()


def on_device(
    hidden_in, pre_gain, w_query, w_key, w_value, stick_offset, w_glu_a, w_glu_b, w_gate_attn,
    w_gate_conv, conv_taps, conv_bias, norm_gain, norm_shift, w_attn_out, w_conv_out, post_gain,
):
    vm = pl.BlockSpec(memory_space=pltpu.VMEM)
    hb = pl.BlockSpec(memory_space=pl.ANY)
    sm = pl.BlockSpec(memory_space=pltpu.SMEM)
    dma = pltpu.SemaphoreType.DMA
    return pl.pallas_call(
        kernel,
        out_shape=jax.ShapeDtypeStruct((64, 512), BF16),
        in_specs=[vm, vm, hb, hb, hb, sm, hb, hb, hb, hb, vm, vm, vm, vm, hb, hb, vm],
        out_specs=vm,
        scratch_shapes=[
            pltpu.VMEM((64, D), BF16),
            pltpu.VMEM((D, 256), BF16),
            pltpu.VMEM((D, 256), BF16),
            pltpu.VMEM((D, 256), BF16),
            pltpu.VMEM((D, 256), BF16),
            pltpu.VMEM((D, 256), BF16),
            pltpu.VMEM((D, 512), BF16),
            pltpu.VMEM((D, 512), BF16),
            pltpu.VMEM((256, D), BF16),
            pltpu.VMEM((1024, 512), BF16),
            pltpu.VMEM((NCHIP, 128, 256), BF16),
            pltpu.VMEM((64, 256), BF16),
            pltpu.VMEM((128, 128), BF16),
            pltpu.VMEM((64, 128), BF16),
            pltpu.VMEM((NCHIP, 128, 128), F32),
            pltpu.VMEM((NCHIP, 128, 128), F32),
            pltpu.VMEM((256, 256), BF16),
            pltpu.VMEM((32, 256), BF16),
            pltpu.VMEM((32, 256), BF16),
            pltpu.VMEM((96, 256), F32),
            pltpu.VMEM((NY, 64, 512), BF16),
            pltpu.VMEM((NY, 64, 512), BF16),
            pltpu.VMEM((64, 128), F32),
            pltpu.VMEM((NY, 64, 128), F32),
            pltpu.VMEM((64, 256), F32),
            pltpu.VMEM((2, 64, 512), F32),
            pltpu.VMEM((128, 128), BF16),
            pltpu.VMEM((64, 1024), BF16),
            pltpu.VMEM((8, 128), F32),
            pltpu.VMEM((NY, 8, 128), F32),
            dma((12,)),
            dma((4,)), dma((4,)),
            dma((2,)), dma((2,)),
            dma((SENDS,)), dma((3,)), dma((NCHIP,)), pltpu.SemaphoreType.REGULAR((8,)),
            dma, dma,
            dma((4,)), dma((4,)), dma((4,)), dma((4,)),
            dma((4,)), dma((4,)),
            dma((4,)), dma((4,)),
            dma((7,)), dma((8,)),
            dma((4,)), dma((4,)),
        ],
        compiler_params=pltpu.CompilerParams(
            collective_id=0, has_side_effects=True, vmem_limit_bytes=56 * 1024 * 1024
        ),
    )(
        hidden_in, pre_gain.reshape(1, -1), w_query, w_key, w_value, stick_offset, w_glu_a,
        w_glu_b, w_gate_attn, w_gate_conv, conv_taps, conv_bias.reshape(1, -1),
        norm_gain.reshape(1, -1), norm_shift.reshape(1, -1), w_attn_out, w_conv_out,
        post_gain.reshape(1, -1),
    )


def solution(mesh):
    torus = Mesh(mesh.devices.reshape(NZ, NX, 2, NY), ("z", "x", "c", "y"))
    every = ("z", "x", "c", "y")
    cols = P(None, "y")
    return jax.shard_map(
        on_device,
        mesh=torus,
        in_specs=(
            P(every, None), P(), cols, cols, cols, P("y"), cols, cols, cols, cols, cols,
            P("y"), P("y"), P("y"), P("y", None), P("y", None), P("y"),
        ),
        out_specs=P(("z", "x", "c"), "y"),
        check_vma=False,
    )
```

```python
import functools
import math

import jax
import jax.numpy as jnp
from jax import lax
from jax.experimental import pallas as pl
from jax.experimental.pallas import tpu as pltpu
from jax.sharding import Mesh
from jax.sharding import PartitionSpec as P

D = 2048
HD = 128
CONV_CH = 1024
WIDTH = 31
EPS = 1e-06
MESH = pl.DeviceIdType.MESH
F32 = jnp.float32
BF16 = jnp.bfloat16
NX = 4
NZ = 8
NY = 4
NCHIP = NX * NZ


STEPS = (1, 2)
WRAPS = (7, 6, 5)
GREETED = STEPS + WRAPS


def dot(a, b):
    return jnp.dot(a, b, preferred_element_type=F32)


def dot_nt(a, b):
    return lax.dot_general(a, b, (((1,), (1,)), ((), ())), preferred_element_type=F32)


def sigmoid(v):
    return jax.nn.sigmoid(v)


(C_K0, C_K1, C_V0, C_V1, C_Q0, C_Q1, C_A, C_B, C_GA, C_GC, C_CO, C_AO) = range(12)


def kernel(
    hidden_hbm, pre_gain_hbm, w_query, w_key, w_value, offset, w_a, w_b, w_ga, w_gc,
    taps_hbm, bias_hbm, ngain_hbm, nshift_hbm, w_ao, w_co, post_gain_hbm,
    out,
    hidden, pre_gain, taps, bias, ngain, nshift, post_gain, hbuf, wk, wv, wq, wa, wb, wga, wgc, wco, wo,
    kbuf, vbuf, kst, vst, qbuf, qst, obuf, tbl, tblr, wbuf, ps, pr, tri,
    gst, halo, gbuf, cst, crx, stx, srx, convb, gateb, att, abuf, ssx, ssr,
    lsem, ssem, h_s, h_r, p_s, p_r, z_s, z_r, q_s, q_r, t_s, t_r, o_s, o_r, ready, halo_s, halo_r,
    w_s, w_r, v_s, v_r, st_s, st_r, c_s, c_r, a_s, a_r, ss_s, ss_r,
):
    z = lax.axis_index("z")
    x = lax.axis_index("x")
    c = lax.axis_index("c")
    y = lax.axis_index("y")
    chip = z * NX + x
    oc = 1 - c

    def dev(zz=z, xx=x, cc=c, yy=y):
        return (zz, xx, cc, yy)

    def ypeer(d):
        return lax.rem(y + d, NY)

    def xpeer(d):
        return lax.rem(x + d, NX)

    def zpeer(d):
        return lax.rem(z + d + NZ, NZ)

    def rc(src, dst, ss, rs, to):
        return pltpu.make_async_remote_copy(
            src_ref=src, dst_ref=dst, send_sem=ss, recv_sem=rs, device_id=to, device_id_type=MESH
        )

    half = pl.ds(pl.multiple_of(c * HD, HD), HD)

    def whalf(yy, cc):
        return pl.ds(pl.multiple_of(yy * 256 + cc * HD, HD), HD)

    sends = []

    def start(copy):
        copy.start()
        sends.append(copy)

    own_cols = pl.ds(pl.multiple_of(c * HD, HD), HD)
    oth_cols = pl.ds(pl.multiple_of(oc * HD, HD), HD)
    lo, hi = pl.ds(0, HD), pl.ds(HD, HD)
    ycols = pl.ds(pl.multiple_of(y * 512, 512), 512)
    yrows = pl.ds(pl.multiple_of(y * 256, 256), 256)
    local = {
        C_K1: (w_key.at[:, oth_cols], wk.at[:, lo]),
        C_K0: (w_key.at[:, own_cols], wk.at[:, hi]),
        C_V1: (w_value.at[:, oth_cols], wv.at[:, lo]),
        C_V0: (w_value.at[:, own_cols], wv.at[:, hi]),
        C_Q1: (w_query.at[:, oth_cols], wq.at[:, hi]),
        C_Q0: (w_query.at[:, own_cols], wq.at[:, lo]),
        C_A: (w_a, wa),
        C_B: (w_b, wb),
        C_GA: (w_ga, wga),
        C_GC: (w_gc, wgc),
        C_CO: (w_co, wco),
        C_AO: (w_ao.at[:, ycols], wo.at[yrows, :]),
    }
    local = {k: pltpu.make_async_copy(s, d, lsem.at[k]) for k, (s, d) in local.items()}
    barrier = pltpu.get_barrier_semaphore()
    next_chip = lax.rem(chip + 1, NCHIP)
    prev_chip = lax.rem(chip + NCHIP - 1, NCHIP)
    pair_chip = c * next_chip + oc * prev_chip
    pz, px = pair_chip // NX, lax.rem(pair_chip, NX)
    greet = [dev(yy=ypeer(d)) for d in (1, 2, 3)]
    greet += [dev(cc=oc, yy=ypeer(d)) for d in (0, 1, 2, 3)]
    greet += [dev(xx=xpeer(d), cc=cc) for d in (1, 2, 3) for cc in (c, oc)]
    for peer in greet:
        pl.semaphore_signal(barrier, inc=1, device_id=peer, device_id_type=MESH)
    greeted = len(greet)
    for k in GREETED:
        @pl.when(z + k < NZ)
        def _():
            pl.semaphore_signal(barrier, inc=1, device_id=dev(zz=zpeer(k)), device_id_type=MESH)

        greeted = greeted + jnp.where(z >= k, 1, 0)
    next_core = (pz, px, oc, y)
    has_next = (c == 1) & (chip < NCHIP - 1)
    has_prev = (c == 0) & (chip > 0)

    @pl.when(has_next)
    def _():
        pl.semaphore_signal(barrier, inc=1, device_id=next_core, device_id_type=MESH)

    greeted = greeted + jnp.where(has_prev, 1, 0)

    first_in = [(hidden_hbm, hidden), (pre_gain_hbm, pre_gain)]
    later_in = [
        (taps_hbm, taps), (bias_hbm, bias), (ngain_hbm, ngain), (nshift_hbm, nshift), (post_gain_hbm, post_gain)
    ]
    small = [
        pltpu.make_async_copy(a, b, ssem.at[i]) for i, (a, b) in enumerate(first_in + later_in)
    ]
    for copy in small[:2]:
        copy.start()
    for copy in local.values():
        copy.start()
    for copy in small[2:]:
        copy.start()

    r2 = lax.broadcasted_iota(jnp.int32, (2 * HD, HD), 0) % HD
    c2 = lax.broadcasted_iota(jnp.int32, (2 * HD, HD), 1)
    tri[...] = jnp.where(r2 > c2, 1.0, 0.0).astype(BF16)
    obuf[...] = jnp.zeros(obuf.shape, F32)
    tbl[...] = jnp.zeros(tbl.shape, F32)
    for copy in small[:2]:
        copy.wait()

    hv = hidden[...].astype(F32)
    inv = lax.rsqrt(jnp.mean(hv * hv, axis=1, keepdims=True) + EPS)
    my16 = pl.ds(pl.multiple_of(y * 16, 16), 16)
    hbuf[my16, :] = (hv * inv * pre_gain[...]).astype(BF16)

    pl.semaphore_wait(barrier, greeted)
    for k in GREETED:
        @pl.when(z >= k)
        def _():
            pl.semaphore_signal(ready.at[k], inc=1, device_id=dev(zz=zpeer(-k)), device_id_type=MESH)

    @pl.when(has_prev)
    def _():
        pl.semaphore_signal(ready.at[0], inc=1, device_id=next_core, device_id_type=MESH)


    for d in (1, 3, 2):
        start(rc(hbuf.at[my16, :], hbuf.at[my16, :], h_s.at[d], h_r.at[y], dev(yy=ypeer(d))))
    for d in (1, 3, 2):
        yy = ypeer(d)
        rows = pl.ds(pl.multiple_of(yy * 16, 16), 16)
        rc(hbuf.at[rows, :], hbuf.at[rows, :], h_s.at[d], h_r.at[yy], dev(yy=yy)).wait_recv()

    my64 = pl.ds(pl.multiple_of(c * 64, 64), 64)
    oth64 = pl.ds(pl.multiple_of(oc * 64, 64), 64)
    partner = dev(cc=oc)
    tables = (kbuf, vbuf)
    for h, (w, st, copies) in enumerate(((wk, kst, (C_K1, C_K0)), (wv, vst, (C_V1, C_V0)))):
        for name in copies:
            local[name].wait()
        both = dot(hbuf[...], w[...]).astype(BF16)
        st[...] = both[:, :HD]
        start(rc(st, tables[h].at[z, my64, :], p_s.at[h], p_r.at[h], partner))
        tables[h][z, my64, :] = both[:, HD:]

    def z_copy(h, row, i, step):
        t = tables[h].at[row]
        return rc(t, t, z_s.at[i], z_r.at[h * NZ + row], dev(zz=zpeer(step)))

    for h in (0, 1):
        rc(kst, tables[h].at[z, oth64, :], p_s.at[h], p_r.at[h], partner).wait_recv()
        for i, step in enumerate(STEPS):
            @pl.when(z < NZ - step)
            def _():
                if h == 0:
                    pl.semaphore_wait(ready.at[step], 1)
                z_copy(h, z, h * 2 + i, step).start()

    local[C_Q0].wait()
    local[C_Q1].wait()
    qv = dot(hbuf[...], wq[...]).astype(BF16)
    qst[...] = qv[:, HD:]

    def qrows(xx, cc):
        return pl.ds(pl.multiple_of(xx * HD + cc * 64, 64), 64)

    mine = qbuf.at[qrows(x, c), :]
    qbuf[qrows(x, c), :] = qv[:, :HD]
    for d in range(NX):
        start(rc(qst, mine, q_s.at[d], q_r.at[x * 2 + c], dev(xx=xpeer(d), cc=oc)))
        if d > 0:
            start(rc(mine, mine, q_s.at[3 + d], q_r.at[x * 2 + c], dev(xx=xpeer(d))))

    local[C_A].wait()
    local[C_B].wait()
    left = dot(hbuf[...], wa[...]).astype(BF16).astype(F32)
    right = dot(hbuf[...], wb[...]).astype(BF16).astype(F32)
    gated = (left * sigmoid(right)).astype(BF16)
    gst[...] = gated[32:, :]
    gbuf[32:, :] = gated.astype(F32)
    halo_to = ((next_chip // NX) * c + z * oc, lax.rem(next_chip, NX) * c + x * oc, oc, y)

    @pl.when(has_next)
    def _():
        pl.semaphore_wait(ready.at[0], 1)

    has_halo = (c == 1) | (chip > 0)
    sends_halo = (c == 0) | (chip < NCHIP - 1)

    @pl.when(sends_halo)
    def _():
        rc(gst, halo, halo_s, halo_r, halo_to).start()

    for i, k in enumerate(WRAPS):
        @pl.when(z + k < NZ)
        def _():
            pl.semaphore_wait(ready.at[k], 1)
            for h in (0, 1):
                z_copy(h, z, 8 + h * 3 + i, k).start()

    local[C_GA].wait()
    local[C_GC].wait()
    gateb[0] = sigmoid(dot(hbuf[...], wga[...]).astype(BF16).astype(F32))
    gateb[1] = sigmoid(dot(hbuf[...], wgc[...]).astype(BF16).astype(F32))

    def arrived(h, k):
        row = zpeer(-k)
        z_copy(h, row, 0, 1).wait_recv()

    @pl.when(z >= 2)
    def _():
        for h in (0, 1):
            arrived(h, 2)
            for i, step in enumerate(STEPS):
                @pl.when(z < NZ - step)
                def _():
                    z_copy(h, zpeer(-2), 4 + h * 2 + i, step).start()


    off = offset[c]
    scale = 1.0 / math.sqrt(HD)

    def blocks(k):
        @pl.when(z >= k)
        def _():
            row = zpeer(-k)
            if k not in (0, 2):
                arrived(0, k)
            fronts = []
            for b in range(NX):
                s = dot_nt(qbuf[b * HD : (b + 1) * HD, :], kbuf[row]) * scale + off
                u = jnp.exp(-jnp.abs(s))
                one = 1.0 + u
                tail = jnp.log(one) + (u - (one - 1.0))
                soft = jnp.maximum(s, 0.0) + tail
                logit = s - soft
                if k == 0:
                    rows = lax.broadcasted_iota(jnp.int32, (HD, HD), 0) + b * HD
                    cols = lax.broadcasted_iota(jnp.int32, (HD, HD), 1) + x * HD
                    soft = jnp.where(cols < rows, soft, 0.0)
                    logit = jnp.where(cols < rows, logit, -jnp.inf)
                top = soft.astype(BF16)
                rest = (soft - top.astype(F32)).astype(BF16)
                fronts.append((logit, jnp.concatenate([top, rest], axis=1)))
            sums = [dot(pair, tri[...]) for _, pair in fronts]
            ones = jnp.ones((NZ, 2 * HD), BF16)
            here = lax.broadcasted_iota(jnp.int32, (NZ, HD), 0) == row
            for b, (_, pair) in enumerate(fronts):
                cols = slice(b * HD, (b + 1) * HD)
                tbl[:, cols] = jnp.where(here, dot_nt(ones, pair), tbl[:, cols])
            sticks = [jnp.exp(f[0] - t).astype(BF16) for f, t in zip(fronts, sums)]
            if k not in (0, 2):
                arrived(1, k)
            for b, stick in enumerate(sticks):
                obuf[row, b] = dot(stick, vbuf[row])

    @pl.when(has_halo)
    def _():
        rc(gst, halo, halo_s, halo_r, halo_to).wait_recv()
        gbuf[0:32, :] = halo[...].astype(F32)

    @pl.when(jnp.logical_not(has_halo))
    def _():
        gbuf[0:32, :] = jnp.zeros((32, 256), F32)

    for copy in small[2:]:
        copy.wait()
    conv = jnp.broadcast_to(bias[...], (64, 256))
    for i in range(WIDTH):
        conv = conv + taps[i : i + 1, :] * gbuf[2 + i : 66 + i, :]
    local_mean = jnp.mean(conv, axis=1, keepdims=True)
    dev_local = conv - local_mean
    local_m2 = jnp.sum(dev_local * dev_local, axis=1, keepdims=True)
    lane = lax.broadcasted_iota(jnp.int32, (64, HD), 1)
    stx[...] = jnp.where(lane < 64, local_mean, local_m2)
    for d in (1, 3, 2):
        start(rc(stx, srx.at[y], st_s.at[d], st_r.at[y], dev(yy=ypeer(d))))
    convb[...] = conv

    for d in (1, 3, 2):
        yy = ypeer(d)
        cols = pl.ds(pl.multiple_of(yy * 512, 512), 512)
        start(rc(w_ao.at[half, cols], wo.at[whalf(y, c), :], w_s.at[d], w_r.at[y], dev(yy=yy)))

    for d in range(NX):
        for cc in (c, oc):
            if d == 0 and cc is c:
                continue
            got = qbuf.at[qrows(xpeer(d), cc), :]
            rc(got, got, q_s.at[0], q_r.at[xpeer(d) * 2 + cc], partner).wait_recv()

    blocks(0)
    blocks(1)
    blocks(2)
    blocks(7)
    blocks(6)
    blocks(5)

    srx[y] = stx[...]
    for d in (1, 3, 2):
        yy = ypeer(d)
        rc(stx, srx.at[yy], st_s.at[d], st_r.at[yy], dev(yy=yy)).wait_recv()
    stats = [srx[i] for i in range(NY)]
    means = [t[:, 0:1] for t in stats]
    mean = (means[0] + means[1] + means[2] + means[3]) * 0.25
    m2 = stats[0][:, 64:65] + stats[1][:, 64:65] + stats[2][:, 64:65] + stats[3][:, 64:65]
    for t in means:
        m2 = m2 + 256.0 * (t - mean) * (t - mean)
    cn = (convb[...] - mean) * lax.rsqrt(m2 / CONV_CH + EPS) * ngain[...] + nshift[...]
    cn = (cn * sigmoid(cn)).astype(BF16)
    local[C_CO].wait()
    for i in range(NY):
        cst[i] = dot(cn, wco[:, i * 512 : (i + 1) * 512]).astype(BF16)
    for d in (1, 3, 2):
        yy = ypeer(d)
        start(rc(cst.at[yy], crx.at[y], c_s.at[d], c_r.at[y], dev(yy=yy)))

    blocks(3)
    blocks(4)
    for d in (1, 3, 2):
        start(rc(tbl, tblr.at[x], t_s.at[d], t_r.at[x], dev(xx=xpeer(d))))
    tblr[x] = tbl[...]

    for d in (1, 3, 2):
        yy = ypeer(d)
        got = wo.at[whalf(yy, c), :]
        rc(got, got, w_s.at[d], w_r.at[yy], dev(yy=yy)).wait_recv()
        start(rc(got, got, v_s.at[d], v_r.at[yy], partner))

    for d in (1, 3, 2):
        xx = xpeer(d)
        rc(tbl, tblr.at[xx], t_s.at[d], t_r.at[xx], dev(xx=xx)).wait_recv()

    totals = [tblr[i] for i in range(NX)]
    row_sum = totals[0] + totals[1] + totals[2] + totals[3]
    at = lax.broadcasted_iota(jnp.int32, (NZ, NX * HD), 0)
    outside = jnp.zeros((NZ, NX * HD), F32)
    for j in range(1, NZ):
        outside = outside + jnp.where(at < j, row_sum[j : j + 1, :], 0.0)
    for i in range(1, NX):
        outside = outside + jnp.where(x < i, 1.0, 0.0) * totals[i]
    weight = jnp.exp(-outside)
    for b in range(NX):
        wbuf[b] = weight[:, b * HD : (b + 1) * HD]
    for d in (1, 3, 2, 0):
        b = xpeer(d)
        per_row = jnp.concatenate([wbuf[b], jnp.zeros((HD - NZ, HD), F32)], axis=0).T
        acc = obuf[0, b] * per_row[:, 0:1]
        for j in range(1, NZ):
            acc = acc + obuf[j, b] * per_row[:, j : j + 1]
        if d > 0:
            ps[d] = acc.astype(BF16)
            start(rc(ps.at[d], pr.at[x], o_s.at[d], o_r.at[x], dev(xx=b)))


    csum = cst[y].astype(F32)
    for d in (1, 3, 2):
        yy = ypeer(d)
        rc(cst.at[yy], crx.at[yy], c_s.at[d], c_r.at[yy], dev(yy=yy)).wait_recv()
        csum = csum + crx[yy].astype(F32)
    gateb[1] = gateb[1] * csum.astype(BF16).astype(F32)

    for d in (1, 3, 2):
        xx = xpeer(d)
        rc(ps.at[d], pr.at[xx], o_s.at[d], o_r.at[xx], dev(xx=xx)).wait_recv()
        acc = acc + pr[xx].astype(F32)
    att[...] = acc.astype(BF16)

    head = pl.ds(pl.multiple_of((y * 2 + c) * HD, HD), HD)
    n = 0
    for d in (0, 1, 3, 2):
        for cc, rows in ((c, my64), (oc, oth64)):
            if d == 0 and cc is c:
                continue
            start(rc(att.at[rows, :], abuf.at[:, head], a_s.at[n], a_r.at[y * 2 + c], dev(cc=cc, yy=ypeer(d))))
            n += 1
    abuf[:, head] = att[my64, :]
    local[C_AO].wait()
    for d in (1, 3, 2):
        yy = ypeer(d)
        came = wo.at[whalf(yy, oc), :]
        rc(came, came, v_s.at[d], v_r.at[yy], partner).wait_recv()
    for d in (0, 1, 3, 2):
        for cc in (c, oc):
            if d == 0 and cc is c:
                continue
            yy = ypeer(d)
            h = yy * 2 + cc
            cols = pl.ds(pl.multiple_of(h * HD, HD), HD)
            rc(att.at[my64, :], abuf.at[:, cols], a_s.at[0], a_r.at[h], dev(cc=oc, yy=yy)).wait_recv()
    branch = dot(abuf[...], wo[...]).astype(BF16).astype(F32)
    merged = gateb[0] * branch + gateb[1]
    sq = merged * merged
    part = sq[:, 0:128] + sq[:, 128:256] + sq[:, 256:384] + sq[:, 384:512]
    part = jnp.concatenate([part, jnp.zeros((64, HD), F32)], axis=0).T
    ssx[...] = jnp.sum(part.reshape(16, 8, HD), axis=0)
    for d in (1, 3, 2):
        start(rc(ssx, ssr.at[y], ss_s.at[d], ss_r.at[y], dev(yy=ypeer(d))))
    total = ssx[...]
    for d in (1, 3, 2):
        yy = ypeer(d)
        rc(ssx, ssr.at[yy], ss_s.at[d], ss_r.at[yy], dev(yy=yy)).wait_recv()
        total = total + ssr[yy]
    total = jnp.broadcast_to(jnp.sum(total, axis=0, keepdims=True), (HD, HD)).T[:64, 0:1]
    out[...] = (merged * lax.rsqrt(total / D + EPS) * post_gain[...]).astype(BF16)

    for copy in sends:
        copy.wait_send()
    for h in (0, 1):
        for i, step in enumerate(STEPS):
            @pl.when(z < NZ - step)
            def _():
                z_copy(h, z, h * 2 + i, step).wait_send()

            @pl.when((z >= 2) & (z < NZ - step))
            def _():
                z_copy(h, zpeer(-2), 4 + h * 2 + i, step).wait_send()

        for i, k in enumerate(WRAPS):
            @pl.when(z + k < NZ)
            def _():
                z_copy(h, z, 8 + h * 3 + i, k).wait_send()

    @pl.when(sends_halo)
    def _():
        rc(gst, halo, halo_s, halo_r, halo_to).wait_send()


def on_device(
    hidden_in, pre_gain, w_query, w_key, w_value, stick_offset, w_glu_a, w_glu_b, w_gate_attn,
    w_gate_conv, conv_taps, conv_bias, norm_gain, norm_shift, w_attn_out, w_conv_out, post_gain,
):
    vm = pl.BlockSpec(memory_space=pltpu.VMEM)
    hb = pl.BlockSpec(memory_space=pl.ANY)
    sm = pl.BlockSpec(memory_space=pltpu.SMEM)
    dma = pltpu.SemaphoreType.DMA
    return pl.pallas_call(
        kernel,
        out_shape=jax.ShapeDtypeStruct((64, 512), BF16),
        in_specs=[hb] * 5 + [sm] + [hb] * 11,
        out_specs=vm,
        scratch_shapes=[
            pltpu.VMEM((16, D), BF16),
            pltpu.VMEM((1, D), F32),
            pltpu.VMEM((WIDTH, 256), F32),
            pltpu.VMEM((1, 256), F32),
            pltpu.VMEM((1, 256), F32),
            pltpu.VMEM((1, 256), F32),
            pltpu.VMEM((1, 512), F32),
            pltpu.VMEM((64, D), BF16),
            pltpu.VMEM((D, 256), BF16),
            pltpu.VMEM((D, 256), BF16),
            pltpu.VMEM((D, 256), BF16),
            pltpu.VMEM((D, 256), BF16),
            pltpu.VMEM((D, 256), BF16),
            pltpu.VMEM((D, 512), BF16),
            pltpu.VMEM((D, 512), BF16),
            pltpu.VMEM((256, D), BF16),
            pltpu.VMEM((1024, 512), BF16),
            pltpu.VMEM((NZ, 128, 128), BF16),
            pltpu.VMEM((NZ, 128, 128), BF16),
            pltpu.VMEM((64, 128), BF16),
            pltpu.VMEM((64, 128), BF16),
            pltpu.VMEM((NX * 128, 128), BF16),
            pltpu.VMEM((64, 128), BF16),
            pltpu.VMEM((NZ, NX, 128, 128), F32),
            pltpu.VMEM((NZ, NX * 128), F32),
            pltpu.VMEM((NX, NZ, NX * 128), F32),
            pltpu.VMEM((NX, NZ, 128), F32),
            pltpu.VMEM((NX, 128, 128), BF16),
            pltpu.VMEM((NX, 128, 128), BF16),
            pltpu.VMEM((256, 128), BF16),
            pltpu.VMEM((32, 256), BF16),
            pltpu.VMEM((32, 256), BF16),
            pltpu.VMEM((96, 256), F32),
            pltpu.VMEM((NY, 64, 512), BF16),
            pltpu.VMEM((NY, 64, 512), BF16),
            pltpu.VMEM((64, 128), F32),
            pltpu.VMEM((NY, 64, 128), F32),
            pltpu.VMEM((64, 256), F32),
            pltpu.VMEM((2, 64, 512), F32),
            pltpu.VMEM((128, 128), BF16),
            pltpu.VMEM((64, 1024), BF16),
            pltpu.VMEM((8, 128), F32),
            pltpu.VMEM((NY, 8, 128), F32),
            dma((12,)), dma((7,)),
            dma((4,)), dma((4,)),
            dma((2,)), dma((2,)),
            dma((14,)), dma((16,)),
            dma((7,)), dma((8,)),
            dma((4,)), dma((4,)),
            dma((4,)), dma((4,)),
            pltpu.SemaphoreType.REGULAR((8,)),
            dma, dma,
            dma((4,)), dma((4,)), dma((4,)), dma((4,)),
            dma((4,)), dma((4,)),
            dma((4,)), dma((4,)),
            dma((7,)), dma((8,)),
            dma((4,)), dma((4,)),
        ],
        compiler_params=pltpu.CompilerParams(
            collective_id=0, has_side_effects=True, vmem_limit_bytes=56 * 1024 * 1024
        ),
    )(
        hidden_in, pre_gain.reshape(1, -1), w_query, w_key, w_value, stick_offset, w_glu_a,
        w_glu_b, w_gate_attn, w_gate_conv, conv_taps, conv_bias.reshape(1, -1),
        norm_gain.reshape(1, -1), norm_shift.reshape(1, -1), w_attn_out, w_conv_out,
        post_gain.reshape(1, -1),
    )


def solution(mesh):
    torus = Mesh(mesh.devices.reshape(NZ, NX, 2, NY), ("z", "x", "c", "y"))
    every = ("z", "x", "c", "y")
    cols = P(None, "y")
    return jax.shard_map(
        on_device,
        mesh=torus,
        in_specs=(
            P(every, None), P(), cols, cols, cols, P("y"), cols, cols, cols, cols, cols,
            P("y"), P("y"), P("y"), P("y", None), P("y", None), P("y"),
        ),
        out_specs=P(("z", "x", "c"), "y"),
        check_vma=False,
    )
```

```python
import functools
import math

import jax
import jax.numpy as jnp
from jax import lax
from jax.experimental import pallas as pl
from jax.experimental.pallas import tpu as pltpu
from jax.sharding import Mesh
from jax.sharding import PartitionSpec as P

D = 2048
HD = 128
CONV_CH = 1024
WIDTH = 31
EPS = 1e-06
MESH = pl.DeviceIdType.MESH
F32 = jnp.float32
BF16 = jnp.bfloat16
NX = 4
NZ = 8
NY = 4
NCHIP = NX * NZ


STEPS = (2, 1)
WRAPS = (7, 6, 5)
GREETED = STEPS + WRAPS


def dot(a, b):
    return jnp.dot(a, b, preferred_element_type=F32)


def dot_nt(a, b):
    return lax.dot_general(a, b, (((1,), (1,)), ((), ())), preferred_element_type=F32)


def sigmoid(v):
    return jax.nn.sigmoid(v)


(C_K0, C_K1, C_V0, C_V1, C_Q0, C_Q1, C_A, C_B, C_GA, C_GC, C_CO, C_AO) = range(12)


def kernel(
    hidden_hbm, pre_gain_hbm, w_query, w_key, w_value, offset_hbm, w_a, w_b, w_ga, w_gc,
    taps_hbm, bias_hbm, ngain_hbm, nshift_hbm, w_ao, w_co, post_gain_hbm,
    out_hbm,
    out, offset, hidden, pre_gain, taps, bias, ngain, nshift, post_gain, hbuf, wk, wv, wq, wa, wb, wga, wgc, wco, wo,
    kbuf, vbuf, kst, vst, qbuf, qst, obuf, tbl, tblr, wbuf, ps, pr, tri,
    gst, halo, gbuf, cst, crx, stx, srx, convb, gateb, att, abuf, ssx, ssr,
    lsem, ssem, h_s, h_r, p_s, p_r, z_s, z_r, q_s, q_r, t_s, t_r, o_s, o_r, ready, halo_s, halo_r,
    w_s, w_r, v_s, v_r, st_s, st_r, c_s, c_r, a_s, a_r, ss_s, ss_r,
):
    z = lax.axis_index("z")
    x = lax.axis_index("x")
    c = lax.axis_index("c")
    y = lax.axis_index("y")
    chip = z * NX + x
    oc = 1 - c

    def dev(zz=z, xx=x, cc=c, yy=y):
        return (zz, xx, cc, yy)

    def ypeer(d):
        return lax.rem(y + d, NY)

    def xpeer(d):
        return lax.rem(x + d, NX)

    def zpeer(d):
        return lax.rem(z + d + NZ, NZ)

    def rc(src, dst, ss, rs, to):
        return pltpu.make_async_remote_copy(
            src_ref=src, dst_ref=dst, send_sem=ss, recv_sem=rs, device_id=to, device_id_type=MESH
        )

    half = pl.ds(pl.multiple_of(c * HD, HD), HD)

    def whalf(yy, cc):
        return pl.ds(pl.multiple_of(yy * 256 + cc * HD, HD), HD)

    sends = []

    def start(copy):
        copy.start()
        sends.append(copy)

    own_cols = pl.ds(pl.multiple_of(c * HD, HD), HD)
    oth_cols = pl.ds(pl.multiple_of(oc * HD, HD), HD)
    lo, hi = pl.ds(0, HD), pl.ds(HD, HD)
    ycols = pl.ds(pl.multiple_of(y * 512, 512), 512)
    yrows = pl.ds(pl.multiple_of(y * 256, 256), 256)
    local = {
        C_K1: (w_key.at[:, oth_cols], wk.at[:, lo]),
        C_K0: (w_key.at[:, own_cols], wk.at[:, hi]),
        C_V1: (w_value.at[:, oth_cols], wv.at[:, lo]),
        C_V0: (w_value.at[:, own_cols], wv.at[:, hi]),
        C_Q1: (w_query.at[:, oth_cols], wq.at[:, hi]),
        C_Q0: (w_query.at[:, own_cols], wq.at[:, lo]),
        C_A: (w_a, wa),
        C_B: (w_b, wb),
        C_GA: (w_ga, wga),
        C_GC: (w_gc, wgc),
        C_CO: (w_co, wco),
        C_AO: (w_ao.at[:, ycols], wo.at[yrows, :]),
    }
    local = {k: pltpu.make_async_copy(s, d, lsem.at[k]) for k, (s, d) in local.items()}
    first_in = [(hidden_hbm, hidden), (pre_gain_hbm, pre_gain)]
    later_in = [
        (taps_hbm, taps), (bias_hbm, bias), (ngain_hbm, ngain), (nshift_hbm, nshift), (post_gain_hbm, post_gain),
        (offset_hbm, offset),
    ]
    small = [
        pltpu.make_async_copy(a, b, ssem.at[i]) for i, (a, b) in enumerate(first_in + later_in)
    ]
    for copy in small[:2]:
        copy.start()

    barrier = pltpu.get_barrier_semaphore()
    next_chip = lax.rem(chip + 1, NCHIP)
    prev_chip = lax.rem(chip + NCHIP - 1, NCHIP)
    pair_chip = c * next_chip + oc * prev_chip
    pz, px = pair_chip // NX, lax.rem(pair_chip, NX)
    greet = [dev(yy=ypeer(d)) for d in (1, 2, 3)]
    greet += [dev(cc=oc, yy=ypeer(d)) for d in (0, 1, 2, 3)]
    greet += [dev(xx=xpeer(d), cc=cc) for d in (1, 2, 3) for cc in (c, oc)]
    for peer in greet:
        pl.semaphore_signal(barrier, inc=1, device_id=peer, device_id_type=MESH)
    greeted = len(greet)
    for k in GREETED:
        @pl.when(z + k < NZ)
        def _():
            pl.semaphore_signal(barrier, inc=1, device_id=dev(zz=zpeer(k)), device_id_type=MESH)

        greeted = greeted + jnp.where(z >= k, 1, 0)
    next_core = (pz, px, oc, y)
    has_next = (c == 1) & (chip < NCHIP - 1)
    has_prev = (c == 0) & (chip > 0)

    @pl.when(has_next)
    def _():
        pl.semaphore_signal(barrier, inc=1, device_id=next_core, device_id_type=MESH)

    greeted = greeted + jnp.where(has_prev, 1, 0)

    for copy in small[:2]:
        copy.wait()

    hv = hidden[...].astype(F32)
    inv = lax.rsqrt(jnp.mean(hv * hv, axis=1, keepdims=True) + EPS)
    my16 = pl.ds(pl.multiple_of(y * 16, 16), 16)
    hbuf[my16, :] = (hv * inv * pre_gain[...]).astype(BF16)

    pl.semaphore_wait(barrier, greeted)
    for k in GREETED:
        @pl.when(z >= k)
        def _():
            pl.semaphore_signal(ready.at[k], inc=1, device_id=dev(zz=zpeer(-k)), device_id_type=MESH)

    @pl.when(has_prev)
    def _():
        pl.semaphore_signal(ready.at[0], inc=1, device_id=next_core, device_id_type=MESH)


    for d in (2, 1, 3):
        start(rc(hbuf.at[my16, :], hbuf.at[my16, :], h_s.at[d], h_r.at[y], dev(yy=ypeer(d))))
    for copy in local.values():
        copy.start()
    for copy in small[2:]:
        copy.start()

    r2 = lax.broadcasted_iota(jnp.int32, (2 * HD, HD), 0) % HD
    c2 = lax.broadcasted_iota(jnp.int32, (2 * HD, HD), 1)
    tri[...] = jnp.where(r2 > c2, 1.0, 0.0).astype(BF16)
    obuf[...] = jnp.zeros(obuf.shape, F32)
    tbl[...] = jnp.zeros(tbl.shape, F32)
    for d in (2, 1, 3):
        yy = ypeer(d)
        rows = pl.ds(pl.multiple_of(yy * 16, 16), 16)
        rc(hbuf.at[rows, :], hbuf.at[rows, :], h_s.at[d], h_r.at[yy], dev(yy=yy)).wait_recv()

    my64 = pl.ds(pl.multiple_of(c * 64, 64), 64)
    oth64 = pl.ds(pl.multiple_of(oc * 64, 64), 64)
    partner = dev(cc=oc)
    tables = (kbuf, vbuf)
    for h, (w, st, copies) in enumerate(((wk, kst, (C_K1, C_K0)), (wv, vst, (C_V1, C_V0)))):
        for name in copies:
            local[name].wait()
        both = dot(hbuf[...], w[...]).astype(BF16)
        st[...] = both[:, :HD]
        start(rc(st, tables[h].at[z, my64, :], p_s.at[h], p_r.at[h], partner))
        tables[h][z, my64, :] = both[:, HD:]

    def z_copy(h, row, i, step):
        t = tables[h].at[row]
        return rc(t, t, z_s.at[i], z_r.at[h * NZ + row], dev(zz=zpeer(step)))

    for h in (0, 1):
        rc(kst, tables[h].at[z, oth64, :], p_s.at[h], p_r.at[h], partner).wait_recv()
        for i, step in enumerate(STEPS):
            @pl.when(z < NZ - step)
            def _():
                if h == 0:
                    pl.semaphore_wait(ready.at[step], 1)
                z_copy(h, z, h * 2 + i, step).start()

    local[C_Q0].wait()
    local[C_Q1].wait()
    qv = dot(hbuf[...], wq[...]).astype(BF16)
    qst[...] = qv[:, HD:]

    def qrows(xx, cc):
        return pl.ds(pl.multiple_of(xx * HD + cc * 64, 64), 64)

    mine = qbuf.at[qrows(x, c), :]
    qbuf[qrows(x, c), :] = qv[:, :HD]
    for d in range(NX):
        start(rc(qst, mine, q_s.at[d], q_r.at[x * 2 + c], dev(xx=xpeer(d), cc=oc)))
        if d > 0:
            start(rc(mine, mine, q_s.at[3 + d], q_r.at[x * 2 + c], dev(xx=xpeer(d))))

    local[C_A].wait()
    local[C_B].wait()
    left = dot(hbuf[...], wa[...]).astype(BF16).astype(F32)
    right = dot(hbuf[...], wb[...]).astype(BF16).astype(F32)
    gated = (left * sigmoid(right)).astype(BF16)
    gst[...] = gated[32:, :]
    gbuf[32:, :] = gated.astype(F32)
    halo_to = ((next_chip // NX) * c + z * oc, lax.rem(next_chip, NX) * c + x * oc, oc, y)

    @pl.when(has_next)
    def _():
        pl.semaphore_wait(ready.at[0], 1)

    has_halo = (c == 1) | (chip > 0)
    sends_halo = (c == 0) | (chip < NCHIP - 1)

    @pl.when(sends_halo)
    def _():
        rc(gst, halo, halo_s, halo_r, halo_to).start()

    def send_shard(d):
        yy = ypeer(d)
        cols = pl.ds(pl.multiple_of(yy * 512, 512), 512)
        start(rc(w_ao.at[half, cols], wo.at[whalf(y, c), :], w_s.at[d], w_r.at[y], dev(yy=yy)))

    send_shard(1)
    send_shard(3)
    for i, k in enumerate(WRAPS):
        @pl.when(z + k < NZ)
        def _():
            pl.semaphore_wait(ready.at[k], 1)
            for h in (0, 1):
                z_copy(h, z, 8 + h * 3 + i, k).start()

    def arrived(h, k):
        row = zpeer(-k)
        z_copy(h, row, 0, 1).wait_recv()

    def relay(h):
        @pl.when((z >= 2) & (z < NZ - 1))
        def _():
            arrived(h, 2)
            for i, step in enumerate(STEPS):
                @pl.when(z < NZ - step)
                def _():
                    z_copy(h, zpeer(-2), 4 + h * 2 + i, step).start()

    relay(0)
    small[7].wait()
    off = offset[c]
    scale = 1.0 / math.sqrt(HD)

    def some_blocks(ks):
        def come(h, k):
            if k == 2:
                pl.when(z == NZ - 1)(functools.partial(arrived, h, k))
            elif k > 0:
                arrived(h, k)

        for k in ks:
            come(0, k)
        fronts = []
        for k in ks:
            row = zpeer(-k)
            for b in range(NX):
                s = dot_nt(qbuf[b * HD : (b + 1) * HD, :], kbuf[row]) * scale + off
                u = jnp.exp(-jnp.abs(s))
                one = 1.0 + u
                tail = jnp.log(one) + (u - (one - 1.0))
                soft = jnp.maximum(s, 0.0) + tail
                logit = s - soft
                if k == 0:
                    rows = lax.broadcasted_iota(jnp.int32, (HD, HD), 0) + b * HD
                    cols = lax.broadcasted_iota(jnp.int32, (HD, HD), 1) + x * HD
                    soft = jnp.where(cols < rows, soft, 0.0)
                    logit = jnp.where(cols < rows, logit, -jnp.inf)
                top = soft.astype(BF16)
                rest = (soft - top.astype(F32)).astype(BF16)
                fronts.append((k, row, b, logit, jnp.concatenate([top, rest], axis=1)))
        sums = [dot(f[4], tri[...]) for f in fronts]
        ones = jnp.ones((NZ, 2 * HD), BF16)
        for k, row, b, _, pair in fronts:
            here = lax.broadcasted_iota(jnp.int32, (NZ, HD), 0) == row
            cols = slice(b * HD, (b + 1) * HD)
            tbl[:, cols] = jnp.where(here, dot_nt(ones, pair), tbl[:, cols])
        sticks = [jnp.exp(f[3] - t).astype(BF16) for f, t in zip(fronts, sums)]
        for k in ks:
            come(1, k)
        for (k, row, b, _, _), stick in zip(fronts, sticks):
            obuf[row, b] = dot(stick, vbuf[row])

    def blocks(low, high):
        pl.when(z >= high)(functools.partial(some_blocks, (low, high)))
        pl.when((z >= low) & (z < high))(functools.partial(some_blocks, (low,)))

    @pl.when(has_halo)
    def _():
        rc(gst, halo, halo_s, halo_r, halo_to).wait_recv()
        gbuf[0:32, :] = halo[...].astype(F32)

    @pl.when(jnp.logical_not(has_halo))
    def _():
        gbuf[0:32, :] = jnp.zeros((32, 256), F32)

    for copy in small[2:7]:
        copy.wait()
    conv = jnp.broadcast_to(bias[...], (64, 256))
    for i in range(WIDTH):
        conv = conv + taps[i : i + 1, :] * gbuf[2 + i : 66 + i, :]
    local_mean = jnp.mean(conv, axis=1, keepdims=True)
    dev_local = conv - local_mean
    local_m2 = jnp.sum(dev_local * dev_local, axis=1, keepdims=True)
    lane = lax.broadcasted_iota(jnp.int32, (64, HD), 1)
    stx[...] = jnp.where(lane < 64, local_mean, local_m2)
    for d in (2, 1, 3):
        start(rc(stx, srx.at[y], st_s.at[d], st_r.at[y], dev(yy=ypeer(d))))
    convb[...] = conv

    send_shard(2)
    relay(1)
    for d in range(NX):
        for cc in (c, oc):
            if d == 0 and cc is c:
                continue
            got = qbuf.at[qrows(xpeer(d), cc), :]
            rc(got, got, q_s.at[0], q_r.at[xpeer(d) * 2 + cc], partner).wait_recv()

    blocks(0, 1)
    blocks(2, 7)
    blocks(5, 6)
    blocks(3, 4)
    for d in (2, 1, 3):
        start(rc(tbl, tblr.at[x], t_s.at[d], t_r.at[x], dev(xx=xpeer(d))))
    tblr[x] = tbl[...]

    local[C_GA].wait()
    local[C_GC].wait()
    gateb[0] = sigmoid(dot(hbuf[...], wga[...]).astype(BF16).astype(F32))
    gateb[1] = sigmoid(dot(hbuf[...], wgc[...]).astype(BF16).astype(F32))

    srx[y] = stx[...]
    for d in (2, 1, 3):
        yy = ypeer(d)
        rc(stx, srx.at[yy], st_s.at[d], st_r.at[yy], dev(yy=yy)).wait_recv()
    stats = [srx[i] for i in range(NY)]
    means = [t[:, 0:1] for t in stats]
    mean = (means[0] + means[1] + means[2] + means[3]) * 0.25
    m2 = stats[0][:, 64:65] + stats[1][:, 64:65] + stats[2][:, 64:65] + stats[3][:, 64:65]
    for t in means:
        m2 = m2 + 256.0 * (t - mean) * (t - mean)
    cn = (convb[...] - mean) * lax.rsqrt(m2 / CONV_CH + EPS) * ngain[...] + nshift[...]
    cn = (cn * sigmoid(cn)).astype(BF16)
    local[C_CO].wait()
    for i in range(NY):
        cst[i] = dot(cn, wco[:, i * 512 : (i + 1) * 512]).astype(BF16)
    for d in (2, 1, 3):
        yy = ypeer(d)
        start(rc(cst.at[yy], crx.at[y], c_s.at[d], c_r.at[y], dev(yy=yy)))

    for d in (2, 1, 3):
        xx = xpeer(d)
        rc(tbl, tblr.at[xx], t_s.at[d], t_r.at[xx], dev(xx=xx)).wait_recv()

    totals = [tblr[i] for i in range(NX)]
    row_sum = totals[0] + totals[1] + totals[2] + totals[3]
    at = lax.broadcasted_iota(jnp.int32, (NZ, NX * HD), 0)
    outside = jnp.zeros((NZ, NX * HD), F32)
    for j in range(1, NZ):
        outside = outside + jnp.where(at < j, row_sum[j : j + 1, :], 0.0)
    for i in range(1, NX):
        outside = outside + jnp.where(x < i, 1.0, 0.0) * totals[i]
    weight = jnp.exp(-outside)
    per_row = jnp.concatenate([weight, jnp.zeros((HD - NZ, NX * HD), F32)], axis=0).T
    for b in range(NX):
        wbuf[b] = per_row[b * HD : (b + 1) * HD, :]
    for d in (2, 1, 3, 0):
        b = xpeer(d)
        per_row = wbuf[b]
        acc = obuf[0, b] * per_row[:, 0:1]
        for j in range(1, NZ):
            acc = acc + obuf[j, b] * per_row[:, j : j + 1]
        if d > 0:
            ps[d] = acc.astype(BF16)
            start(rc(ps.at[d], pr.at[x], o_s.at[d], o_r.at[x], dev(xx=b)))

    for d in (2, 1, 3):
        yy = ypeer(d)
        got = wo.at[whalf(yy, c), :]
        rc(got, got, w_s.at[d], w_r.at[yy], dev(yy=yy)).wait_recv()
        start(rc(got, got, v_s.at[d], v_r.at[yy], partner))


    csum = cst[y].astype(F32)
    for d in (2, 1, 3):
        yy = ypeer(d)
        rc(cst.at[yy], crx.at[yy], c_s.at[d], c_r.at[yy], dev(yy=yy)).wait_recv()
        csum = csum + crx[yy].astype(F32)
    gateb[1] = gateb[1] * csum.astype(BF16).astype(F32)

    for d in (2, 1, 3):
        xx = xpeer(d)
        rc(ps.at[d], pr.at[xx], o_s.at[d], o_r.at[xx], dev(xx=xx)).wait_recv()
        acc = acc + pr[xx].astype(F32)
    att[...] = acc.astype(BF16)

    head = pl.ds(pl.multiple_of((y * 2 + c) * HD, HD), HD)
    n = 0
    for d in (2, 1, 3, 0):
        for cc, rows in ((c, my64), (oc, oth64)):
            if d == 0 and cc is c:
                continue
            start(rc(att.at[rows, :], abuf.at[:, head], a_s.at[n], a_r.at[y * 2 + c], dev(cc=cc, yy=ypeer(d))))
            n += 1
    abuf[:, head] = att[my64, :]
    local[C_AO].wait()
    for d in (2, 1, 3):
        yy = ypeer(d)
        came = wo.at[whalf(yy, oc), :]
        rc(came, came, v_s.at[d], v_r.at[yy], partner).wait_recv()
    for d in (2, 1, 3, 0):
        for cc in (c, oc):
            if d == 0 and cc is c:
                continue
            yy = ypeer(d)
            h = yy * 2 + cc
            cols = pl.ds(pl.multiple_of(h * HD, HD), HD)
            rc(att.at[my64, :], abuf.at[:, cols], a_s.at[0], a_r.at[h], dev(cc=oc, yy=yy)).wait_recv()
    branch = dot(abuf[...], wo[...]).astype(BF16).astype(F32)
    merged = gateb[0] * branch + gateb[1]
    sq = merged * merged
    part = sq[:, 0:128] + sq[:, 128:256] + sq[:, 256:384] + sq[:, 384:512]
    part = jnp.concatenate([part, jnp.zeros((64, HD), F32)], axis=0).T
    ssx[...] = jnp.sum(part.reshape(16, 8, HD), axis=0)
    for d in (2, 1, 3):
        start(rc(ssx, ssr.at[y], ss_s.at[d], ss_r.at[y], dev(yy=ypeer(d))))
    total = ssx[...]
    for d in (2, 1, 3):
        yy = ypeer(d)
        rc(ssx, ssr.at[yy], ss_s.at[d], ss_r.at[yy], dev(yy=yy)).wait_recv()
        total = total + ssr[yy]
    total = jnp.broadcast_to(jnp.sum(total, axis=0, keepdims=True), (HD, HD)).T[:64, 0:1]
    out[...] = (merged * lax.rsqrt(total / D + EPS) * post_gain[...]).astype(BF16)

    written = pltpu.make_async_copy(out, out_hbm, ssem.at[8])
    written.start()
    for copy in sends:
        copy.wait_send()
    for h in (0, 1):
        for i, step in enumerate(STEPS):
            @pl.when(z < NZ - step)
            def _():
                z_copy(h, z, h * 2 + i, step).wait_send()

            @pl.when((z >= 2) & (z < NZ - step))
            def _():
                z_copy(h, zpeer(-2), 4 + h * 2 + i, step).wait_send()

        for i, k in enumerate(WRAPS):
            @pl.when(z + k < NZ)
            def _():
                z_copy(h, z, 8 + h * 3 + i, k).wait_send()

    @pl.when(sends_halo)
    def _():
        rc(gst, halo, halo_s, halo_r, halo_to).wait_send()

    written.wait()


def on_device(
    hidden_in, pre_gain, w_query, w_key, w_value, stick_offset, w_glu_a, w_glu_b, w_gate_attn,
    w_gate_conv, conv_taps, conv_bias, norm_gain, norm_shift, w_attn_out, w_conv_out, post_gain,
):
    hb = pl.BlockSpec(memory_space=pl.ANY)
    dma = pltpu.SemaphoreType.DMA
    return pl.pallas_call(
        kernel,
        out_shape=jax.ShapeDtypeStruct((64, 512), BF16),
        in_specs=[hb] * 17,
        out_specs=hb,
        scratch_shapes=[
            pltpu.VMEM((64, 512), BF16),
            pltpu.SMEM((2,), F32),
            pltpu.VMEM((16, D), BF16),
            pltpu.VMEM((1, D), F32),
            pltpu.VMEM((WIDTH, 256), F32),
            pltpu.VMEM((1, 256), F32),
            pltpu.VMEM((1, 256), F32),
            pltpu.VMEM((1, 256), F32),
            pltpu.VMEM((1, 512), F32),
            pltpu.VMEM((64, D), BF16),
            pltpu.VMEM((D, 256), BF16),
            pltpu.VMEM((D, 256), BF16),
            pltpu.VMEM((D, 256), BF16),
            pltpu.VMEM((D, 256), BF16),
            pltpu.VMEM((D, 256), BF16),
            pltpu.VMEM((D, 512), BF16),
            pltpu.VMEM((D, 512), BF16),
            pltpu.VMEM((256, D), BF16),
            pltpu.VMEM((1024, 512), BF16),
            pltpu.VMEM((NZ, 128, 128), BF16),
            pltpu.VMEM((NZ, 128, 128), BF16),
            pltpu.VMEM((64, 128), BF16),
            pltpu.VMEM((64, 128), BF16),
            pltpu.VMEM((NX * 128, 128), BF16),
            pltpu.VMEM((64, 128), BF16),
            pltpu.VMEM((NZ, NX, 128, 128), F32),
            pltpu.VMEM((NZ, NX * 128), F32),
            pltpu.VMEM((NX, NZ, NX * 128), F32),
            pltpu.VMEM((NX, 128, 128), F32),
            pltpu.VMEM((NX, 128, 128), BF16),
            pltpu.VMEM((NX, 128, 128), BF16),
            pltpu.VMEM((256, 128), BF16),
            pltpu.VMEM((32, 256), BF16),
            pltpu.VMEM((32, 256), BF16),
            pltpu.VMEM((96, 256), F32),
            pltpu.VMEM((NY, 64, 512), BF16),
            pltpu.VMEM((NY, 64, 512), BF16),
            pltpu.VMEM((64, 128), F32),
            pltpu.VMEM((NY, 64, 128), F32),
            pltpu.VMEM((64, 256), F32),
            pltpu.VMEM((2, 64, 512), F32),
            pltpu.VMEM((128, 128), BF16),
            pltpu.VMEM((64, 1024), BF16),
            pltpu.VMEM((8, 128), F32),
            pltpu.VMEM((NY, 8, 128), F32),
            dma((12,)), dma((9,)),
            dma((4,)), dma((4,)),
            dma((2,)), dma((2,)),
            dma((14,)), dma((16,)),
            dma((7,)), dma((8,)),
            dma((4,)), dma((4,)),
            dma((4,)), dma((4,)),
            pltpu.SemaphoreType.REGULAR((8,)),
            dma, dma,
            dma((4,)), dma((4,)), dma((4,)), dma((4,)),
            dma((4,)), dma((4,)),
            dma((4,)), dma((4,)),
            dma((7,)), dma((8,)),
            dma((4,)), dma((4,)),
        ],
        compiler_params=pltpu.CompilerParams(
            collective_id=0, has_side_effects=True, vmem_limit_bytes=56 * 1024 * 1024
        ),
    )(
        hidden_in, pre_gain.reshape(1, -1), w_query, w_key, w_value, stick_offset, w_glu_a,
        w_glu_b, w_gate_attn, w_gate_conv, conv_taps, conv_bias.reshape(1, -1),
        norm_gain.reshape(1, -1), norm_shift.reshape(1, -1), w_attn_out, w_conv_out,
        post_gain.reshape(1, -1),
    )


def solution(mesh):
    torus = Mesh(mesh.devices.reshape(NZ, NX, 2, NY), ("z", "x", "c", "y"))
    every = ("z", "x", "c", "y")
    cols = P(None, "y")
    return jax.shard_map(
        on_device,
        mesh=torus,
        in_specs=(
            P(every, None), P(), cols, cols, cols, P("y"), cols, cols, cols, cols, cols,
            P("y"), P("y"), P("y"), P("y", None), P("y", None), P("y"),
        ),
        out_specs=P(("z", "x", "c"), "y"),
        check_vma=False,
    )
```

```python
import functools
import math

import jax
import jax.numpy as jnp
from jax import lax
from jax.experimental import pallas as pl
from jax.experimental.pallas import tpu as pltpu
from jax.sharding import Mesh
from jax.sharding import PartitionSpec as P

D = 2048
HD = 128
CONV_CH = 1024
WIDTH = 31
EPS = 1e-06
MESH = pl.DeviceIdType.MESH
F32 = jnp.float32
BF16 = jnp.bfloat16
NX = 4
NZ = 8
NY = 4
NCHIP = NX * NZ


STEPS = (2, 1)
WRAPS = (7, 6, 5)
GREETED = STEPS + WRAPS


def dot(a, b):
    return jnp.dot(a, b, preferred_element_type=F32)


def dot_nt(a, b):
    return lax.dot_general(a, b, (((1,), (1,)), ((), ())), preferred_element_type=F32)


def sigmoid(v):
    return jax.nn.sigmoid(v)


(C_K0, C_K1, C_V0, C_V1, C_Q0, C_Q1, C_A, C_B, C_GA, C_GC, C_CO, C_AO) = range(12)


def kernel(
    hidden_hbm, pre_gain_hbm, w_query, w_key, w_value, offset_hbm, w_a, w_b, w_ga, w_gc,
    taps_hbm, bias_hbm, ngain_hbm, nshift_hbm, w_ao, w_co, post_gain_hbm,
    out,
    offset, hidden, pre_gain, taps, bias, ngain, nshift, post_gain, hbuf, wk, wv, wq, wa, wb, wga, wgc, wco, wo,
    kbuf, vbuf, kst, vst, qbuf, qst, obuf, tbl, tblr, wbuf, ps, pr, tri,
    gst, halo, gbuf, cst, crx, stx, srx, convb, gateb, att, abuf, ssx, ssr,
    lsem, ssem, h_s, h_r, p_s, p_r, z_s, z_r, q_s, q_r, t_s, t_r, o_s, o_r, ready, halo_s, halo_r,
    w_s, w_r, v_s, v_r, st_s, st_r, c_s, c_r, a_s, a_r, ss_s, ss_r,
):
    z = lax.axis_index("z")
    x = lax.axis_index("x")
    c = lax.axis_index("c")
    y = lax.axis_index("y")
    chip = z * NX + x
    oc = 1 - c

    def dev(zz=z, xx=x, cc=c, yy=y):
        return (zz, xx, cc, yy)

    def ypeer(d):
        return lax.rem(y + d, NY)

    def xpeer(d):
        return lax.rem(x + d, NX)

    def zpeer(d):
        return lax.rem(z + d + NZ, NZ)

    def rc(src, dst, ss, rs, to):
        return pltpu.make_async_remote_copy(
            src_ref=src, dst_ref=dst, send_sem=ss, recv_sem=rs, device_id=to, device_id_type=MESH
        )

    half = pl.ds(pl.multiple_of(c * HD, HD), HD)

    def whalf(yy, cc):
        return pl.ds(pl.multiple_of(yy * 256 + cc * HD, HD), HD)

    sends = []

    def start(copy):
        copy.start()
        sends.append(copy)

    own_cols = pl.ds(pl.multiple_of(c * HD, HD), HD)
    oth_cols = pl.ds(pl.multiple_of(oc * HD, HD), HD)
    lo, hi = pl.ds(0, HD), pl.ds(HD, HD)
    ycols = pl.ds(pl.multiple_of(y * 512, 512), 512)
    yrows = pl.ds(pl.multiple_of(y * 256, 256), 256)
    local = {
        C_K1: (w_key.at[:, oth_cols], wk.at[:, lo]),
        C_K0: (w_key.at[:, own_cols], wk.at[:, hi]),
        C_V1: (w_value.at[:, oth_cols], wv.at[:, lo]),
        C_V0: (w_value.at[:, own_cols], wv.at[:, hi]),
        C_Q1: (w_query.at[:, oth_cols], wq.at[:, hi]),
        C_Q0: (w_query.at[:, own_cols], wq.at[:, lo]),
        C_A: (w_a, wa),
        C_B: (w_b, wb),
        C_GA: (w_ga, wga),
        C_GC: (w_gc, wgc),
        C_CO: (w_co, wco),
        C_AO: (w_ao.at[:, ycols], wo.at[yrows, :]),
    }
    local = {k: pltpu.make_async_copy(s, d, lsem.at[k]) for k, (s, d) in local.items()}
    first_in = [(hidden_hbm, hidden), (pre_gain_hbm, pre_gain)]
    later_in = [
        (taps_hbm, taps), (bias_hbm, bias), (ngain_hbm, ngain), (nshift_hbm, nshift), (post_gain_hbm, post_gain),
        (offset_hbm, offset),
    ]
    small = [
        pltpu.make_async_copy(a, b, ssem.at[i]) for i, (a, b) in enumerate(first_in + later_in)
    ]
    for copy in small[:2]:
        copy.start()

    barrier = pltpu.get_barrier_semaphore()
    next_chip = lax.rem(chip + 1, NCHIP)
    prev_chip = lax.rem(chip + NCHIP - 1, NCHIP)
    pair_chip = c * next_chip + oc * prev_chip
    pz, px = pair_chip // NX, lax.rem(pair_chip, NX)
    greet = [dev(yy=ypeer(d)) for d in (1, 2, 3)]
    greet += [dev(cc=oc, yy=ypeer(d)) for d in (0, 1, 2, 3)]
    greet += [dev(xx=xpeer(d), cc=cc) for d in (1, 2, 3) for cc in (c, oc)]
    for peer in greet:
        pl.semaphore_signal(barrier, inc=1, device_id=peer, device_id_type=MESH)
    greeted = len(greet)
    for k in GREETED:
        @pl.when(z + k < NZ)
        def _():
            for cc in (c, oc) if k in STEPS else (c,):
                pl.semaphore_signal(barrier, inc=1, device_id=dev(zz=zpeer(k), cc=cc), device_id_type=MESH)

        greeted = greeted + jnp.where(z >= k, 2 if k in STEPS else 1, 0)
    next_core = (pz, px, oc, y)
    has_next = (c == 1) & (chip < NCHIP - 1)
    has_prev = (c == 0) & (chip > 0)

    @pl.when(has_next)
    def _():
        pl.semaphore_signal(barrier, inc=1, device_id=next_core, device_id_type=MESH)

    greeted = greeted + jnp.where(has_prev, 1, 0)

    for copy in small[:2]:
        copy.wait()

    hv = hidden[...].astype(F32)
    inv = lax.rsqrt(jnp.mean(hv * hv, axis=1, keepdims=True) + EPS)
    my16 = pl.ds(pl.multiple_of(y * 16, 16), 16)
    hbuf[my16, :] = (hv * inv * pre_gain[...]).astype(BF16)

    pl.semaphore_wait(barrier, greeted)
    for k in GREETED:
        @pl.when(z >= k)
        def _():
            for cc in (c, oc) if k in STEPS else (c,):
                pl.semaphore_signal(ready.at[k], inc=1, device_id=dev(zz=zpeer(-k), cc=cc), device_id_type=MESH)

    @pl.when(has_prev)
    def _():
        pl.semaphore_signal(ready.at[0], inc=1, device_id=next_core, device_id_type=MESH)


    for d in (2, 1, 3):
        start(rc(hbuf.at[my16, :], hbuf.at[my16, :], h_s.at[d], h_r.at[y], dev(yy=ypeer(d))))
    for copy in local.values():
        copy.start()
    for copy in small[2:]:
        copy.start()

    r2 = lax.broadcasted_iota(jnp.int32, (2 * HD, HD), 0) % HD
    c2 = lax.broadcasted_iota(jnp.int32, (2 * HD, HD), 1)
    tri[...] = jnp.where(r2 > c2, 1.0, 0.0).astype(BF16)
    obuf[...] = jnp.zeros(obuf.shape, F32)
    tbl[...] = jnp.zeros(tbl.shape, F32)
    for d in (2, 1, 3):
        yy = ypeer(d)
        rows = pl.ds(pl.multiple_of(yy * 16, 16), 16)
        rc(hbuf.at[rows, :], hbuf.at[rows, :], h_s.at[d], h_r.at[yy], dev(yy=yy)).wait_recv()

    my64 = pl.ds(pl.multiple_of(c * 64, 64), 64)
    oth64 = pl.ds(pl.multiple_of(oc * 64, 64), 64)
    partner = dev(cc=oc)
    tables = (kbuf, vbuf)
    for h, (w, st, copies) in enumerate(((wk, kst, (C_K1, C_K0)), (wv, vst, (C_V1, C_V0)))):
        for name in copies:
            local[name].wait()
        both = dot(hbuf[...], w[...]).astype(BF16)
        st[...] = both[:, :HD]
        start(rc(st, tables[h].at[z, my64, :], p_s.at[h], p_r.at[h], partner))
        tables[h][z, my64, :] = both[:, HD:]

    def z_copy(h, row, i, step):
        t = tables[h].at[row]
        return rc(t, t, z_s.at[i], z_r.at[h * NZ + row], dev(zz=zpeer(step)))

    for i, step in enumerate(STEPS):
        @pl.when(z < NZ - step)
        def _():
            pl.semaphore_wait(ready.at[step], 2)
            for h, st in enumerate((kst, vst)):
                half_own = tables[h].at[z, my64, :]
                there = z_r.at[h * NZ + z]
                rc(half_own, half_own, z_s.at[i], there, dev(zz=zpeer(step))).start()
                rc(st, half_own, z_s.at[i], there, dev(zz=zpeer(step), cc=oc)).start()

    local[C_Q0].wait()
    local[C_Q1].wait()
    qv = dot(hbuf[...], wq[...]).astype(BF16)
    qst[...] = qv[:, HD:]

    def qrows(xx, cc):
        return pl.ds(pl.multiple_of(xx * HD + cc * 64, 64), 64)

    mine = qbuf.at[qrows(x, c), :]
    qbuf[qrows(x, c), :] = qv[:, :HD]
    for d in range(NX):
        start(rc(qst, mine, q_s.at[d], q_r.at[x * 2 + c], dev(xx=xpeer(d), cc=oc)))
        if d > 0:
            start(rc(mine, mine, q_s.at[3 + d], q_r.at[x * 2 + c], dev(xx=xpeer(d))))

    local[C_A].wait()
    local[C_B].wait()
    left = dot(hbuf[...], wa[...]).astype(BF16).astype(F32)
    right = dot(hbuf[...], wb[...]).astype(BF16).astype(F32)
    gated = (left * sigmoid(right)).astype(BF16)
    gst[...] = gated[32:, :]
    gbuf[32:, :] = gated.astype(F32)
    halo_to = ((next_chip // NX) * c + z * oc, lax.rem(next_chip, NX) * c + x * oc, oc, y)

    @pl.when(has_next)
    def _():
        pl.semaphore_wait(ready.at[0], 1)

    has_halo = (c == 1) | (chip > 0)
    sends_halo = (c == 0) | (chip < NCHIP - 1)

    @pl.when(sends_halo)
    def _():
        rc(gst, halo, halo_s, halo_r, halo_to).start()

    def send_shard(d):
        yy = ypeer(d)
        cols = pl.ds(pl.multiple_of(yy * 512, 512), 512)
        start(rc(w_ao.at[half, cols], wo.at[whalf(y, c), :], w_s.at[d], w_r.at[y], dev(yy=yy)))

    send_shard(1)
    send_shard(3)
    for h in (0, 1):
        rc(kst, tables[h].at[z, oth64, :], p_s.at[h], p_r.at[h], partner).wait_recv()

    for i, k in enumerate(WRAPS):
        @pl.when(z + k < NZ)
        def _():
            pl.semaphore_wait(ready.at[k], 1)
            for h in (0, 1):
                z_copy(h, z, 4 + i, k).start()

    def arrived(h, k):
        row = zpeer(-k)
        z_copy(h, row, 0, 1).wait_recv()

    def relay(h):
        @pl.when((z >= 2) & (z < NZ - 1))
        def _():
            arrived(h, 2)
            for i, step in enumerate(STEPS):
                @pl.when(z < NZ - step)
                def _():
                    z_copy(h, zpeer(-2), 2 + i, step).start()

    relay(0)
    small[7].wait()
    off = offset[c]
    scale = 1.0 / math.sqrt(HD)

    def some_blocks(ks):
        def come(h, k):
            if k == 2:
                pl.when(z == NZ - 1)(functools.partial(arrived, h, k))
            elif k > 0:
                arrived(h, k)

        for k in ks:
            come(0, k)
        fronts = []
        for k in ks:
            row = zpeer(-k)
            for b in range(NX):
                s = dot_nt(qbuf[b * HD : (b + 1) * HD, :], kbuf[row]) * scale + off
                u = jnp.exp(-jnp.abs(s))
                one = 1.0 + u
                tail = jnp.log(one) + (u - (one - 1.0))
                soft = jnp.maximum(s, 0.0) + tail
                logit = s - soft
                if k == 0:
                    rows = lax.broadcasted_iota(jnp.int32, (HD, HD), 0) + b * HD
                    cols = lax.broadcasted_iota(jnp.int32, (HD, HD), 1) + x * HD
                    soft = jnp.where(cols < rows, soft, 0.0)
                    logit = jnp.where(cols < rows, logit, -jnp.inf)
                top = soft.astype(BF16)
                rest = (soft - top.astype(F32)).astype(BF16)
                fronts.append((k, row, b, logit, jnp.concatenate([top, rest], axis=1)))
        sums = [dot(f[4], tri[...]) for f in fronts]
        ones = jnp.ones((NZ, 2 * HD), BF16)
        for k, row, b, _, pair in fronts:
            here = lax.broadcasted_iota(jnp.int32, (NZ, HD), 0) == row
            cols = slice(b * HD, (b + 1) * HD)
            tbl[:, cols] = jnp.where(here, dot_nt(ones, pair), tbl[:, cols])
        sticks = [jnp.exp(f[3] - t).astype(BF16) for f, t in zip(fronts, sums)]
        for k in ks:
            come(1, k)
        for (k, row, b, _, _), stick in zip(fronts, sticks):
            obuf[row, b] = dot(stick, vbuf[row])

    def blocks(low, high):
        pl.when(z >= high)(functools.partial(some_blocks, (low, high)))
        pl.when((z >= low) & (z < high))(functools.partial(some_blocks, (low,)))

    @pl.when(has_halo)
    def _():
        rc(gst, halo, halo_s, halo_r, halo_to).wait_recv()
        gbuf[0:32, :] = halo[...].astype(F32)

    @pl.when(jnp.logical_not(has_halo))
    def _():
        gbuf[0:32, :] = jnp.zeros((32, 256), F32)

    for copy in small[2:7]:
        copy.wait()
    conv = jnp.broadcast_to(bias[...], (64, 256))
    for i in range(WIDTH):
        conv = conv + taps[i : i + 1, :] * gbuf[2 + i : 66 + i, :]
    local_mean = jnp.mean(conv, axis=1, keepdims=True)
    dev_local = conv - local_mean
    local_m2 = jnp.sum(dev_local * dev_local, axis=1, keepdims=True)
    lane = lax.broadcasted_iota(jnp.int32, (64, HD), 1)
    stx[...] = jnp.where(lane < 64, local_mean, local_m2)
    for d in (2, 1, 3):
        start(rc(stx, srx.at[y], st_s.at[d], st_r.at[y], dev(yy=ypeer(d))))
    convb[...] = conv

    send_shard(2)
    relay(1)
    for d in range(NX):
        for cc in (c, oc):
            if d == 0 and cc is c:
                continue
            got = qbuf.at[qrows(xpeer(d), cc), :]
            rc(got, got, q_s.at[0], q_r.at[xpeer(d) * 2 + cc], partner).wait_recv()

    blocks(0, 1)
    blocks(2, 7)
    blocks(5, 6)
    blocks(3, 4)
    for d in (2, 1, 3):
        start(rc(tbl, tblr.at[x], t_s.at[d], t_r.at[x], dev(xx=xpeer(d))))
    tblr[x] = tbl[...]

    local[C_GA].wait()
    local[C_GC].wait()
    gateb[0] = sigmoid(dot(hbuf[...], wga[...]).astype(BF16).astype(F32))
    gateb[1] = sigmoid(dot(hbuf[...], wgc[...]).astype(BF16).astype(F32))

    srx[y] = stx[...]
    for d in (2, 1, 3):
        yy = ypeer(d)
        rc(stx, srx.at[yy], st_s.at[d], st_r.at[yy], dev(yy=yy)).wait_recv()
    stats = [srx[i] for i in range(NY)]
    means = [t[:, 0:1] for t in stats]
    mean = (means[0] + means[1] + means[2] + means[3]) * 0.25
    m2 = stats[0][:, 64:65] + stats[1][:, 64:65] + stats[2][:, 64:65] + stats[3][:, 64:65]
    for t in means:
        m2 = m2 + 256.0 * (t - mean) * (t - mean)
    cn = (convb[...] - mean) * lax.rsqrt(m2 / CONV_CH + EPS) * ngain[...] + nshift[...]
    cn = (cn * sigmoid(cn)).astype(BF16)
    local[C_CO].wait()
    for i in range(NY):
        cst[i] = dot(cn, wco[:, i * 512 : (i + 1) * 512]).astype(BF16)
    for d in (2, 1, 3):
        yy = ypeer(d)
        start(rc(cst.at[yy], crx.at[y], c_s.at[d], c_r.at[y], dev(yy=yy)))

    for d in (2, 1, 3):
        xx = xpeer(d)
        rc(tbl, tblr.at[xx], t_s.at[d], t_r.at[xx], dev(xx=xx)).wait_recv()

    totals = [tblr[i] for i in range(NX)]
    row_sum = totals[0] + totals[1] + totals[2] + totals[3]
    at = lax.broadcasted_iota(jnp.int32, (NZ, NX * HD), 0)
    outside = jnp.zeros((NZ, NX * HD), F32)
    for j in range(1, NZ):
        outside = outside + jnp.where(at < j, row_sum[j : j + 1, :], 0.0)
    for i in range(1, NX):
        outside = outside + jnp.where(x < i, 1.0, 0.0) * totals[i]
    weight = jnp.exp(-outside)
    per_row = jnp.concatenate([weight, jnp.zeros((HD - NZ, NX * HD), F32)], axis=0).T
    for b in range(NX):
        wbuf[b] = per_row[b * HD : (b + 1) * HD, :]
    for d in (2, 1, 3, 0):
        b = xpeer(d)
        per_row = wbuf[b]
        acc = obuf[0, b] * per_row[:, 0:1]
        for j in range(1, NZ):
            acc = acc + obuf[j, b] * per_row[:, j : j + 1]
        if d > 0:
            ps[d] = acc.astype(BF16)
            start(rc(ps.at[d], pr.at[x], o_s.at[d], o_r.at[x], dev(xx=b)))

    for d in (2, 1, 3):
        yy = ypeer(d)
        got = wo.at[whalf(yy, c), :]
        rc(got, got, w_s.at[d], w_r.at[yy], dev(yy=yy)).wait_recv()
        start(rc(got, got, v_s.at[d], v_r.at[yy], partner))

    for d in (2, 1, 3):
        xx = xpeer(d)
        rc(ps.at[d], pr.at[xx], o_s.at[d], o_r.at[xx], dev(xx=xx)).wait_recv()
        acc = acc + pr[xx].astype(F32)
    att[...] = acc.astype(BF16)

    head = pl.ds(pl.multiple_of((y * 2 + c) * HD, HD), HD)
    n = 0
    for d in (2, 1, 3, 0):
        for cc, rows in ((c, my64), (oc, oth64)):
            if d == 0 and cc is c:
                continue
            start(rc(att.at[rows, :], abuf.at[:, head], a_s.at[n], a_r.at[y * 2 + c], dev(cc=cc, yy=ypeer(d))))
            n += 1
    abuf[:, head] = att[my64, :]
    local[C_AO].wait()
    for d in (2, 1, 3):
        yy = ypeer(d)
        came = wo.at[whalf(yy, oc), :]
        rc(came, came, v_s.at[d], v_r.at[yy], partner).wait_recv()

    csum = cst[y].astype(F32)
    for d in (2, 1, 3):
        yy = ypeer(d)
        rc(cst.at[yy], crx.at[yy], c_s.at[d], c_r.at[yy], dev(yy=yy)).wait_recv()
        csum = csum + crx[yy].astype(F32)
    gateb[1] = gateb[1] * csum.astype(BF16).astype(F32)

    for d in (2, 1, 3, 0):
        for cc in (c, oc):
            if d == 0 and cc is c:
                continue
            yy = ypeer(d)
            h = yy * 2 + cc
            cols = pl.ds(pl.multiple_of(h * HD, HD), HD)
            rc(att.at[my64, :], abuf.at[:, cols], a_s.at[0], a_r.at[h], dev(cc=oc, yy=yy)).wait_recv()
    branch = dot(abuf[...], wo[...]).astype(BF16).astype(F32)
    merged = gateb[0] * branch + gateb[1]
    sq = merged * merged
    part = sq[:, 0:128] + sq[:, 128:256] + sq[:, 256:384] + sq[:, 384:512]
    part = jnp.concatenate([part, jnp.zeros((64, HD), F32)], axis=0).T
    ssx[...] = jnp.sum(part.reshape(16, 8, HD), axis=0)
    for d in (2, 1, 3):
        start(rc(ssx, ssr.at[y], ss_s.at[d], ss_r.at[y], dev(yy=ypeer(d))))
    total = ssx[...]
    for d in (2, 1, 3):
        yy = ypeer(d)
        rc(ssx, ssr.at[yy], ss_s.at[d], ss_r.at[yy], dev(yy=yy)).wait_recv()
        total = total + ssr[yy]
    total = jnp.broadcast_to(jnp.sum(total, axis=0, keepdims=True), (HD, HD)).T[:64, 0:1]
    out[...] = (merged * lax.rsqrt(total / D + EPS) * post_gain[...]).astype(BF16)

    for copy in sends:
        copy.wait_send()
    def z_sent(i, cond):
        @pl.when(cond)
        def _():
            two = kbuf.at[0:2]
            rc(two, two, z_s.at[i], z_r.at[0], partner).wait_send()

    for i, step in enumerate(STEPS):
        z_sent(i, z < NZ - step)
        z_sent(2 + i, (z >= 2) & (z < NZ - step))
    for i, k in enumerate(WRAPS):
        z_sent(4 + i, z + k < NZ)

    @pl.when(sends_halo)
    def _():
        rc(gst, halo, halo_s, halo_r, halo_to).wait_send()


def on_device(
    hidden_in, pre_gain, w_query, w_key, w_value, stick_offset, w_glu_a, w_glu_b, w_gate_attn,
    w_gate_conv, conv_taps, conv_bias, norm_gain, norm_shift, w_attn_out, w_conv_out, post_gain,
):
    args = (
        hidden_in, pre_gain.reshape(1, -1), w_query, w_key, w_value, stick_offset, w_glu_a,
        w_glu_b, w_gate_attn, w_gate_conv, conv_taps, conv_bias.reshape(1, -1),
        norm_gain.reshape(1, -1), norm_shift.reshape(1, -1), w_attn_out, w_conv_out,
        post_gain.reshape(1, -1),
    )
    hb = pl.BlockSpec(memory_space=pl.ANY)
    dma = pltpu.SemaphoreType.DMA
    return pl.pallas_call(
        kernel,
        out_shape=jax.ShapeDtypeStruct((64, 512), BF16),
        in_specs=[hb] * 17,
        out_specs=pl.BlockSpec(memory_space=pltpu.VMEM),
        scratch_shapes=[
            pltpu.SMEM((2,), F32),
            pltpu.VMEM((16, D), BF16),
            pltpu.VMEM((1, D), F32),
            pltpu.VMEM((WIDTH, 256), F32),
            pltpu.VMEM((1, 256), F32),
            pltpu.VMEM((1, 256), F32),
            pltpu.VMEM((1, 256), F32),
            pltpu.VMEM((1, 512), F32),
            pltpu.VMEM((64, D), BF16),
            pltpu.VMEM((D, 256), BF16),
            pltpu.VMEM((D, 256), BF16),
            pltpu.VMEM((D, 256), BF16),
            pltpu.VMEM((D, 256), BF16),
            pltpu.VMEM((D, 256), BF16),
            pltpu.VMEM((D, 512), BF16),
            pltpu.VMEM((D, 512), BF16),
            pltpu.VMEM((256, D), BF16),
            pltpu.VMEM((1024, 512), BF16),
            pltpu.VMEM((NZ, 128, 128), BF16),
            pltpu.VMEM((NZ, 128, 128), BF16),
            pltpu.VMEM((64, 128), BF16),
            pltpu.VMEM((64, 128), BF16),
            pltpu.VMEM((NX * 128, 128), BF16),
            pltpu.VMEM((64, 128), BF16),
            pltpu.VMEM((NZ, NX, 128, 128), F32),
            pltpu.VMEM((NZ, NX * 128), F32),
            pltpu.VMEM((NX, NZ, NX * 128), F32),
            pltpu.VMEM((NX, 128, 128), F32),
            pltpu.VMEM((NX, 128, 128), BF16),
            pltpu.VMEM((NX, 128, 128), BF16),
            pltpu.VMEM((256, 128), BF16),
            pltpu.VMEM((32, 256), BF16),
            pltpu.VMEM((32, 256), BF16),
            pltpu.VMEM((96, 256), F32),
            pltpu.VMEM((NY, 64, 512), BF16),
            pltpu.VMEM((NY, 64, 512), BF16),
            pltpu.VMEM((64, 128), F32),
            pltpu.VMEM((NY, 64, 128), F32),
            pltpu.VMEM((64, 256), F32),
            pltpu.VMEM((2, 64, 512), F32),
            pltpu.VMEM((128, 128), BF16),
            pltpu.VMEM((64, 1024), BF16),
            pltpu.VMEM((8, 128), F32),
            pltpu.VMEM((NY, 8, 128), F32),
            dma((12,)), dma((8,)),
            dma((4,)), dma((4,)),
            dma((2,)), dma((2,)),
            dma((7,)), dma((16,)),
            dma((7,)), dma((8,)),
            dma((4,)), dma((4,)),
            dma((4,)), dma((4,)),
            pltpu.SemaphoreType.REGULAR((8,)),
            dma, dma,
            dma((4,)), dma((4,)), dma((4,)), dma((4,)),
            dma((4,)), dma((4,)),
            dma((4,)), dma((4,)),
            dma((7,)), dma((8,)),
            dma((4,)), dma((4,)),
        ],
        compiler_params=pltpu.CompilerParams(
            collective_id=0, has_side_effects=True, vmem_limit_bytes=40 * 1024 * 1024
        ),
    )(*(pltpu.with_memory_space_constraint(a, pltpu.HBM) for a in args))


def solution(mesh):
    torus = Mesh(mesh.devices.reshape(NZ, NX, 2, NY), ("z", "x", "c", "y"))
    every = ("z", "x", "c", "y")
    cols = P(None, "y")
    return jax.shard_map(
        on_device,
        mesh=torus,
        in_specs=(
            P(every, None), P(), cols, cols, cols, P("y"), cols, cols, cols, cols, cols,
            P("y"), P("y"), P("y"), P("y", None), P("y", None), P("y"),
        ),
        out_specs=P(("z", "x", "c"), "y"),
        check_vma=False,
    )
```

```python
import functools
import math

import jax
import jax.numpy as jnp
from jax import lax
from jax.experimental import pallas as pl
from jax.experimental.pallas import tpu as pltpu
from jax.sharding import Mesh
from jax.sharding import PartitionSpec as P

D = 2048
HD = 128
CONV_CH = 1024
WIDTH = 31
EPS = 1e-06
MESH = pl.DeviceIdType.MESH
F32 = jnp.float32
BF16 = jnp.bfloat16
NX = 4
NZ = 8
NY = 4
NCHIP = NX * NZ


STEPS = (2, 1)
WRAPS = (7, 6, 5)
GREETED = STEPS + WRAPS


def dot(a, b):
    return jnp.dot(a, b, preferred_element_type=F32)


def dot_nt(a, b):
    return lax.dot_general(a, b, (((1,), (1,)), ((), ())), preferred_element_type=F32)


def sigmoid(v):
    return jax.nn.sigmoid(v)


(C_K0, C_V0, C_Q0, C_A, C_B, C_GA, C_GC, C_CO, C_AO, C_K1, C_V1, C_Q1) = range(12)
SHARED = {C_K1: C_K0, C_V1: C_V0, C_Q1: C_Q0}


def kernel(
    hidden_hbm, pre_gain_hbm, w_query, w_key, w_value, offset_hbm, w_a, w_b, w_ga, w_gc,
    taps_hbm, bias_hbm, ngain_hbm, nshift_hbm, w_ao, w_co, post_gain_hbm,
    out,
    offset, hidden, pre_gain, taps, bias, ngain, nshift, post_gain, hbuf, wk, wv, wq, wa, wb, wga, wgc, wco, wo,
    kbuf, vbuf, kst, vst, qbuf, qst, obuf, tbl, tblr, wbuf, ps, pr, tri,
    gst, halo, gbuf, cst, crx, stx, srx, convb, gateb, att, abuf, ssx, ssr,
    lsem, ssem, h_s, h_r, p_s, p_r, z_s, z_r, q_s, q_r, t_s, t_r, o_s, o_r, ready, halo_s, halo_r,
    w_s, w_r, v_s, v_r, st_s, st_r, c_s, c_r, a_s, a_r, ss_s, ss_r,
):
    z = lax.axis_index("z")
    x = lax.axis_index("x")
    c = lax.axis_index("c")
    y = lax.axis_index("y")
    chip = z * NX + x
    oc = 1 - c

    def dev(zz=z, xx=x, cc=c, yy=y):
        return (zz, xx, cc, yy)

    def ypeer(d):
        return lax.rem(y + d, NY)

    def xpeer(d):
        return lax.rem(x + d, NX)

    def zpeer(d):
        return lax.rem(z + d + NZ, NZ)

    def rc(src, dst, ss, rs, to):
        return pltpu.make_async_remote_copy(
            src_ref=src, dst_ref=dst, send_sem=ss, recv_sem=rs, device_id=to, device_id_type=MESH
        )

    half = pl.ds(pl.multiple_of(c * HD, HD), HD)

    def whalf(yy, cc):
        return pl.ds(pl.multiple_of(yy * 256 + cc * HD, HD), HD)

    def start(copy):
        copy.start()

    def came(whole, group):
        rc(whole, whole, group[0], group[1], dev(cc=oc)).wait_recv()

    def gone(whole, group):
        rc(whole, whole, group[0], group[1], dev(cc=oc)).wait_send()

    all_h = hbuf.at[0:48, :], (h_s, h_r)
    all_p = qbuf.at[0:128, :], (p_s, p_r)
    all_q = qbuf.at[0:448, :], (q_s, q_r)
    all_t = tblr.at[0:3], (t_s, t_r)
    all_o = pr.at[0:3], (o_s, o_r)
    all_w = wo.at[0:384, :], (w_s, w_r)
    all_v = wo.at[0:384, :], (v_s, v_r)
    all_st = srx.at[0:3], (st_s, st_r)
    all_c = crx.at[0:3], (c_s, c_r)
    all_a = abuf.at[:, 0:896], (a_s, a_r)
    all_ss = ssr.at[0:3], (ss_s, ss_r)

    own_cols = pl.ds(pl.multiple_of(c * HD, HD), HD)
    oth_cols = pl.ds(pl.multiple_of(oc * HD, HD), HD)
    lo, hi = pl.ds(0, HD), pl.ds(HD, HD)
    ycols = pl.ds(pl.multiple_of(y * 512, 512), 512)
    yrows = pl.ds(pl.multiple_of(y * 256, 256), 256)
    local = {
        C_K1: (w_key.at[:, oth_cols], wk.at[:, lo]),
        C_K0: (w_key.at[:, own_cols], wk.at[:, hi]),
        C_V1: (w_value.at[:, oth_cols], wv.at[:, lo]),
        C_V0: (w_value.at[:, own_cols], wv.at[:, hi]),
        C_Q1: (w_query.at[:, oth_cols], wq.at[:, hi]),
        C_Q0: (w_query.at[:, own_cols], wq.at[:, lo]),
        C_A: (w_a, wa),
        C_B: (w_b, wb),
        C_GA: (w_ga, wga),
        C_GC: (w_gc, wgc),
        C_CO: (w_co, wco),
        C_AO: (w_ao.at[:, ycols], wo.at[yrows, :]),
    }
    local = {k: pltpu.make_async_copy(s, d, lsem.at[SHARED.get(k, k)]) for k, (s, d) in local.items()}
    first_in = [(hidden_hbm, hidden), (pre_gain_hbm, pre_gain)]
    later_in = [
        (taps_hbm, taps), (bias_hbm, bias), (ngain_hbm, ngain), (nshift_hbm, nshift), (post_gain_hbm, post_gain),
        (offset_hbm, offset),
    ]
    small = [
        pltpu.make_async_copy(a, b, ssem.at[i]) for i, (a, b) in enumerate(first_in + later_in)
    ]
    for copy in small[:2]:
        copy.start()

    barrier = pltpu.get_barrier_semaphore()
    next_chip = lax.rem(chip + 1, NCHIP)
    prev_chip = lax.rem(chip + NCHIP - 1, NCHIP)
    pair_chip = c * next_chip + oc * prev_chip
    pz, px = pair_chip // NX, lax.rem(pair_chip, NX)
    greet = [dev(yy=ypeer(d)) for d in (1, 2, 3)]
    greet += [dev(cc=oc, yy=ypeer(d)) for d in (0, 1, 2, 3)]
    greet += [dev(xx=xpeer(d), cc=cc) for d in (1, 2, 3) for cc in (c, oc)]
    for peer in greet:
        pl.semaphore_signal(barrier, inc=1, device_id=peer, device_id_type=MESH)
    greeted = len(greet)
    for k in GREETED:
        @pl.when(z + k < NZ)
        def _():
            for cc in (c, oc) if k in STEPS else (c,):
                pl.semaphore_signal(barrier, inc=1, device_id=dev(zz=zpeer(k), cc=cc), device_id_type=MESH)

        greeted = greeted + jnp.where(z >= k, 2 if k in STEPS else 1, 0)
    next_core = (pz, px, oc, y)
    has_next = (c == 1) & (chip < NCHIP - 1)
    has_prev = (c == 0) & (chip > 0)

    @pl.when(has_next)
    def _():
        pl.semaphore_signal(barrier, inc=1, device_id=next_core, device_id_type=MESH)

    greeted = greeted + jnp.where(has_prev, 1, 0)

    for copy in small[:2]:
        copy.wait()

    hv = hidden[...].astype(F32)
    inv = lax.rsqrt(jnp.mean(hv * hv, axis=1, keepdims=True) + EPS)
    my16 = pl.ds(pl.multiple_of(y * 16, 16), 16)
    hbuf[my16, :] = (hv * inv * pre_gain[...]).astype(BF16)

    pl.semaphore_wait(barrier, greeted)
    for k in GREETED:
        @pl.when(z >= k)
        def _():
            for cc in (c, oc) if k in STEPS else (c,):
                pl.semaphore_signal(ready.at[k], inc=1, device_id=dev(zz=zpeer(-k), cc=cc), device_id_type=MESH)

    @pl.when(has_prev)
    def _():
        pl.semaphore_signal(ready.at[0], inc=1, device_id=next_core, device_id_type=MESH)


    for d in (2, 1, 3):
        start(rc(hbuf.at[my16, :], hbuf.at[my16, :], h_s, h_r, dev(yy=ypeer(d))))
    for copy in local.values():
        copy.start()
    for copy in small[2:]:
        copy.start()

    r2 = lax.broadcasted_iota(jnp.int32, (2 * HD, HD), 0) % HD
    c2 = lax.broadcasted_iota(jnp.int32, (2 * HD, HD), 1)
    tri[...] = jnp.where(r2 > c2, 1.0, 0.0).astype(BF16)
    obuf[...] = jnp.zeros(obuf.shape, F32)
    tbl[...] = jnp.zeros(tbl.shape, F32)
    came(*all_h)

    def send_shard(d):
        yy = ypeer(d)
        cols = pl.ds(pl.multiple_of(yy * 512, 512), 512)
        start(rc(w_ao.at[half, cols], wo.at[whalf(y, c), :], w_s, w_r, dev(yy=yy)))

    send_shard(1)
    send_shard(3)

    my64 = pl.ds(pl.multiple_of(c * 64, 64), 64)
    oth64 = pl.ds(pl.multiple_of(oc * 64, 64), 64)
    partner = dev(cc=oc)
    tables = (kbuf, vbuf)
    for h, (w, st, name) in enumerate(((wk, kst, C_K0), (wv, vst, C_V0))):
        pltpu.make_async_copy(w, w, lsem.at[name]).wait()
        both = dot(hbuf[...], w[...]).astype(BF16)
        st[...] = both[:, :HD]
        start(rc(st, tables[h].at[z, my64, :], p_s, p_r, partner))
        tables[h][z, my64, :] = both[:, HD:]

    def z_copy(h, row, i, step):
        t = tables[h].at[row]
        return rc(t, t, z_s.at[i], z_r.at[h * NZ + row], dev(zz=zpeer(step)))

    for i, step in enumerate(STEPS):
        @pl.when(z < NZ - step)
        def _():
            pl.semaphore_wait(ready.at[step], 2)
            for h, st in enumerate((kst, vst)):
                half_own = tables[h].at[z, my64, :]
                there = z_r.at[h * NZ + z]
                rc(half_own, half_own, z_s.at[i], there, dev(zz=zpeer(step))).start()
                rc(st, half_own, z_s.at[i], there, dev(zz=zpeer(step), cc=oc)).start()

    pltpu.make_async_copy(wq, wq, lsem.at[C_Q0]).wait()
    qv = dot(hbuf[...], wq[...]).astype(BF16)
    qst[...] = qv[:, HD:]

    def qrows(xx, cc):
        return pl.ds(pl.multiple_of(xx * HD + cc * 64, 64), 64)

    mine = qbuf.at[qrows(x, c), :]
    qbuf[qrows(x, c), :] = qv[:, :HD]
    for d in range(NX):
        start(rc(qst, mine, q_s, q_r, dev(xx=xpeer(d), cc=oc)))
        if d > 0:
            start(rc(mine, mine, q_s, q_r, dev(xx=xpeer(d))))

    local[C_A].wait()
    local[C_B].wait()
    left = dot(hbuf[...], wa[...]).astype(BF16).astype(F32)
    right = dot(hbuf[...], wb[...]).astype(BF16).astype(F32)
    gated = (left * sigmoid(right)).astype(BF16)
    gst[...] = gated[32:, :]
    gbuf[32:, :] = gated.astype(F32)
    halo_to = ((next_chip // NX) * c + z * oc, lax.rem(next_chip, NX) * c + x * oc, oc, y)

    @pl.when(has_next)
    def _():
        pl.semaphore_wait(ready.at[0], 1)

    has_halo = (c == 1) | (chip > 0)
    sends_halo = (c == 0) | (chip < NCHIP - 1)

    @pl.when(sends_halo)
    def _():
        rc(gst, halo, halo_s, halo_r, halo_to).start()

    came(*all_p)

    for i, k in enumerate(WRAPS):
        @pl.when(z + k < NZ)
        def _():
            pl.semaphore_wait(ready.at[k], 1)
            for h in (0, 1):
                z_copy(h, z, 4 + i, k).start()

    def arrived(h, k):
        row = zpeer(-k)
        z_copy(h, row, 0, 1).wait_recv()

    def relay(h):
        @pl.when((z >= 2) & (z < NZ - 1))
        def _():
            arrived(h, 2)
            for i, step in enumerate(STEPS):
                @pl.when(z < NZ - step)
                def _():
                    z_copy(h, zpeer(-2), 2 + i, step).start()

    relay(0)
    small[7].wait()
    off = offset[c]
    scale = 1.0 / math.sqrt(HD)

    def some_blocks(ks):
        def come(h, k):
            if k == 2:
                pl.when(z == NZ - 1)(functools.partial(arrived, h, k))
            elif k > 0:
                arrived(h, k)

        for k in ks:
            come(0, k)
        fronts = []
        for k in ks:
            row = zpeer(-k)
            for b in range(NX):
                s = dot_nt(qbuf[b * HD : (b + 1) * HD, :], kbuf[row]) * scale + off
                u = jnp.exp(-jnp.abs(s))
                one = 1.0 + u
                tail = jnp.log(one) + (u - (one - 1.0))
                soft = jnp.maximum(s, 0.0) + tail
                logit = s - soft
                if k == 0:
                    rows = lax.broadcasted_iota(jnp.int32, (HD, HD), 0) + b * HD
                    cols = lax.broadcasted_iota(jnp.int32, (HD, HD), 1) + x * HD
                    soft = jnp.where(cols < rows, soft, 0.0)
                    logit = jnp.where(cols < rows, logit, -jnp.inf)
                top = soft.astype(BF16)
                rest = (soft - top.astype(F32)).astype(BF16)
                fronts.append((k, row, b, logit, jnp.concatenate([top, rest], axis=1)))
        sums = [dot(f[4], tri[...]) for f in fronts]
        ones = jnp.ones((NZ, 2 * HD), BF16)
        for k, row, b, _, pair in fronts:
            here = lax.broadcasted_iota(jnp.int32, (NZ, HD), 0) == row
            cols = slice(b * HD, (b + 1) * HD)
            tbl[:, cols] = jnp.where(here, dot_nt(ones, pair), tbl[:, cols])
        sticks = [jnp.exp(f[3] - t).astype(BF16) for f, t in zip(fronts, sums)]
        for k in ks:
            come(1, k)
        for (k, row, b, _, _), stick in zip(fronts, sticks):
            obuf[row, b] = dot(stick, vbuf[row])

    def blocks(low, high):
        pl.when(z >= high)(functools.partial(some_blocks, (low, high)))
        pl.when((z >= low) & (z < high))(functools.partial(some_blocks, (low,)))

    @pl.when(has_halo)
    def _():
        rc(gst, halo, halo_s, halo_r, halo_to).wait_recv()
        gbuf[0:32, :] = halo[...].astype(F32)

    @pl.when(jnp.logical_not(has_halo))
    def _():
        gbuf[0:32, :] = jnp.zeros((32, 256), F32)

    for copy in small[2:7]:
        copy.wait()
    conv = jnp.broadcast_to(bias[...], (64, 256))
    for i in range(WIDTH):
        conv = conv + taps[i : i + 1, :] * gbuf[2 + i : 66 + i, :]
    local_mean = jnp.mean(conv, axis=1, keepdims=True)
    dev_local = conv - local_mean
    local_m2 = jnp.sum(dev_local * dev_local, axis=1, keepdims=True)
    lane = lax.broadcasted_iota(jnp.int32, (64, HD), 1)
    stx[...] = jnp.where(lane < 64, local_mean, local_m2)
    for d in (2, 1, 3):
        start(rc(stx, srx.at[y], st_s, st_r, dev(yy=ypeer(d))))
    convb[...] = conv

    send_shard(2)
    relay(1)
    came(*all_q)

    blocks(0, 1)
    blocks(2, 7)
    blocks(5, 6)
    blocks(3, 4)
    for d in (2, 1, 3):
        start(rc(tbl, tblr.at[x], t_s, t_r, dev(xx=xpeer(d))))
    tblr[x] = tbl[...]

    local[C_GA].wait()
    local[C_GC].wait()
    gateb[0] = sigmoid(dot(hbuf[...], wga[...]).astype(BF16).astype(F32))
    gateb[1] = sigmoid(dot(hbuf[...], wgc[...]).astype(BF16).astype(F32))

    srx[y] = stx[...]
    came(*all_st)
    stats = [srx[i] for i in range(NY)]
    means = [t[:, 0:1] for t in stats]
    mean = (means[0] + means[1] + means[2] + means[3]) * 0.25
    m2 = stats[0][:, 64:65] + stats[1][:, 64:65] + stats[2][:, 64:65] + stats[3][:, 64:65]
    for t in means:
        m2 = m2 + 256.0 * (t - mean) * (t - mean)
    cn = (convb[...] - mean) * lax.rsqrt(m2 / CONV_CH + EPS) * ngain[...] + nshift[...]
    cn = (cn * sigmoid(cn)).astype(BF16)
    local[C_CO].wait()
    for i in range(NY):
        cst[i] = dot(cn, wco[:, i * 512 : (i + 1) * 512]).astype(BF16)
    for d in (2, 1, 3):
        yy = ypeer(d)
        start(rc(cst.at[yy], crx.at[y], c_s, c_r, dev(yy=yy)))

    came(*all_t)

    totals = [tblr[i] for i in range(NX)]
    row_sum = totals[0] + totals[1] + totals[2] + totals[3]
    at = lax.broadcasted_iota(jnp.int32, (NZ, NX * HD), 0)
    outside = jnp.zeros((NZ, NX * HD), F32)
    for j in range(1, NZ):
        outside = outside + jnp.where(at < j, row_sum[j : j + 1, :], 0.0)
    for i in range(1, NX):
        outside = outside + jnp.where(x < i, 1.0, 0.0) * totals[i]
    weight = jnp.exp(-outside)
    per_row = jnp.concatenate([weight, jnp.zeros((HD - NZ, NX * HD), F32)], axis=0).T
    for b in range(NX):
        wbuf[b] = per_row[b * HD : (b + 1) * HD, :]
    for d in (2, 1, 3, 0):
        b = xpeer(d)
        per_row = wbuf[b]
        acc = obuf[0, b] * per_row[:, 0:1]
        for j in range(1, NZ):
            acc = acc + obuf[j, b] * per_row[:, j : j + 1]
        if d > 0:
            ps[d] = acc.astype(BF16)
            start(rc(ps.at[d], pr.at[x], o_s, o_r, dev(xx=b)))

    came(*all_w)
    for d in (2, 1, 3):
        got = wo.at[whalf(ypeer(d), c), :]
        start(rc(got, got, v_s, v_r, partner))

    came(*all_o)
    for d in (2, 1, 3):
        xx = xpeer(d)
        acc = acc + pr[xx].astype(F32)
    att[...] = acc.astype(BF16)

    head = pl.ds(pl.multiple_of((y * 2 + c) * HD, HD), HD)
    for d in (2, 1, 3, 0):
        for cc, rows in ((c, my64), (oc, oth64)):
            if d == 0 and cc is c:
                continue
            start(rc(att.at[rows, :], abuf.at[:, head], a_s, a_r, dev(cc=cc, yy=ypeer(d))))
    abuf[:, head] = att[my64, :]
    local[C_AO].wait()
    came(*all_v)

    csum = cst[y].astype(F32)
    came(*all_c)
    for d in (2, 1, 3):
        yy = ypeer(d)
        csum = csum + crx[yy].astype(F32)
    gateb[1] = gateb[1] * csum.astype(BF16).astype(F32)

    came(*all_a)
    branch = dot(abuf[...], wo[...]).astype(BF16).astype(F32)
    merged = gateb[0] * branch + gateb[1]
    sq = merged * merged
    part = sq[:, 0:128] + sq[:, 128:256] + sq[:, 256:384] + sq[:, 384:512]
    part = jnp.concatenate([part, jnp.zeros((64, HD), F32)], axis=0).T
    ssx[...] = jnp.sum(part.reshape(16, 8, HD), axis=0)
    for d in (2, 1, 3):
        start(rc(ssx, ssr.at[y], ss_s, ss_r, dev(yy=ypeer(d))))
    total = ssx[...]
    came(*all_ss)
    for d in (2, 1, 3):
        total = total + ssr[ypeer(d)]
    total = jnp.broadcast_to(jnp.sum(total, axis=0, keepdims=True), (HD, HD)).T[:64, 0:1]
    out[...] = (merged * lax.rsqrt(total / D + EPS) * post_gain[...]).astype(BF16)

    for group in (all_h, all_p, all_q, all_t, all_o, all_w, all_v, all_st, all_c, all_a, all_ss):
        gone(*group)
    def z_sent(i, cond):
        @pl.when(cond)
        def _():
            two = kbuf.at[0:2]
            rc(two, two, z_s.at[i], z_r.at[0], partner).wait_send()

    for i, step in enumerate(STEPS):
        z_sent(i, z < NZ - step)
        z_sent(2 + i, (z >= 2) & (z < NZ - step))
    for i, k in enumerate(WRAPS):
        z_sent(4 + i, z + k < NZ)

    @pl.when(sends_halo)
    def _():
        rc(gst, halo, halo_s, halo_r, halo_to).wait_send()


def on_device(
    hidden_in, pre_gain, w_query, w_key, w_value, stick_offset, w_glu_a, w_glu_b, w_gate_attn,
    w_gate_conv, conv_taps, conv_bias, norm_gain, norm_shift, w_attn_out, w_conv_out, post_gain,
):
    args = (
        hidden_in, pre_gain.reshape(1, -1), w_query, w_key, w_value, stick_offset, w_glu_a,
        w_glu_b, w_gate_attn, w_gate_conv, conv_taps, conv_bias.reshape(1, -1),
        norm_gain.reshape(1, -1), norm_shift.reshape(1, -1), w_attn_out, w_conv_out,
        post_gain.reshape(1, -1),
    )
    hb = pl.BlockSpec(memory_space=pl.ANY)
    dma = pltpu.SemaphoreType.DMA
    return pl.pallas_call(
        kernel,
        out_shape=jax.ShapeDtypeStruct((64, 512), BF16),
        in_specs=[hb] * 17,
        out_specs=pl.BlockSpec(memory_space=pltpu.VMEM),
        scratch_shapes=[
            pltpu.SMEM((2,), F32),
            pltpu.VMEM((16, D), BF16),
            pltpu.VMEM((1, D), F32),
            pltpu.VMEM((WIDTH, 256), F32),
            pltpu.VMEM((1, 256), F32),
            pltpu.VMEM((1, 256), F32),
            pltpu.VMEM((1, 256), F32),
            pltpu.VMEM((1, 512), F32),
            pltpu.VMEM((64, D), BF16),
            pltpu.VMEM((D, 256), BF16),
            pltpu.VMEM((D, 256), BF16),
            pltpu.VMEM((D, 256), BF16),
            pltpu.VMEM((D, 256), BF16),
            pltpu.VMEM((D, 256), BF16),
            pltpu.VMEM((D, 512), BF16),
            pltpu.VMEM((D, 512), BF16),
            pltpu.VMEM((256, D), BF16),
            pltpu.VMEM((1024, 512), BF16),
            pltpu.VMEM((NZ, 128, 128), BF16),
            pltpu.VMEM((NZ, 128, 128), BF16),
            pltpu.VMEM((64, 128), BF16),
            pltpu.VMEM((64, 128), BF16),
            pltpu.VMEM((NX * 128, 128), BF16),
            pltpu.VMEM((64, 128), BF16),
            pltpu.VMEM((NZ, NX, 128, 128), F32),
            pltpu.VMEM((NZ, NX * 128), F32),
            pltpu.VMEM((NX, NZ, NX * 128), F32),
            pltpu.VMEM((NX, 128, 128), F32),
            pltpu.VMEM((NX, 128, 128), BF16),
            pltpu.VMEM((NX, 128, 128), BF16),
            pltpu.VMEM((256, 128), BF16),
            pltpu.VMEM((32, 256), BF16),
            pltpu.VMEM((32, 256), BF16),
            pltpu.VMEM((96, 256), F32),
            pltpu.VMEM((NY, 64, 512), BF16),
            pltpu.VMEM((NY, 64, 512), BF16),
            pltpu.VMEM((64, 128), F32),
            pltpu.VMEM((NY, 64, 128), F32),
            pltpu.VMEM((64, 256), F32),
            pltpu.VMEM((2, 64, 512), F32),
            pltpu.VMEM((128, 128), BF16),
            pltpu.VMEM((64, 1024), BF16),
            pltpu.VMEM((8, 128), F32),
            pltpu.VMEM((NY, 8, 128), F32),
            dma((9,)), dma((8,)),
            dma, dma,
            dma, dma,
            dma((7,)), dma((16,)),
            dma, dma,
            dma, dma,
            dma, dma,
            pltpu.SemaphoreType.REGULAR((8,)),
            dma, dma,
            dma, dma, dma, dma,
            dma, dma,
            dma, dma,
            dma, dma,
            dma, dma,
        ],
        compiler_params=pltpu.CompilerParams(
            collective_id=0, has_side_effects=True, vmem_limit_bytes=40 * 1024 * 1024
        ),
    )(*(pltpu.with_memory_space_constraint(a, pltpu.HBM) for a in args))


def solution(mesh):
    torus = Mesh(mesh.devices.reshape(NZ, NX, 2, NY), ("z", "x", "c", "y"))
    every = ("z", "x", "c", "y")
    cols = P(None, "y")
    return jax.shard_map(
        on_device,
        mesh=torus,
        in_specs=(
            P(every, None), P(), cols, cols, cols, P("y"), cols, cols, cols, cols, cols,
            P("y"), P("y"), P("y"), P("y", None), P("y", None), P("y"),
        ),
        out_specs=P(("z", "x", "c"), "y"),
        check_vma=False,
    )
```

```python
import functools
import math

import jax
import jax.numpy as jnp
from jax import lax
from jax.experimental import pallas as pl
from jax.experimental.pallas import tpu as pltpu
from jax.sharding import Mesh
from jax.sharding import PartitionSpec as P

D = 2048
HD = 128
CONV_CH = 1024
WIDTH = 31
EPS = 1e-06
MESH = pl.DeviceIdType.MESH
F32 = jnp.float32
BF16 = jnp.bfloat16
NX = 4
NZ = 8
NY = 4
NCHIP = NX * NZ


STEPS = (2, 1)
WRAPS = (7, 6, 5)
GREETED = STEPS + WRAPS


def dot(a, b):
    return jnp.dot(a, b, preferred_element_type=F32)


def dot_nt(a, b):
    return lax.dot_general(a, b, (((1,), (1,)), ((), ())), preferred_element_type=F32)


def sigmoid(v):
    return jax.nn.sigmoid(v)


(C_K0, C_V0, C_Q0, C_A, C_B, C_GA, C_GC, C_CO, C_AO, C_K1, C_V1, C_Q1) = range(12)
SHARED = {C_K1: C_K0, C_V1: C_V0, C_Q1: C_Q0}


def kernel(
    hidden_hbm, pre_gain_hbm, w_query, w_key, w_value, offset_hbm, w_a, w_b, w_ga, w_gc,
    taps_hbm, bias_hbm, ngain_hbm, nshift_hbm, w_ao, w_co, post_gain_hbm,
    out,
    offset, hidden, pre_gain, taps, bias, ngain, nshift, post_gain, hbuf, wk, wv, wq, wa, wb, wga, wgc, wco, wo,
    kbuf, vbuf, kst, vst, qbuf, qst, obuf, stk, tbl, tblr, wbuf, own, ps, pr, tri,
    gst, halo, gbuf, cst, crx, stx, srx, convb, gateb, att, abuf, ssx, ssr,
    lsem, ssem, h_s, h_r, p_s, p_r, z_s, z_r, q_s, q_r, t_s, t_r, o_s, o_r, ready, halo_s, halo_r,
    w_s, w_r, v_s, v_r, st_s, st_r, c_s, c_r, a_s, a_r, ss_s, ss_r,
):
    z = lax.axis_index("z")
    x = lax.axis_index("x")
    c = lax.axis_index("c")
    y = lax.axis_index("y")
    chip = z * NX + x
    oc = 1 - c

    def dev(zz=z, xx=x, cc=c, yy=y):
        return (zz, xx, cc, yy)

    def ypeer(d):
        return lax.rem(y + d, NY)

    def xpeer(d):
        return lax.rem(x + d, NX)

    def zpeer(d):
        return lax.rem(z + d + NZ, NZ)

    def rc(src, dst, ss, rs, to):
        return pltpu.make_async_remote_copy(
            src_ref=src, dst_ref=dst, send_sem=ss, recv_sem=rs, device_id=to, device_id_type=MESH
        )

    half = pl.ds(pl.multiple_of(c * HD, HD), HD)

    def whalf(yy, cc):
        return pl.ds(pl.multiple_of(yy * 256 + cc * HD, HD), HD)

    def start(copy):
        copy.start()

    def came(whole, group):
        rc(whole, whole, group[0], group[1], dev(cc=oc)).wait_recv()

    def gone(whole, group):
        rc(whole, whole, group[0], group[1], dev(cc=oc)).wait_send()

    all_h = hbuf.at[0:48, :], (h_s, h_r)
    all_p = qbuf.at[0:128, :], (p_s, p_r)
    all_q = qbuf.at[0:448, :], (q_s, q_r)
    all_t = tblr.at[0:3], (t_s, t_r)
    all_o = [(pr.at[0:3, i * 64 : (i + 1) * 64], (o_s.at[i], o_r.at[i])) for i in (0, 1)]
    all_w = wo.at[0:384, :], (w_s, w_r)
    all_v = wo.at[0:384, :], (v_s, v_r)
    all_st = srx.at[0:3], (st_s, st_r)
    all_c = crx.at[0:3], (c_s, c_r)
    all_a = abuf.at[:, 0:896], (a_s, a_r)
    all_ss = ssr.at[0:3], (ss_s, ss_r)

    own_cols = pl.ds(pl.multiple_of(c * HD, HD), HD)
    oth_cols = pl.ds(pl.multiple_of(oc * HD, HD), HD)
    lo, hi = pl.ds(0, HD), pl.ds(HD, HD)
    ycols = pl.ds(pl.multiple_of(y * 512, 512), 512)
    yrows = pl.ds(pl.multiple_of(y * 256, 256), 256)
    local = {
        C_K1: (w_key.at[:, oth_cols], wk.at[:, lo]),
        C_K0: (w_key.at[:, own_cols], wk.at[:, hi]),
        C_V1: (w_value.at[:, oth_cols], wv.at[:, lo]),
        C_V0: (w_value.at[:, own_cols], wv.at[:, hi]),
        C_Q1: (w_query.at[:, oth_cols], wq.at[:, hi]),
        C_Q0: (w_query.at[:, own_cols], wq.at[:, lo]),
        C_A: (w_a, wa),
        C_B: (w_b, wb),
        C_GA: (w_ga, wga),
        C_GC: (w_gc, wgc),
        C_CO: (w_co, wco),
        C_AO: (w_ao.at[:, ycols], wo.at[yrows, :]),
    }
    local = {k: pltpu.make_async_copy(s, d, lsem.at[SHARED.get(k, k)]) for k, (s, d) in local.items()}
    first_in = [(hidden_hbm, hidden), (pre_gain_hbm, pre_gain)]
    later_in = [
        (taps_hbm, taps), (bias_hbm, bias), (ngain_hbm, ngain), (nshift_hbm, nshift), (post_gain_hbm, post_gain),
        (offset_hbm, offset),
    ]
    small = [
        pltpu.make_async_copy(a, b, ssem.at[i]) for i, (a, b) in enumerate(first_in + later_in)
    ]
    for copy in small[:2]:
        copy.start()

    barrier = pltpu.get_barrier_semaphore()
    next_chip = lax.rem(chip + 1, NCHIP)
    prev_chip = lax.rem(chip + NCHIP - 1, NCHIP)
    pair_chip = c * next_chip + oc * prev_chip
    pz, px = pair_chip // NX, lax.rem(pair_chip, NX)
    greet = [dev(yy=ypeer(d)) for d in (1, 2, 3)]
    greet += [dev(cc=oc, yy=ypeer(d)) for d in (0, 1, 2, 3)]
    greet += [dev(xx=xpeer(d), cc=cc) for d in (1, 2, 3) for cc in (c, oc)]
    for peer in greet:
        pl.semaphore_signal(barrier, inc=1, device_id=peer, device_id_type=MESH)
    greeted = len(greet)
    for k in GREETED:
        @pl.when(z + k < NZ)
        def _():
            for cc in (c, oc) if k in STEPS else (c,):
                pl.semaphore_signal(barrier, inc=1, device_id=dev(zz=zpeer(k), cc=cc), device_id_type=MESH)

        greeted = greeted + jnp.where(z >= k, 2 if k in STEPS else 1, 0)
    next_core = (pz, px, oc, y)
    has_next = (c == 1) & (chip < NCHIP - 1)
    has_prev = (c == 0) & (chip > 0)

    @pl.when(has_next)
    def _():
        pl.semaphore_signal(barrier, inc=1, device_id=next_core, device_id_type=MESH)

    greeted = greeted + jnp.where(has_prev, 1, 0)

    for copy in small[:2]:
        copy.wait()

    hv = hidden[...].astype(F32)
    inv = lax.rsqrt(jnp.mean(hv * hv, axis=1, keepdims=True) + EPS)
    my16 = pl.ds(pl.multiple_of(y * 16, 16), 16)
    hbuf[my16, :] = (hv * inv * pre_gain[...]).astype(BF16)

    pl.semaphore_wait(barrier, greeted)
    for k in GREETED:
        @pl.when(z >= k)
        def _():
            for cc in (c, oc) if k in STEPS else (c,):
                pl.semaphore_signal(ready.at[k], inc=1, device_id=dev(zz=zpeer(-k), cc=cc), device_id_type=MESH)

    @pl.when(has_prev)
    def _():
        pl.semaphore_signal(ready.at[0], inc=1, device_id=next_core, device_id_type=MESH)


    for d in (2, 1, 3):
        start(rc(hbuf.at[my16, :], hbuf.at[my16, :], h_s, h_r, dev(yy=ypeer(d))))
    for copy in local.values():
        copy.start()
    for copy in small[2:]:
        copy.start()

    r2 = lax.broadcasted_iota(jnp.int32, (2 * HD, HD), 0) % HD
    c2 = lax.broadcasted_iota(jnp.int32, (2 * HD, HD), 1)
    tri[...] = jnp.where(r2 > c2, 1.0, 0.0).astype(BF16)
    obuf[...] = jnp.zeros(obuf.shape, F32)
    tbl[...] = jnp.zeros(tbl.shape, F32)
    came(*all_h)

    def send_shard(d):
        yy = ypeer(d)
        cols = pl.ds(pl.multiple_of(yy * 512, 512), 512)
        start(rc(w_ao.at[half, cols], wo.at[whalf(y, c), :], w_s, w_r, dev(yy=yy)))

    send_shard(1)
    send_shard(3)

    my64 = pl.ds(pl.multiple_of(c * 64, 64), 64)
    oth64 = pl.ds(pl.multiple_of(oc * 64, 64), 64)
    partner = dev(cc=oc)
    tables = (kbuf, vbuf)
    for h, (w, st, name) in enumerate(((wk, kst, C_K0), (wv, vst, C_V0))):
        pltpu.make_async_copy(w, w, lsem.at[name]).wait()
        both = dot(hbuf[...], w[...]).astype(BF16)
        st[...] = both[:, :HD]
        start(rc(st, tables[h].at[z, my64, :], p_s, p_r, partner))
        tables[h][z, my64, :] = both[:, HD:]

    def z_copy(h, row, i, step):
        t = tables[h].at[row]
        return rc(t, t, z_s.at[i], z_r.at[h * NZ + row], dev(zz=zpeer(step)))

    for i, step in enumerate(STEPS):
        @pl.when(z < NZ - step)
        def _():
            pl.semaphore_wait(ready.at[step], 2)
            for h, st in enumerate((kst, vst)):
                half_own = tables[h].at[z, my64, :]
                there = z_r.at[h * NZ + z]
                rc(half_own, half_own, z_s.at[i], there, dev(zz=zpeer(step))).start()
                rc(st, half_own, z_s.at[i], there, dev(zz=zpeer(step), cc=oc)).start()

    pltpu.make_async_copy(wq, wq, lsem.at[C_Q0]).wait()
    qv = dot(hbuf[...], wq[...]).astype(BF16)
    qst[...] = qv[:, HD:]

    def qrows(xx, cc):
        return pl.ds(pl.multiple_of(xx * HD + cc * 64, 64), 64)

    mine = qbuf.at[qrows(x, c), :]
    qbuf[qrows(x, c), :] = qv[:, :HD]
    for d in range(NX):
        start(rc(qst, mine, q_s, q_r, dev(xx=xpeer(d), cc=oc)))
        if d > 0:
            start(rc(mine, mine, q_s, q_r, dev(xx=xpeer(d))))

    local[C_A].wait()
    local[C_B].wait()
    left = dot(hbuf[...], wa[...]).astype(BF16).astype(F32)
    right = dot(hbuf[...], wb[...]).astype(BF16).astype(F32)
    gated = (left * sigmoid(right)).astype(BF16)
    gst[...] = gated[32:, :]
    gbuf[32:, :] = gated.astype(F32)
    halo_to = ((next_chip // NX) * c + z * oc, lax.rem(next_chip, NX) * c + x * oc, oc, y)

    @pl.when(has_next)
    def _():
        pl.semaphore_wait(ready.at[0], 1)

    has_halo = (c == 1) | (chip > 0)
    sends_halo = (c == 0) | (chip < NCHIP - 1)

    @pl.when(sends_halo)
    def _():
        rc(gst, halo, halo_s, halo_r, halo_to).start()

    came(*all_p)

    for i, k in enumerate(WRAPS):
        @pl.when(z + k < NZ)
        def _():
            pl.semaphore_wait(ready.at[k], 1)
            for h in (0, 1):
                z_copy(h, z, 4 + i, k).start()

    def arrived(h, k):
        row = zpeer(-k)
        z_copy(h, row, 0, 1).wait_recv()

    def relay(h):
        @pl.when((z >= 2) & (z < NZ - 1))
        def _():
            arrived(h, 2)
            for i, step in enumerate(STEPS):
                @pl.when(z < NZ - step)
                def _():
                    z_copy(h, zpeer(-2), 2 + i, step).start()

    relay(0)
    small[7].wait()
    off = offset[c]
    scale = 1.0 / math.sqrt(HD)

    def come(h, k):
        if k == 2:
            pl.when(z == NZ - 1)(functools.partial(arrived, h, k))
        elif k > 0:
            arrived(h, k)

    def some_blocks(ks):
        for k in ks:
            come(0, k)
        fronts = []
        for k in ks:
            row = zpeer(-k)
            for b in range(NX):
                s = dot_nt(qbuf[b * HD : (b + 1) * HD, :], kbuf[row]) * scale + off
                u = jnp.exp(-jnp.abs(s))
                one = 1.0 + u
                tail = jnp.log(one) + (u - (one - 1.0))
                soft = jnp.maximum(s, 0.0) + tail
                logit = s - soft
                if k == 0:
                    rows = lax.broadcasted_iota(jnp.int32, (HD, HD), 0) + b * HD
                    cols = lax.broadcasted_iota(jnp.int32, (HD, HD), 1) + x * HD
                    soft = jnp.where(cols < rows, soft, 0.0)
                    logit = jnp.where(cols < rows, logit, -jnp.inf)
                top = soft.astype(BF16)
                rest = (soft - top.astype(F32)).astype(BF16)
                fronts.append((k, row, b, logit, jnp.concatenate([top, rest], axis=1)))
        sums = [dot(f[4], tri[...]) for f in fronts]
        ones = jnp.ones((NZ, 2 * HD), BF16)
        for k, row, b, _, pair in fronts:
            here = lax.broadcasted_iota(jnp.int32, (NZ, HD), 0) == row
            cols = slice(b * HD, (b + 1) * HD)
            tbl[:, cols] = jnp.where(here, dot_nt(ones, pair), tbl[:, cols])
        for (k, row, b, logit, _), t in zip(fronts, sums):
            stk[k, b * HD : (b + 1) * HD, :] = jnp.exp(logit - t).astype(BF16)

    def blocks(low, high):
        pl.when(z >= high)(functools.partial(some_blocks, (low, high)))
        pl.when((z >= low) & (z < high))(functools.partial(some_blocks, (low,)))

    @pl.when(has_halo)
    def _():
        rc(gst, halo, halo_s, halo_r, halo_to).wait_recv()
        gbuf[0:32, :] = halo[...].astype(F32)

    @pl.when(jnp.logical_not(has_halo))
    def _():
        gbuf[0:32, :] = jnp.zeros((32, 256), F32)

    for copy in small[2:7]:
        copy.wait()
    conv = jnp.broadcast_to(bias[...], (64, 256))
    for i in range(WIDTH):
        conv = conv + taps[i : i + 1, :] * gbuf[2 + i : 66 + i, :]
    local_mean = jnp.mean(conv, axis=1, keepdims=True)
    dev_local = conv - local_mean
    local_m2 = jnp.sum(dev_local * dev_local, axis=1, keepdims=True)
    lane = lax.broadcasted_iota(jnp.int32, (64, HD), 1)
    stx[...] = jnp.where(lane < 64, local_mean, local_m2)
    for d in (2, 1, 3):
        start(rc(stx, srx.at[y], st_s, st_r, dev(yy=ypeer(d))))
    convb[...] = conv

    send_shard(2)
    relay(1)
    came(*all_q)

    blocks(0, 1)
    blocks(2, 7)
    blocks(5, 6)
    blocks(3, 4)
    for d in (2, 1, 3):
        start(rc(tbl, tblr.at[x], t_s, t_r, dev(xx=xpeer(d))))
    tblr[x] = tbl[...]

    srx[y] = stx[...]
    came(*all_st)
    stats = [srx[i] for i in range(NY)]
    means = [t[:, 0:1] for t in stats]
    mean = (means[0] + means[1] + means[2] + means[3]) * 0.25
    m2 = stats[0][:, 64:65] + stats[1][:, 64:65] + stats[2][:, 64:65] + stats[3][:, 64:65]
    for t in means:
        m2 = m2 + 256.0 * (t - mean) * (t - mean)
    cn = (convb[...] - mean) * lax.rsqrt(m2 / CONV_CH + EPS) * ngain[...] + nshift[...]
    cn = (cn * sigmoid(cn)).astype(BF16)
    local[C_CO].wait()
    for i in range(NY):
        cst[i] = dot(cn, wco[:, i * 512 : (i + 1) * 512]).astype(BF16)
    for d in (2, 1, 3):
        yy = ypeer(d)
        start(rc(cst.at[yy], crx.at[y], c_s, c_r, dev(yy=yy)))

    for k in (0, 1, 2, 7, 6, 5, 3, 4):
        @pl.when(z >= k)
        def _():
            come(1, k)
            row = zpeer(-k)
            obuf[row] = dot(stk[k], vbuf[row])

    came(*all_t)

    totals = [tblr[i] for i in range(NX)]
    row_sum = totals[0] + totals[1] + totals[2] + totals[3]
    at = lax.broadcasted_iota(jnp.int32, (NZ, NX * HD), 0)
    outside = jnp.zeros((NZ, NX * HD), F32)
    for j in range(1, NZ):
        outside = outside + jnp.where(at < j, row_sum[j : j + 1, :], 0.0)
    for i in range(1, NX):
        outside = outside + jnp.where(x < i, 1.0, 0.0) * totals[i]
    weight = jnp.exp(-outside)
    per_row = weight.T
    for b in range(NX):
        wbuf[b] = per_row[b * HD : (b + 1) * HD, :]
    for d in (2, 1, 3, 0):
        b = xpeer(d)
        per_row = wbuf[b]
        rows = pl.ds(pl.multiple_of(b * HD, HD), HD)
        acc = obuf[0, rows, :] * per_row[:, 0:1]
        for j in range(1, NZ):
            acc = acc + obuf[j, rows, :] * per_row[:, j : j + 1]
        if d > 0:
            ps[d] = acc.astype(BF16)
        else:
            own[...] = acc
    halves = [slice(i * 64, (i + 1) * 64) for i in (0, 1)]
    for i in (0, 1):
        for d in (2, 1, 3):
            start(rc(ps.at[d, halves[i]], pr.at[x, halves[i]], o_s.at[i], o_r.at[i], dev(xx=xpeer(d))))

    came(*all_w)
    for d in (2, 1, 3):
        got = wo.at[whalf(ypeer(d), c), :]
        start(rc(got, got, v_s, v_r, partner))

    local[C_GA].wait()
    local[C_GC].wait()
    gateb[0] = sigmoid(dot(hbuf[...], wga[...]).astype(BF16).astype(F32))
    gateb[1] = sigmoid(dot(hbuf[...], wgc[...]).astype(BF16).astype(F32))

    head = pl.ds(pl.multiple_of((y * 2 + c) * HD, HD), HD)
    for i, rows in enumerate(halves):
        came(*all_o[i])
        acc = own[rows, :]
        for d in (2, 1, 3):
            acc = acc + pr[xpeer(d), rows, :].astype(F32)
        att[rows, :] = acc.astype(BF16)
        for d in (2, 1, 3):
            start(rc(att.at[rows, :], abuf.at[:, head], a_s, a_r, dev(cc=i, yy=ypeer(d))))

        @pl.when(c == i)
        def _():
            abuf[:, head] = att[rows, :]

        @pl.when(c != i)
        def _():
            rc(att.at[rows, :], abuf.at[:, head], a_s, a_r, dev(cc=i)).start()

    local[C_AO].wait()
    came(*all_v)

    csum = cst[y].astype(F32)
    came(*all_c)
    for d in (2, 1, 3):
        yy = ypeer(d)
        csum = csum + crx[yy].astype(F32)
    gateb[1] = gateb[1] * csum.astype(BF16).astype(F32)

    came(*all_a)
    branch = dot(abuf[...], wo[...]).astype(BF16).astype(F32)
    merged = gateb[0] * branch + gateb[1]
    sq = merged * merged
    part = sq[:, 0:128] + sq[:, 128:256] + sq[:, 256:384] + sq[:, 384:512]
    part = jnp.concatenate([part, jnp.zeros((64, HD), F32)], axis=0).T
    ssx[...] = jnp.sum(part.reshape(16, 8, HD), axis=0)
    for d in (2, 1, 3):
        start(rc(ssx, ssr.at[y], ss_s, ss_r, dev(yy=ypeer(d))))
    total = ssx[...]
    came(*all_ss)
    for d in (2, 1, 3):
        total = total + ssr[ypeer(d)]
    total = jnp.broadcast_to(jnp.sum(total, axis=0, keepdims=True), (HD, HD)).T[:64, 0:1]
    out[...] = (merged * lax.rsqrt(total / D + EPS) * post_gain[...]).astype(BF16)

    for group in (all_h, all_p, all_q, all_t, *all_o, all_w, all_v, all_st, all_c, all_a, all_ss):
        gone(*group)
    def z_sent(i, cond):
        @pl.when(cond)
        def _():
            two = kbuf.at[0:2]
            rc(two, two, z_s.at[i], z_r.at[0], partner).wait_send()

    for i, step in enumerate(STEPS):
        z_sent(i, z < NZ - step)
        z_sent(2 + i, (z >= 2) & (z < NZ - step))
    for i, k in enumerate(WRAPS):
        z_sent(4 + i, z + k < NZ)

    @pl.when(sends_halo)
    def _():
        rc(gst, halo, halo_s, halo_r, halo_to).wait_send()


def on_device(
    hidden_in, pre_gain, w_query, w_key, w_value, stick_offset, w_glu_a, w_glu_b, w_gate_attn,
    w_gate_conv, conv_taps, conv_bias, norm_gain, norm_shift, w_attn_out, w_conv_out, post_gain,
):
    args = (
        hidden_in, pre_gain.reshape(1, -1), w_query, w_key, w_value, stick_offset, w_glu_a,
        w_glu_b, w_gate_attn, w_gate_conv, conv_taps, conv_bias.reshape(1, -1),
        norm_gain.reshape(1, -1), norm_shift.reshape(1, -1), w_attn_out, w_conv_out,
        post_gain.reshape(1, -1),
    )
    hb = pl.BlockSpec(memory_space=pl.ANY)
    dma = pltpu.SemaphoreType.DMA
    return pl.pallas_call(
        kernel,
        out_shape=jax.ShapeDtypeStruct((64, 512), BF16),
        in_specs=[hb] * 17,
        out_specs=pl.BlockSpec(memory_space=pltpu.VMEM),
        scratch_shapes=[
            pltpu.SMEM((2,), F32),
            pltpu.VMEM((16, D), BF16),
            pltpu.VMEM((1, D), F32),
            pltpu.VMEM((WIDTH, 256), F32),
            pltpu.VMEM((1, 256), F32),
            pltpu.VMEM((1, 256), F32),
            pltpu.VMEM((1, 256), F32),
            pltpu.VMEM((1, 512), F32),
            pltpu.VMEM((64, D), BF16),
            pltpu.VMEM((D, 256), BF16),
            pltpu.VMEM((D, 256), BF16),
            pltpu.VMEM((D, 256), BF16),
            pltpu.VMEM((D, 256), BF16),
            pltpu.VMEM((D, 256), BF16),
            pltpu.VMEM((D, 512), BF16),
            pltpu.VMEM((D, 512), BF16),
            pltpu.VMEM((256, D), BF16),
            pltpu.VMEM((1024, 512), BF16),
            pltpu.VMEM((NZ, 128, 128), BF16),
            pltpu.VMEM((NZ, 128, 128), BF16),
            pltpu.VMEM((64, 128), BF16),
            pltpu.VMEM((64, 128), BF16),
            pltpu.VMEM((NX * 128, 128), BF16),
            pltpu.VMEM((64, 128), BF16),
            pltpu.VMEM((NZ, NX * 128, 128), F32),
            pltpu.VMEM((NZ, NX * 128, 128), BF16),
            pltpu.VMEM((NZ, NX * 128), F32),
            pltpu.VMEM((NX, NZ, NX * 128), F32),
            pltpu.VMEM((NX, 128, NZ), F32),
            pltpu.VMEM((128, 128), F32),
            pltpu.VMEM((NX, 128, 128), BF16),
            pltpu.VMEM((NX, 128, 128), BF16),
            pltpu.VMEM((256, 128), BF16),
            pltpu.VMEM((32, 256), BF16),
            pltpu.VMEM((32, 256), BF16),
            pltpu.VMEM((96, 256), F32),
            pltpu.VMEM((NY, 64, 512), BF16),
            pltpu.VMEM((NY, 64, 512), BF16),
            pltpu.VMEM((64, 128), F32),
            pltpu.VMEM((NY, 64, 128), F32),
            pltpu.VMEM((64, 256), F32),
            pltpu.VMEM((2, 64, 512), F32),
            pltpu.VMEM((128, 128), BF16),
            pltpu.VMEM((64, 1024), BF16),
            pltpu.VMEM((8, 128), F32),
            pltpu.VMEM((NY, 8, 128), F32),
            dma((9,)), dma((8,)),
            dma, dma,
            dma, dma,
            dma((7,)), dma((16,)),
            dma, dma,
            dma, dma,
            dma((2,)), dma((2,)),
            pltpu.SemaphoreType.REGULAR((8,)),
            dma, dma,
            dma, dma, dma, dma,
            dma, dma,
            dma, dma,
            dma, dma,
            dma, dma,
        ],
        compiler_params=pltpu.CompilerParams(
            collective_id=0, has_side_effects=True, vmem_limit_bytes=40 * 1024 * 1024
        ),
    )(*(pltpu.with_memory_space_constraint(a, pltpu.HBM) for a in args))


def solution(mesh):
    torus = Mesh(mesh.devices.reshape(NZ, NX, 2, NY), ("z", "x", "c", "y"))
    every = ("z", "x", "c", "y")
    cols = P(None, "y")
    return jax.shard_map(
        on_device,
        mesh=torus,
        in_specs=(
            P(every, None), P(), cols, cols, cols, P("y"), cols, cols, cols, cols, cols,
            P("y"), P("y"), P("y"), P("y", None), P("y", None), P("y"),
        ),
        out_specs=P(("z", "x", "c"), "y"),
        check_vma=False,
    )
```

```python
import functools
import math

import jax
import jax.numpy as jnp
from jax import lax
from jax.experimental import pallas as pl
from jax.experimental.pallas import tpu as pltpu
from jax.sharding import Mesh
from jax.sharding import PartitionSpec as P

D = 2048
HD = 128
CONV_CH = 1024
WIDTH = 31
EPS = 1e-06
MESH = pl.DeviceIdType.MESH
F32 = jnp.float32
BF16 = jnp.bfloat16
NX = 4
NZ = 8
NY = 4
NCHIP = NX * NZ


STEPS = (2, 1)
WRAPS = (7, 6, 5)
GREETED = STEPS + WRAPS


def dot(a, b):
    return jnp.dot(a, b, preferred_element_type=F32)


def dot_nt(a, b):
    return lax.dot_general(a, b, (((1,), (1,)), ((), ())), preferred_element_type=F32)


def sigmoid(v):
    return jax.nn.sigmoid(v)


(C_K0, C_V0, C_Q0, C_A, C_B, C_GA, C_GC, C_CO, C_AO, C_K1, C_V1, C_Q1) = range(12)
SHARED = {C_K1: C_K0, C_V1: C_V0, C_Q1: C_Q0}


def kernel(
    hidden_hbm, pre_gain_hbm, w_query, w_key, w_value, offset_hbm, w_a, w_b, w_ga, w_gc,
    taps_hbm, bias_hbm, ngain_hbm, nshift_hbm, w_ao, w_co, post_gain_hbm,
    out,
    offset, hidden, pre_gain, taps, bias, ngain, nshift, post_gain, hbuf, wk, wv, wq, wa, wb, wga, wgc, wco, wo,
    kbuf, vbuf, kst, vst, qbuf, qst, obuf, stk, tbl, tblr, wbuf, own, ps, pr, tri,
    gst, halo, gbuf, cst, crx, stx, srx, convb, gateb, att, abuf, ssx, ssr,
    lsem, ssem, h_s, h_r, p_s, p_r, z_s, z_r, q_s, q_r, t_s, t_r, o_s, o_r, ready, halo_s, halo_r,
    w_s, w_r, v_s, v_r, st_s, st_r, c_s, c_r, a_s, a_r, ss_s, ss_r,
):
    z = lax.axis_index("z")
    x = lax.axis_index("x")
    c = lax.axis_index("c")
    y = lax.axis_index("y")
    chip = z * NX + x
    oc = 1 - c

    def dev(zz=z, xx=x, cc=c, yy=y):
        return (zz, xx, cc, yy)

    def ypeer(d):
        return lax.rem(y + d, NY)

    def xpeer(d):
        return lax.rem(x + d, NX)

    def zpeer(d):
        return lax.rem(z + d + NZ, NZ)

    def rc(src, dst, ss, rs, to):
        return pltpu.make_async_remote_copy(
            src_ref=src, dst_ref=dst, send_sem=ss, recv_sem=rs, device_id=to, device_id_type=MESH
        )

    half = pl.ds(pl.multiple_of(c * HD, HD), HD)

    def whalf(yy, cc):
        return pl.ds(pl.multiple_of(yy * 256 + cc * HD, HD), HD)

    def start(copy):
        copy.start()

    def came(whole, group):
        rc(whole, whole, group[0], group[1], dev(cc=oc)).wait_recv()

    def gone(whole, group):
        rc(whole, whole, group[0], group[1], dev(cc=oc)).wait_send()

    all_h = hbuf.at[0:48, :], (h_s, h_r)
    all_p = qbuf.at[0:128, :], (p_s, p_r)
    all_q = qbuf.at[0:448, :], (q_s, q_r)
    all_t = tblr.at[0:3], (t_s, t_r)
    all_o = [(pr.at[0:3, i * 64 : (i + 1) * 64], (o_s.at[i], o_r.at[i])) for i in (0, 1)]
    all_w = wo.at[0:384, :], (w_s, w_r)
    all_v = wo.at[0:384, :], (v_s, v_r)
    all_st = srx.at[0:3], (st_s, st_r)
    all_c = crx.at[0:3], (c_s, c_r)
    all_a = abuf.at[:, 0:896], (a_s, a_r)
    all_ss = ssr.at[0:3], (ss_s, ss_r)

    own_cols = pl.ds(pl.multiple_of(c * HD, HD), HD)
    oth_cols = pl.ds(pl.multiple_of(oc * HD, HD), HD)
    lo, hi = pl.ds(0, HD), pl.ds(HD, HD)
    ycols = pl.ds(pl.multiple_of(y * 512, 512), 512)
    yrows = pl.ds(pl.multiple_of(y * 256, 256), 256)
    local = {
        C_K1: (w_key.at[:, oth_cols], wk.at[:, lo]),
        C_K0: (w_key.at[:, own_cols], wk.at[:, hi]),
        C_V1: (w_value.at[:, oth_cols], wv.at[:, lo]),
        C_V0: (w_value.at[:, own_cols], wv.at[:, hi]),
        C_Q1: (w_query.at[:, oth_cols], wq.at[:, hi]),
        C_Q0: (w_query.at[:, own_cols], wq.at[:, lo]),
        C_A: (w_a, wa),
        C_B: (w_b, wb),
        C_GA: (w_ga, wga),
        C_GC: (w_gc, wgc),
        C_CO: (w_co, wco),
        C_AO: (w_ao.at[:, ycols], wo.at[yrows, :]),
    }
    local = {k: pltpu.make_async_copy(s, d, lsem.at[SHARED.get(k, k)]) for k, (s, d) in local.items()}
    first_in = [(hidden_hbm, hidden), (pre_gain_hbm, pre_gain)]
    later_in = [
        (taps_hbm, taps), (bias_hbm, bias), (ngain_hbm, ngain), (nshift_hbm, nshift), (post_gain_hbm, post_gain),
        (offset_hbm, offset),
    ]
    small = [
        pltpu.make_async_copy(a, b, ssem.at[i]) for i, (a, b) in enumerate(first_in + later_in)
    ]
    for copy in small[:2]:
        copy.start()

    barrier = pltpu.get_barrier_semaphore()
    next_chip = lax.rem(chip + 1, NCHIP)
    prev_chip = lax.rem(chip + NCHIP - 1, NCHIP)
    pair_chip = c * next_chip + oc * prev_chip
    pz, px = pair_chip // NX, lax.rem(pair_chip, NX)
    greet = [dev(yy=ypeer(d)) for d in (1, 2, 3)]
    greet += [dev(cc=oc, yy=ypeer(d)) for d in (0, 1, 2, 3)]
    greet += [dev(xx=xpeer(d), cc=cc) for d in (1, 2, 3) for cc in (c, oc)]
    for peer in greet:
        pl.semaphore_signal(barrier, inc=1, device_id=peer, device_id_type=MESH)
    greeted = len(greet)
    for k in GREETED:
        @pl.when(z + k < NZ)
        def _():
            for cc in (c, oc) if k in STEPS else (c,):
                pl.semaphore_signal(barrier, inc=1, device_id=dev(zz=zpeer(k), cc=cc), device_id_type=MESH)

        greeted = greeted + jnp.where(z >= k, 2 if k in STEPS else 1, 0)
    next_core = (pz, px, oc, y)
    has_next = (c == 1) & (chip < NCHIP - 1)
    has_prev = (c == 0) & (chip > 0)

    @pl.when(has_next)
    def _():
        pl.semaphore_signal(barrier, inc=1, device_id=next_core, device_id_type=MESH)

    greeted = greeted + jnp.where(has_prev, 1, 0)

    for copy in small[:2]:
        copy.wait()

    hv = hidden[...].astype(F32)
    inv = lax.rsqrt(jnp.mean(hv * hv, axis=1, keepdims=True) + EPS)
    my16 = pl.ds(pl.multiple_of(y * 16, 16), 16)
    hbuf[my16, :] = (hv * inv * pre_gain[...]).astype(BF16)

    pl.semaphore_wait(barrier, greeted)
    for k in GREETED:
        @pl.when(z >= k)
        def _():
            for cc in (c, oc) if k in STEPS else (c,):
                pl.semaphore_signal(ready.at[k], inc=1, device_id=dev(zz=zpeer(-k), cc=cc), device_id_type=MESH)

    @pl.when(has_prev)
    def _():
        pl.semaphore_signal(ready.at[0], inc=1, device_id=next_core, device_id_type=MESH)


    for d in (2, 1, 3):
        start(rc(hbuf.at[my16, :], hbuf.at[my16, :], h_s, h_r, dev(yy=ypeer(d))))
    for copy in local.values():
        copy.start()
    for copy in small[2:]:
        copy.start()

    r2 = lax.broadcasted_iota(jnp.int32, (2 * HD, HD), 0) % HD
    c2 = lax.broadcasted_iota(jnp.int32, (2 * HD, HD), 1)
    tri[...] = jnp.where(r2 > c2, 1.0, 0.0).astype(BF16)
    obuf[...] = jnp.zeros(obuf.shape, F32)
    tbl[...] = jnp.zeros(tbl.shape, F32)
    came(*all_h)

    def send_shard(d):
        yy = ypeer(d)
        cols = pl.ds(pl.multiple_of(yy * 512, 512), 512)
        start(rc(w_ao.at[half, cols], wo.at[whalf(y, c), :], w_s, w_r, dev(yy=yy)))

    send_shard(1)
    send_shard(3)

    my64 = pl.ds(pl.multiple_of(c * 64, 64), 64)
    oth64 = pl.ds(pl.multiple_of(oc * 64, 64), 64)
    partner = dev(cc=oc)
    tables = (kbuf, vbuf)

    def z_own(h, i):
        step = STEPS[i]

        @pl.when(z < NZ - step)
        def _():
            if h == 0:
                pl.semaphore_wait(ready.at[step], 2)
            mine, there = tables[h].at[z, my64, :], z_r.at[h * NZ + z]
            rc(mine, mine, z_s.at[i], there, dev(zz=zpeer(step))).start()
            rc((kst, vst)[h], mine, z_s.at[i], there, dev(zz=zpeer(step), cc=oc)).start()

    for h, (w, st, name) in enumerate(((wk, kst, C_K0), (wv, vst, C_V0))):
        pltpu.make_async_copy(w, w, lsem.at[name]).wait()
        both = dot(hbuf[...], w[...]).astype(BF16)
        st[...] = both[:, :HD]
        start(rc(st, tables[h].at[z, my64, :], p_s, p_r, partner))
        tables[h][z, my64, :] = both[:, HD:]
        z_own(h, 0)
        if h == 0:
            z_own(h, 1)

    def z_copy(h, row, i, step):
        t = tables[h].at[row]
        return rc(t, t, z_s.at[i], z_r.at[h * NZ + row], dev(zz=zpeer(step)))

    pltpu.make_async_copy(wq, wq, lsem.at[C_Q0]).wait()
    qv = dot(hbuf[...], wq[...]).astype(BF16)
    qst[...] = qv[:, HD:]

    def qrows(xx, cc):
        return pl.ds(pl.multiple_of(xx * HD + cc * 64, 64), 64)

    mine = qbuf.at[qrows(x, c), :]
    qbuf[qrows(x, c), :] = qv[:, :HD]
    for d in range(NX):
        start(rc(qst, mine, q_s, q_r, dev(xx=xpeer(d), cc=oc)))
        if d > 0:
            start(rc(mine, mine, q_s, q_r, dev(xx=xpeer(d))))

    local[C_A].wait()
    local[C_B].wait()
    left = dot(hbuf[...], wa[...]).astype(BF16).astype(F32)
    right = dot(hbuf[...], wb[...]).astype(BF16).astype(F32)
    gated = (left * sigmoid(right)).astype(BF16)
    gst[...] = gated[32:, :]
    gbuf[32:, :] = gated.astype(F32)
    halo_to = ((next_chip // NX) * c + z * oc, lax.rem(next_chip, NX) * c + x * oc, oc, y)

    @pl.when(has_next)
    def _():
        pl.semaphore_wait(ready.at[0], 1)

    has_halo = (c == 1) | (chip > 0)
    sends_halo = (c == 0) | (chip < NCHIP - 1)

    @pl.when(sends_halo)
    def _():
        rc(gst, halo, halo_s, halo_r, halo_to).start()

    came(*all_p)

    for i, k in enumerate(WRAPS):
        @pl.when(z + k < NZ)
        def _():
            pl.semaphore_wait(ready.at[k], 1)
            for h in (0, 1):
                z_copy(h, z, 4 + i, k).start()

    def arrived(h, k):
        row = zpeer(-k)
        z_copy(h, row, 0, 1).wait_recv()

    def relay(h):
        @pl.when((z >= 2) & (z < NZ - 1))
        def _():
            arrived(h, 2)
            for i, step in enumerate(STEPS):
                @pl.when(z < NZ - step)
                def _():
                    z_copy(h, zpeer(-2), 2 + i, step).start()

    relay(0)
    z_own(1, 1)
    small[7].wait()
    off = offset[c]
    scale = 1.0 / math.sqrt(HD)

    def come(h, k):
        if k == 2:
            pl.when(z == NZ - 1)(functools.partial(arrived, h, k))
        elif k > 0:
            arrived(h, k)

    def some_blocks(ks):
        for k in ks:
            come(0, k)
        fronts = []
        for k in ks:
            row = zpeer(-k)
            for b in range(NX):
                s = dot_nt(qbuf[b * HD : (b + 1) * HD, :], kbuf[row]) * scale + off
                u = jnp.exp(-jnp.abs(s))
                one = 1.0 + u
                tail = jnp.log(one) + (u - (one - 1.0))
                soft = jnp.maximum(s, 0.0) + tail
                logit = s - soft
                if k == 0:
                    rows = lax.broadcasted_iota(jnp.int32, (HD, HD), 0) + b * HD
                    cols = lax.broadcasted_iota(jnp.int32, (HD, HD), 1) + x * HD
                    soft = jnp.where(cols < rows, soft, 0.0)
                    logit = jnp.where(cols < rows, logit, -jnp.inf)
                top = soft.astype(BF16)
                rest = (soft - top.astype(F32)).astype(BF16)
                fronts.append((k, row, b, logit, jnp.concatenate([top, rest], axis=1)))
        sums = [dot(f[4], tri[...]) for f in fronts]
        ones = jnp.ones((NZ, 2 * HD), BF16)
        for k, row, b, _, pair in fronts:
            here = lax.broadcasted_iota(jnp.int32, (NZ, HD), 0) == row
            cols = slice(b * HD, (b + 1) * HD)
            tbl[:, cols] = jnp.where(here, dot_nt(ones, pair), tbl[:, cols])
        for (k, row, b, logit, _), t in zip(fronts, sums):
            stk[k, b * HD : (b + 1) * HD, :] = jnp.exp(logit - t).astype(BF16)

    def blocks(low, high):
        pl.when(z >= high)(functools.partial(some_blocks, (low, high)))
        pl.when((z >= low) & (z < high))(functools.partial(some_blocks, (low,)))

    @pl.when(has_halo)
    def _():
        rc(gst, halo, halo_s, halo_r, halo_to).wait_recv()
        gbuf[0:32, :] = halo[...].astype(F32)

    @pl.when(jnp.logical_not(has_halo))
    def _():
        gbuf[0:32, :] = jnp.zeros((32, 256), F32)

    for copy in small[2:7]:
        copy.wait()
    conv = jnp.broadcast_to(bias[...], (64, 256))
    for i in range(WIDTH):
        conv = conv + taps[i : i + 1, :] * gbuf[2 + i : 66 + i, :]
    local_mean = jnp.mean(conv, axis=1, keepdims=True)
    dev_local = conv - local_mean
    local_m2 = jnp.sum(dev_local * dev_local, axis=1, keepdims=True)
    lane = lax.broadcasted_iota(jnp.int32, (64, HD), 1)
    stx[...] = jnp.where(lane < 64, local_mean, local_m2)
    for d in (2, 1, 3):
        start(rc(stx, srx.at[y], st_s, st_r, dev(yy=ypeer(d))))
    convb[...] = conv

    send_shard(2)
    came(*all_q)

    blocks(0, 1)
    relay(1)
    blocks(2, 7)
    @pl.when(z < NZ - 2)
    def _():
        blocks(3, 4)

    blocks(5, 6)

    @pl.when(z >= NZ - 2)
    def _():
        some_blocks((3, 4))

    for d in (2, 1, 3):
        start(rc(tbl, tblr.at[x], t_s, t_r, dev(xx=xpeer(d))))
    tblr[x] = tbl[...]

    srx[y] = stx[...]
    came(*all_st)
    stats = [srx[i] for i in range(NY)]
    means = [t[:, 0:1] for t in stats]
    mean = (means[0] + means[1] + means[2] + means[3]) * 0.25
    m2 = stats[0][:, 64:65] + stats[1][:, 64:65] + stats[2][:, 64:65] + stats[3][:, 64:65]
    for t in means:
        m2 = m2 + 256.0 * (t - mean) * (t - mean)
    cn = (convb[...] - mean) * lax.rsqrt(m2 / CONV_CH + EPS) * ngain[...] + nshift[...]
    cn = (cn * sigmoid(cn)).astype(BF16)
    local[C_CO].wait()
    for i in range(NY):
        cst[i] = dot(cn, wco[:, i * 512 : (i + 1) * 512]).astype(BF16)
    for d in (2, 1, 3):
        yy = ypeer(d)
        start(rc(cst.at[yy], crx.at[y], c_s, c_r, dev(yy=yy)))

    for k in (0, 1, 2, 7, 6, 5, 3, 4):
        @pl.when(z >= k)
        def _():
            come(1, k)
            row = zpeer(-k)
            obuf[row] = dot(stk[k], vbuf[row])

    came(*all_t)

    totals = [tblr[i] for i in range(NX)]
    row_sum = totals[0] + totals[1] + totals[2] + totals[3]
    at = lax.broadcasted_iota(jnp.int32, (NZ, NX * HD), 0)
    outside = jnp.zeros((NZ, NX * HD), F32)
    for j in range(1, NZ):
        outside = outside + jnp.where(at < j, row_sum[j : j + 1, :], 0.0)
    for i in range(1, NX):
        outside = outside + jnp.where(x < i, 1.0, 0.0) * totals[i]
    weight = jnp.exp(-outside)
    per_row = weight.T
    for b in range(NX):
        wbuf[b] = per_row[b * HD : (b + 1) * HD, :]
    for d in (2, 1, 3, 0):
        b = xpeer(d)
        per_row = wbuf[b]
        rows = pl.ds(pl.multiple_of(b * HD, HD), HD)
        acc = obuf[0, rows, :] * per_row[:, 0:1]
        for j in range(1, NZ):
            acc = acc + obuf[j, rows, :] * per_row[:, j : j + 1]
        if d > 0:
            ps[d] = acc.astype(BF16)
        else:
            own[...] = acc
    halves = [slice(i * 64, (i + 1) * 64) for i in (0, 1)]
    for i in (0, 1):
        for d in (2, 1, 3):
            start(rc(ps.at[d, halves[i]], pr.at[x, halves[i]], o_s.at[i], o_r.at[i], dev(xx=xpeer(d))))

    came(*all_w)
    for d in (2, 1, 3):
        got = wo.at[whalf(ypeer(d), c), :]
        start(rc(got, got, v_s, v_r, partner))

    local[C_GA].wait()
    local[C_GC].wait()
    gateb[0] = sigmoid(dot(hbuf[...], wga[...]).astype(BF16).astype(F32))
    gateb[1] = sigmoid(dot(hbuf[...], wgc[...]).astype(BF16).astype(F32))

    head = pl.ds(pl.multiple_of((y * 2 + c) * HD, HD), HD)
    for i, rows in enumerate(halves):
        came(*all_o[i])
        acc = own[rows, :]
        for d in (2, 1, 3):
            acc = acc + pr[xpeer(d), rows, :].astype(F32)
        att[rows, :] = acc.astype(BF16)
        for d in (2, 1, 3):
            start(rc(att.at[rows, :], abuf.at[:, head], a_s, a_r, dev(cc=i, yy=ypeer(d))))

        @pl.when(c == i)
        def _():
            abuf[:, head] = att[rows, :]

        @pl.when(c != i)
        def _():
            rc(att.at[rows, :], abuf.at[:, head], a_s, a_r, dev(cc=i)).start()

    local[C_AO].wait()
    came(*all_v)

    csum = cst[y].astype(F32)
    came(*all_c)
    for d in (2, 1, 3):
        yy = ypeer(d)
        csum = csum + crx[yy].astype(F32)
    gateb[1] = gateb[1] * csum.astype(BF16).astype(F32)

    came(*all_a)
    branch = dot(abuf[...], wo[...]).astype(BF16).astype(F32)
    merged = gateb[0] * branch + gateb[1]
    sq = merged * merged
    part = sq[:, 0:128] + sq[:, 128:256] + sq[:, 256:384] + sq[:, 384:512]
    part = jnp.concatenate([part, jnp.zeros((64, HD), F32)], axis=0).T
    ssx[...] = jnp.sum(part.reshape(16, 8, HD), axis=0)
    for d in (2, 1, 3):
        start(rc(ssx, ssr.at[y], ss_s, ss_r, dev(yy=ypeer(d))))
    total = ssx[...]
    came(*all_ss)
    for d in (2, 1, 3):
        total = total + ssr[ypeer(d)]
    total = jnp.broadcast_to(jnp.sum(total, axis=0, keepdims=True), (HD, HD)).T[:64, 0:1]
    out[...] = (merged * lax.rsqrt(total / D + EPS) * post_gain[...]).astype(BF16)

    for group in (all_h, all_p, all_q, all_t, *all_o, all_w, all_v, all_st, all_c, all_a, all_ss):
        gone(*group)
    def z_sent(i, cond):
        @pl.when(cond)
        def _():
            two = kbuf.at[0:2]
            rc(two, two, z_s.at[i], z_r.at[0], partner).wait_send()

    for i, step in enumerate(STEPS):
        z_sent(i, z < NZ - step)
        z_sent(2 + i, (z >= 2) & (z < NZ - step))
    for i, k in enumerate(WRAPS):
        z_sent(4 + i, z + k < NZ)

    @pl.when(sends_halo)
    def _():
        rc(gst, halo, halo_s, halo_r, halo_to).wait_send()


def on_device(
    hidden_in, pre_gain, w_query, w_key, w_value, stick_offset, w_glu_a, w_glu_b, w_gate_attn,
    w_gate_conv, conv_taps, conv_bias, norm_gain, norm_shift, w_attn_out, w_conv_out, post_gain,
):
    args = (
        hidden_in, pre_gain.reshape(1, -1), w_query, w_key, w_value, stick_offset, w_glu_a,
        w_glu_b, w_gate_attn, w_gate_conv, conv_taps, conv_bias.reshape(1, -1),
        norm_gain.reshape(1, -1), norm_shift.reshape(1, -1), w_attn_out, w_conv_out,
        post_gain.reshape(1, -1),
    )
    hb = pl.BlockSpec(memory_space=pl.ANY)
    dma = pltpu.SemaphoreType.DMA
    return pl.pallas_call(
        kernel,
        out_shape=jax.ShapeDtypeStruct((64, 512), BF16),
        in_specs=[hb] * 17,
        out_specs=pl.BlockSpec(memory_space=pltpu.VMEM),
        scratch_shapes=[
            pltpu.SMEM((2,), F32),
            pltpu.VMEM((16, D), BF16),
            pltpu.VMEM((1, D), F32),
            pltpu.VMEM((WIDTH, 256), F32),
            pltpu.VMEM((1, 256), F32),
            pltpu.VMEM((1, 256), F32),
            pltpu.VMEM((1, 256), F32),
            pltpu.VMEM((1, 512), F32),
            pltpu.VMEM((64, D), BF16),
            pltpu.VMEM((D, 256), BF16),
            pltpu.VMEM((D, 256), BF16),
            pltpu.VMEM((D, 256), BF16),
            pltpu.VMEM((D, 256), BF16),
            pltpu.VMEM((D, 256), BF16),
            pltpu.VMEM((D, 512), BF16),
            pltpu.VMEM((D, 512), BF16),
            pltpu.VMEM((256, D), BF16),
            pltpu.VMEM((1024, 512), BF16),
            pltpu.VMEM((NZ, 128, 128), BF16),
            pltpu.VMEM((NZ, 128, 128), BF16),
            pltpu.VMEM((64, 128), BF16),
            pltpu.VMEM((64, 128), BF16),
            pltpu.VMEM((NX * 128, 128), BF16),
            pltpu.VMEM((64, 128), BF16),
            pltpu.VMEM((NZ, NX * 128, 128), F32),
            pltpu.VMEM((NZ, NX * 128, 128), BF16),
            pltpu.VMEM((NZ, NX * 128), F32),
            pltpu.VMEM((NX, NZ, NX * 128), F32),
            pltpu.VMEM((NX, 128, NZ), F32),
            pltpu.VMEM((128, 128), F32),
            pltpu.VMEM((NX, 128, 128), BF16),
            pltpu.VMEM((NX, 128, 128), BF16),
            pltpu.VMEM((256, 128), BF16),
            pltpu.VMEM((32, 256), BF16),
            pltpu.VMEM((32, 256), BF16),
            pltpu.VMEM((96, 256), F32),
            pltpu.VMEM((NY, 64, 512), BF16),
            pltpu.VMEM((NY, 64, 512), BF16),
            pltpu.VMEM((64, 128), F32),
            pltpu.VMEM((NY, 64, 128), F32),
            pltpu.VMEM((64, 256), F32),
            pltpu.VMEM((2, 64, 512), F32),
            pltpu.VMEM((128, 128), BF16),
            pltpu.VMEM((64, 1024), BF16),
            pltpu.VMEM((8, 128), F32),
            pltpu.VMEM((NY, 8, 128), F32),
            dma((9,)), dma((8,)),
            dma, dma,
            dma, dma,
            dma((7,)), dma((16,)),
            dma, dma,
            dma, dma,
            dma((2,)), dma((2,)),
            pltpu.SemaphoreType.REGULAR((8,)),
            dma, dma,
            dma, dma, dma, dma,
            dma, dma,
            dma, dma,
            dma, dma,
            dma, dma,
        ],
        compiler_params=pltpu.CompilerParams(
            collective_id=0, has_side_effects=True, vmem_limit_bytes=40 * 1024 * 1024
        ),
    )(*(pltpu.with_memory_space_constraint(a, pltpu.HBM) for a in args))


def solution(mesh):
    torus = Mesh(mesh.devices.reshape(NZ, NX, 2, NY), ("z", "x", "c", "y"))
    every = ("z", "x", "c", "y")
    cols = P(None, "y")
    return jax.shard_map(
        on_device,
        mesh=torus,
        in_specs=(
            P(every, None), P(), cols, cols, cols, P("y"), cols, cols, cols, cols, cols,
            P("y"), P("y"), P("y"), P("y", None), P("y", None), P("y"),
        ),
        out_specs=P(("z", "x", "c"), "y"),
        check_vma=False,
    )
```

```python
import functools
import math

import jax
import jax.numpy as jnp
from jax import lax
from jax.experimental import pallas as pl
from jax.experimental.pallas import tpu as pltpu
from jax.sharding import Mesh
from jax.sharding import PartitionSpec as P

D = 2048
HD = 128
CONV_CH = 1024
WIDTH = 31
EPS = 1e-06
MESH = pl.DeviceIdType.MESH
F32 = jnp.float32
BF16 = jnp.bfloat16
NX = 4
NZ = 8
NY = 4
NCHIP = NX * NZ


STEPS = (2, 1)
WRAPS = (5, 6, 7)
GREETED = STEPS + WRAPS


def dot(a, b):
    return jnp.dot(a, b, preferred_element_type=F32)


def dot_nt(a, b):
    return lax.dot_general(a, b, (((1,), (1,)), ((), ())), preferred_element_type=F32)


def sigmoid(v):
    return jax.nn.sigmoid(v)


(C_K0, C_V0, C_Q0, C_A, C_B, C_GA, C_GC, C_CO, C_AO, C_K1, C_V1, C_Q1) = range(12)
SHARED = {C_K1: C_K0, C_V1: C_V0, C_Q1: C_Q0}


def kernel(
    hidden_hbm, pre_gain_hbm, w_query, w_key, w_value, offset_hbm, w_a, w_b, w_ga, w_gc,
    taps_hbm, bias_hbm, ngain_hbm, nshift_hbm, w_ao, w_co, post_gain_hbm,
    out,
    offset, hidden, pre_gain, taps, bias, ngain, nshift, post_gain, hbuf, wk, wv, wq, wa, wb, wga, wgc, wco, wo,
    kbuf, vbuf, kst, vst, qbuf, qst, obuf, stk, tbl, tblr, wbuf, own, ps, pr, tri,
    gst, halo, gbuf, cst, crx, stx, srx, convb, gateb, att, abuf, ssx, ssr,
    lsem, ssem, h_s, h_r, p_s, p_r, z_s, z_r, q_s, q_r, t_s, t_r, o_s, o_r, ready, halo_s, halo_r,
    w_s, w_r, v_s, v_r, st_s, st_r, c_s, c_r, a_s, a_r, ss_s, ss_r,
):
    z = lax.axis_index("z")
    x = lax.axis_index("x")
    c = lax.axis_index("c")
    y = lax.axis_index("y")
    chip = z * NX + x
    oc = 1 - c

    def dev(zz=z, xx=x, cc=c, yy=y):
        return (zz, xx, cc, yy)

    def ypeer(d):
        return lax.rem(y + d, NY)

    def xpeer(d):
        return lax.rem(x + d, NX)

    def zpeer(d):
        return lax.rem(z + d + NZ, NZ)

    def rc(src, dst, ss, rs, to):
        return pltpu.make_async_remote_copy(
            src_ref=src, dst_ref=dst, send_sem=ss, recv_sem=rs, device_id=to, device_id_type=MESH
        )

    half = pl.ds(pl.multiple_of(c * HD, HD), HD)

    def whalf(yy, cc):
        return pl.ds(pl.multiple_of(yy * 256 + cc * HD, HD), HD)

    def start(copy):
        copy.start()

    def came(whole, group):
        rc(whole, whole, group[0], group[1], dev(cc=oc)).wait_recv()

    def gone(whole, group):
        rc(whole, whole, group[0], group[1], dev(cc=oc)).wait_send()

    all_h = hbuf.at[0:48, :], (h_s, h_r)
    all_p = qbuf.at[0:128, :], (p_s, p_r)
    all_q = qbuf.at[0:448, :], (q_s, q_r)
    all_t = tblr.at[0:3], (t_s, t_r)
    all_o = [(pr.at[0:3, i * 64 : (i + 1) * 64], (o_s.at[i], o_r.at[i])) for i in (0, 1)]
    all_w = wo.at[0:384, :], (w_s, w_r)
    all_v = wo.at[0:384, :], (v_s, v_r)
    all_st = srx.at[0:3], (st_s, st_r)
    all_c = crx.at[0:3], (c_s, c_r)
    all_a = abuf.at[:, 0:896], (a_s, a_r)
    all_ss = ssr.at[0:3], (ss_s, ss_r)

    own_cols = pl.ds(pl.multiple_of(c * HD, HD), HD)
    oth_cols = pl.ds(pl.multiple_of(oc * HD, HD), HD)
    lo, hi = pl.ds(0, HD), pl.ds(HD, HD)
    ycols = pl.ds(pl.multiple_of(y * 512, 512), 512)
    yrows = pl.ds(pl.multiple_of(y * 256, 256), 256)
    local = {
        C_K1: (w_key.at[:, oth_cols], wk.at[:, lo]),
        C_K0: (w_key.at[:, own_cols], wk.at[:, hi]),
        C_V1: (w_value.at[:, oth_cols], wv.at[:, lo]),
        C_V0: (w_value.at[:, own_cols], wv.at[:, hi]),
        C_Q1: (w_query.at[:, oth_cols], wq.at[:, hi]),
        C_Q0: (w_query.at[:, own_cols], wq.at[:, lo]),
        C_A: (w_a, wa),
        C_B: (w_b, wb),
        C_GA: (w_ga, wga),
        C_GC: (w_gc, wgc),
        C_CO: (w_co, wco),
        C_AO: (w_ao.at[:, ycols], wo.at[yrows, :]),
    }
    local = {k: pltpu.make_async_copy(s, d, lsem.at[SHARED.get(k, k)]) for k, (s, d) in local.items()}
    first_in = [(hidden_hbm, hidden), (pre_gain_hbm, pre_gain)]
    later_in = [
        (taps_hbm, taps), (bias_hbm, bias), (ngain_hbm, ngain), (nshift_hbm, nshift), (post_gain_hbm, post_gain),
        (offset_hbm, offset),
    ]
    small = [
        pltpu.make_async_copy(a, b, ssem.at[i]) for i, (a, b) in enumerate(first_in + later_in)
    ]
    for copy in small[:2]:
        copy.start()

    barrier = pltpu.get_barrier_semaphore()
    next_chip = lax.rem(chip + 1, NCHIP)
    prev_chip = lax.rem(chip + NCHIP - 1, NCHIP)
    pair_chip = c * next_chip + oc * prev_chip
    pz, px = pair_chip // NX, lax.rem(pair_chip, NX)
    greet = [dev(yy=ypeer(d)) for d in (1, 2, 3)]
    greet += [dev(cc=oc, yy=ypeer(d)) for d in (0, 1, 2, 3)]
    greet += [dev(xx=xpeer(d), cc=cc) for d in (1, 2, 3) for cc in (c, oc)]
    for peer in greet:
        pl.semaphore_signal(barrier, inc=1, device_id=peer, device_id_type=MESH)
    greeted = len(greet)
    for k in GREETED:
        @pl.when(z + k < NZ)
        def _():
            for cc in (c, oc) if k in STEPS else (c,):
                pl.semaphore_signal(barrier, inc=1, device_id=dev(zz=zpeer(k), cc=cc), device_id_type=MESH)

        greeted = greeted + jnp.where(z >= k, 2 if k in STEPS else 1, 0)
    next_core = (pz, px, oc, y)
    has_next = (c == 1) & (chip < NCHIP - 1)
    has_prev = (c == 0) & (chip > 0)

    @pl.when(has_next)
    def _():
        pl.semaphore_signal(barrier, inc=1, device_id=next_core, device_id_type=MESH)

    greeted = greeted + jnp.where(has_prev, 1, 0)

    for copy in small[:2]:
        copy.wait()

    hv = hidden[...].astype(F32)
    inv = lax.rsqrt(jnp.mean(hv * hv, axis=1, keepdims=True) + EPS)
    my16 = pl.ds(pl.multiple_of(y * 16, 16), 16)
    hbuf[my16, :] = (hv * inv * pre_gain[...]).astype(BF16)

    pl.semaphore_wait(barrier, greeted)
    for k in GREETED:
        @pl.when(z >= k)
        def _():
            for cc in (c, oc) if k in STEPS else (c,):
                pl.semaphore_signal(ready.at[k], inc=1, device_id=dev(zz=zpeer(-k), cc=cc), device_id_type=MESH)

    @pl.when(has_prev)
    def _():
        pl.semaphore_signal(ready.at[0], inc=1, device_id=next_core, device_id_type=MESH)


    for d in (2, 1, 3):
        start(rc(hbuf.at[my16, :], hbuf.at[my16, :], h_s, h_r, dev(yy=ypeer(d))))
    for copy in local.values():
        copy.start()
    for copy in small[2:]:
        copy.start()

    r2 = lax.broadcasted_iota(jnp.int32, (2 * HD, HD), 0) % HD
    c2 = lax.broadcasted_iota(jnp.int32, (2 * HD, HD), 1)
    tri[...] = jnp.where(r2 > c2, 1.0, 0.0).astype(BF16)
    obuf[...] = jnp.zeros(obuf.shape, F32)
    tbl[...] = jnp.zeros(tbl.shape, F32)
    came(*all_h)

    def send_shard(d):
        yy = ypeer(d)
        cols = pl.ds(pl.multiple_of(yy * 512, 512), 512)
        start(rc(w_ao.at[half, cols], wo.at[whalf(y, c), :], w_s, w_r, dev(yy=yy)))

    send_shard(1)
    send_shard(3)

    my64 = pl.ds(pl.multiple_of(c * 64, 64), 64)
    oth64 = pl.ds(pl.multiple_of(oc * 64, 64), 64)
    partner = dev(cc=oc)
    tables = (kbuf, vbuf)

    def z_own(h, i, cond=True):
        step = STEPS[i]

        @pl.when((z < NZ - step) & cond)
        def _():
            if h == 0:
                pl.semaphore_wait(ready.at[step], 2)
            mine, there = tables[h].at[z, my64, :], z_r.at[h * NZ + z]
            rc(mine, mine, z_s.at[i], there, dev(zz=zpeer(step))).start()
            rc((kst, vst)[h], mine, z_s.at[i], there, dev(zz=zpeer(step), cc=oc)).start()

    def z_copy(h, row, i, step):
        t = tables[h].at[row]
        return rc(t, t, z_s.at[i], z_r.at[h * NZ + row], dev(zz=zpeer(step)))

    def project(h):
        w, st, name = ((wk, kst, C_K0), (wv, vst, C_V0))[h]
        pltpu.make_async_copy(w, w, lsem.at[name]).wait()
        both = dot(hbuf[...], w[...]).astype(BF16)
        st[...] = both[:, :HD]
        start(rc(st, tables[h].at[z, my64, :], p_s, p_r, partner))
        tables[h][z, my64, :] = both[:, HD:]
        if h == 0:
            z_own(h, 0)
            z_own(h, 1)
        else:
            z_own(h, 0, c == 0)

    project(0)
    pltpu.make_async_copy(wq, wq, lsem.at[C_Q0]).wait()
    qv = dot(hbuf[...], wq[...]).astype(BF16)
    qst[...] = qv[:, HD:]

    def qrows(xx, cc):
        return pl.ds(pl.multiple_of(xx * HD + cc * 64, 64), 64)

    mine = qbuf.at[qrows(x, c), :]
    qbuf[qrows(x, c), :] = qv[:, :HD]
    for d in range(NX):
        start(rc(qst, mine, q_s, q_r, dev(xx=xpeer(d), cc=oc)))
        if d > 0:
            start(rc(mine, mine, q_s, q_r, dev(xx=xpeer(d))))

    project(1)
    local[C_A].wait()
    local[C_B].wait()
    left = dot(hbuf[...], wa[...]).astype(BF16).astype(F32)
    right = dot(hbuf[...], wb[...]).astype(BF16).astype(F32)
    gated = (left * sigmoid(right)).astype(BF16)
    gst[...] = gated[32:, :]
    gbuf[32:, :] = gated.astype(F32)
    halo_to = ((next_chip // NX) * c + z * oc, lax.rem(next_chip, NX) * c + x * oc, oc, y)

    @pl.when(has_next)
    def _():
        pl.semaphore_wait(ready.at[0], 1)

    has_halo = (c == 1) | (chip > 0)
    sends_halo = (c == 0) | (chip < NCHIP - 1)

    @pl.when(sends_halo)
    def _():
        rc(gst, halo, halo_s, halo_r, halo_to).start()

    came(*all_p)

    def wrap(h):
        for i, k in enumerate(WRAPS):
            @pl.when(z + k < NZ)
            def _():
                if h == 0:
                    pl.semaphore_wait(ready.at[k], 1)
                z_copy(h, z, 4 + i, k).start()

    wrap(0)

    def arrived(h, k):
        row = zpeer(-k)
        z_copy(h, row, 0, 1).wait_recv()

    def relay(h, low=2, high=NZ - 1):
        @pl.when((z >= low) & (z < high))
        def _():
            arrived(h, 2)
            for i, step in enumerate(STEPS):
                @pl.when(z < NZ - step)
                def _():
                    z_copy(h, zpeer(-2), 2 + i, step).start()

    relay(0)
    z_own(1, 0, c == 1)
    z_own(1, 1)
    small[7].wait()
    off = offset[c]
    scale = 1.0 / math.sqrt(HD)

    def come(h, k):
        if k == 2:
            pl.when(z == NZ - 1)(functools.partial(arrived, h, k))
        elif k > 0:
            arrived(h, k)

    def some_blocks(ks):
        for k in ks:
            come(0, k)
        fronts = []
        for k in ks:
            row = zpeer(-k)
            for b in range(NX):
                s = dot_nt(qbuf[b * HD : (b + 1) * HD, :], kbuf[row]) * scale + off
                u = jnp.exp(-jnp.abs(s))
                one = 1.0 + u
                tail = jnp.log(one) + (u - (one - 1.0))
                soft = jnp.maximum(s, 0.0) + tail
                logit = s - soft
                if k == 0:
                    rows = lax.broadcasted_iota(jnp.int32, (HD, HD), 0) + b * HD
                    cols = lax.broadcasted_iota(jnp.int32, (HD, HD), 1) + x * HD
                    soft = jnp.where(cols < rows, soft, 0.0)
                    logit = jnp.where(cols < rows, logit, -jnp.inf)
                top = soft.astype(BF16)
                rest = (soft - top.astype(F32)).astype(BF16)
                fronts.append((k, row, b, logit, jnp.concatenate([top, rest], axis=1)))
        sums = [dot(f[4], tri[...]) for f in fronts]
        ones = jnp.ones((NZ, 2 * HD), BF16)
        for k, row, b, _, pair in fronts:
            here = lax.broadcasted_iota(jnp.int32, (NZ, HD), 0) == row
            cols = slice(b * HD, (b + 1) * HD)
            tbl[:, cols] = jnp.where(here, dot_nt(ones, pair), tbl[:, cols])
        for (k, row, b, logit, _), t in zip(fronts, sums):
            stk[k, b * HD : (b + 1) * HD, :] = jnp.exp(logit - t).astype(BF16)

    def blocks(low, high):
        pl.when(z >= high)(functools.partial(some_blocks, (low, high)))
        pl.when((z >= low) & (z < high))(functools.partial(some_blocks, (low,)))

    @pl.when(has_halo)
    def _():
        rc(gst, halo, halo_s, halo_r, halo_to).wait_recv()
        gbuf[0:32, :] = halo[...].astype(F32)

    @pl.when(jnp.logical_not(has_halo))
    def _():
        gbuf[0:32, :] = jnp.zeros((32, 256), F32)

    for copy in small[2:7]:
        copy.wait()
    conv = jnp.broadcast_to(bias[...], (64, 256))
    for i in range(WIDTH):
        conv = conv + taps[i : i + 1, :] * gbuf[2 + i : 66 + i, :]
    local_mean = jnp.mean(conv, axis=1, keepdims=True)
    dev_local = conv - local_mean
    local_m2 = jnp.sum(dev_local * dev_local, axis=1, keepdims=True)
    lane = lax.broadcasted_iota(jnp.int32, (64, HD), 1)
    stx[...] = jnp.where(lane < 64, local_mean, local_m2)
    for d in (2, 1, 3):
        start(rc(stx, srx.at[y], st_s, st_r, dev(yy=ypeer(d))))
    convb[...] = conv

    send_shard(2)
    wrap(1)
    came(*all_q)

    blocks(0, 1)
    @pl.when((z >= 2) & (z < 5))
    def _():
        some_blocks((2,))

    @pl.when(z >= 5)
    def _():
        some_blocks((2, 5))

    relay(1, high=5)
    blocks(6, 7)
    blocks(3, 4)

    for d in (2, 1, 3):
        start(rc(tbl, tblr.at[x], t_s, t_r, dev(xx=xpeer(d))))
    tblr[x] = tbl[...]

    relay(1, low=5)
    srx[y] = stx[...]
    came(*all_st)
    stats = [srx[i] for i in range(NY)]
    means = [t[:, 0:1] for t in stats]
    mean = (means[0] + means[1] + means[2] + means[3]) * 0.25
    m2 = stats[0][:, 64:65] + stats[1][:, 64:65] + stats[2][:, 64:65] + stats[3][:, 64:65]
    for t in means:
        m2 = m2 + 256.0 * (t - mean) * (t - mean)
    cn = (convb[...] - mean) * lax.rsqrt(m2 / CONV_CH + EPS) * ngain[...] + nshift[...]
    cn = (cn * sigmoid(cn)).astype(BF16)
    local[C_CO].wait()
    for i in range(NY):
        cst[i] = dot(cn, wco[:, i * 512 : (i + 1) * 512]).astype(BF16)
    for d in (2, 1, 3):
        yy = ypeer(d)
        start(rc(cst.at[yy], crx.at[y], c_s, c_r, dev(yy=yy)))

    for k in (0, 1, 2, 7, 6, 5, 3, 4):
        @pl.when(z >= k)
        def _():
            come(1, k)
            row = zpeer(-k)
            obuf[row] = dot(stk[k], vbuf[row])

    came(*all_t)

    totals = [tblr[i] for i in range(NX)]
    row_sum = totals[0] + totals[1] + totals[2] + totals[3]
    at = lax.broadcasted_iota(jnp.int32, (NZ, NX * HD), 0)
    outside = jnp.zeros((NZ, NX * HD), F32)
    for j in range(1, NZ):
        outside = outside + jnp.where(at < j, row_sum[j : j + 1, :], 0.0)
    for i in range(1, NX):
        outside = outside + jnp.where(x < i, 1.0, 0.0) * totals[i]
    weight = jnp.exp(-outside)
    per_row = weight.T
    for b in range(NX):
        wbuf[b] = per_row[b * HD : (b + 1) * HD, :]
    for d in (2, 1, 3, 0):
        b = xpeer(d)
        per_row = wbuf[b]
        rows = pl.ds(pl.multiple_of(b * HD, HD), HD)
        acc = obuf[0, rows, :] * per_row[:, 0:1]
        for j in range(1, NZ):
            acc = acc + obuf[j, rows, :] * per_row[:, j : j + 1]
        if d > 0:
            ps[d] = acc.astype(BF16)
        else:
            own[...] = acc
    halves = [slice(i * 64, (i + 1) * 64) for i in (0, 1)]
    for i in (0, 1):
        for d in (2, 1, 3):
            start(rc(ps.at[d, halves[i]], pr.at[x, halves[i]], o_s.at[i], o_r.at[i], dev(xx=xpeer(d))))

    came(*all_w)
    for d in (2, 1, 3):
        got = wo.at[whalf(ypeer(d), c), :]
        start(rc(got, got, v_s, v_r, partner))

    local[C_GA].wait()
    local[C_GC].wait()
    gateb[0] = sigmoid(dot(hbuf[...], wga[...]).astype(BF16).astype(F32))
    gateb[1] = sigmoid(dot(hbuf[...], wgc[...]).astype(BF16).astype(F32))

    head = pl.ds(pl.multiple_of((y * 2 + c) * HD, HD), HD)
    for i, rows in enumerate(halves):
        came(*all_o[i])
        acc = own[rows, :]
        for d in (2, 1, 3):
            acc = acc + pr[xpeer(d), rows, :].astype(F32)
        att[rows, :] = acc.astype(BF16)
        for d in (2, 1, 3):
            start(rc(att.at[rows, :], abuf.at[:, head], a_s, a_r, dev(cc=i, yy=ypeer(d))))

        @pl.when(c == i)
        def _():
            abuf[:, head] = att[rows, :]

        @pl.when(c != i)
        def _():
            rc(att.at[rows, :], abuf.at[:, head], a_s, a_r, dev(cc=i)).start()

    local[C_AO].wait()
    came(*all_v)

    csum = cst[y].astype(F32)
    came(*all_c)
    for d in (2, 1, 3):
        yy = ypeer(d)
        csum = csum + crx[yy].astype(F32)
    gateb[1] = gateb[1] * csum.astype(BF16).astype(F32)

    came(*all_a)
    branch = dot(abuf[...], wo[...]).astype(BF16).astype(F32)
    merged = gateb[0] * branch + gateb[1]
    sq = merged * merged
    part = sq[:, 0:128] + sq[:, 128:256] + sq[:, 256:384] + sq[:, 384:512]
    part = jnp.concatenate([part, jnp.zeros((64, HD), F32)], axis=0).T
    ssx[...] = jnp.sum(part.reshape(16, 8, HD), axis=0)
    for d in (2, 1, 3):
        start(rc(ssx, ssr.at[y], ss_s, ss_r, dev(yy=ypeer(d))))
    total = ssx[...]
    came(*all_ss)
    for d in (2, 1, 3):
        total = total + ssr[ypeer(d)]
    total = jnp.broadcast_to(jnp.sum(total, axis=0, keepdims=True), (HD, HD)).T[:64, 0:1]
    out[...] = (merged * lax.rsqrt(total / D + EPS) * post_gain[...]).astype(BF16)

    for group in (all_h, all_p, all_q, all_t, *all_o, all_w, all_v, all_st, all_c, all_a, all_ss):
        gone(*group)
    def z_sent(i, cond):
        @pl.when(cond)
        def _():
            two = kbuf.at[0:2]
            rc(two, two, z_s.at[i], z_r.at[0], partner).wait_send()

    for i, step in enumerate(STEPS):
        z_sent(i, z < NZ - step)
        z_sent(2 + i, (z >= 2) & (z < NZ - step))
    for i, k in enumerate(WRAPS):
        z_sent(4 + i, z + k < NZ)

    @pl.when(sends_halo)
    def _():
        rc(gst, halo, halo_s, halo_r, halo_to).wait_send()


def on_device(
    hidden_in, pre_gain, w_query, w_key, w_value, stick_offset, w_glu_a, w_glu_b, w_gate_attn,
    w_gate_conv, conv_taps, conv_bias, norm_gain, norm_shift, w_attn_out, w_conv_out, post_gain,
):
    args = (
        hidden_in, pre_gain.reshape(1, -1), w_query, w_key, w_value, stick_offset, w_glu_a,
        w_glu_b, w_gate_attn, w_gate_conv, conv_taps, conv_bias.reshape(1, -1),
        norm_gain.reshape(1, -1), norm_shift.reshape(1, -1), w_attn_out, w_conv_out,
        post_gain.reshape(1, -1),
    )
    hb = pl.BlockSpec(memory_space=pl.ANY)
    dma = pltpu.SemaphoreType.DMA
    return pl.pallas_call(
        kernel,
        out_shape=jax.ShapeDtypeStruct((64, 512), BF16),
        in_specs=[hb] * 17,
        out_specs=pl.BlockSpec(memory_space=pltpu.VMEM),
        scratch_shapes=[
            pltpu.SMEM((2,), F32),
            pltpu.VMEM((16, D), BF16),
            pltpu.VMEM((1, D), F32),
            pltpu.VMEM((WIDTH, 256), F32),
            pltpu.VMEM((1, 256), F32),
            pltpu.VMEM((1, 256), F32),
            pltpu.VMEM((1, 256), F32),
            pltpu.VMEM((1, 512), F32),
            pltpu.VMEM((64, D), BF16),
            pltpu.VMEM((D, 256), BF16),
            pltpu.VMEM((D, 256), BF16),
            pltpu.VMEM((D, 256), BF16),
            pltpu.VMEM((D, 256), BF16),
            pltpu.VMEM((D, 256), BF16),
            pltpu.VMEM((D, 512), BF16),
            pltpu.VMEM((D, 512), BF16),
            pltpu.VMEM((256, D), BF16),
            pltpu.VMEM((1024, 512), BF16),
            pltpu.VMEM((NZ, 128, 128), BF16),
            pltpu.VMEM((NZ, 128, 128), BF16),
            pltpu.VMEM((64, 128), BF16),
            pltpu.VMEM((64, 128), BF16),
            pltpu.VMEM((NX * 128, 128), BF16),
            pltpu.VMEM((64, 128), BF16),
            pltpu.VMEM((NZ, NX * 128, 128), F32),
            pltpu.VMEM((NZ, NX * 128, 128), BF16),
            pltpu.VMEM((NZ, NX * 128), F32),
            pltpu.VMEM((NX, NZ, NX * 128), F32),
            pltpu.VMEM((NX, 128, NZ), F32),
            pltpu.VMEM((128, 128), F32),
            pltpu.VMEM((NX, 128, 128), BF16),
            pltpu.VMEM((NX, 128, 128), BF16),
            pltpu.VMEM((256, 128), BF16),
            pltpu.VMEM((32, 256), BF16),
            pltpu.VMEM((32, 256), BF16),
            pltpu.VMEM((96, 256), F32),
            pltpu.VMEM((NY, 64, 512), BF16),
            pltpu.VMEM((NY, 64, 512), BF16),
            pltpu.VMEM((64, 128), F32),
            pltpu.VMEM((NY, 64, 128), F32),
            pltpu.VMEM((64, 256), F32),
            pltpu.VMEM((2, 64, 512), F32),
            pltpu.VMEM((128, 128), BF16),
            pltpu.VMEM((64, 1024), BF16),
            pltpu.VMEM((8, 128), F32),
            pltpu.VMEM((NY, 8, 128), F32),
            dma((9,)), dma((8,)),
            dma, dma,
            dma, dma,
            dma((7,)), dma((16,)),
            dma, dma,
            dma, dma,
            dma((2,)), dma((2,)),
            pltpu.SemaphoreType.REGULAR((8,)),
            dma, dma,
            dma, dma, dma, dma,
            dma, dma,
            dma, dma,
            dma, dma,
            dma, dma,
        ],
        compiler_params=pltpu.CompilerParams(
            collective_id=0, has_side_effects=True, vmem_limit_bytes=40 * 1024 * 1024
        ),
    )(*(pltpu.with_memory_space_constraint(a, pltpu.HBM) for a in args))


def solution(mesh):
    torus = Mesh(mesh.devices.reshape(NZ, NX, 2, NY), ("z", "x", "c", "y"))
    every = ("z", "x", "c", "y")
    cols = P(None, "y")
    return jax.shard_map(
        on_device,
        mesh=torus,
        in_specs=(
            P(every, None), P(), cols, cols, cols, P("y"), cols, cols, cols, cols, cols,
            P("y"), P("y"), P("y"), P("y", None), P("y", None), P("y"),
        ),
        out_specs=P(("z", "x", "c"), "y"),
        check_vma=False,
    )
```

```python
import functools
import math

import jax
import jax.numpy as jnp
from jax import lax
from jax.experimental import pallas as pl
from jax.experimental.pallas import tpu as pltpu
from jax.sharding import Mesh
from jax.sharding import PartitionSpec as P

D = 2048
HD = 128
CONV_CH = 1024
WIDTH = 31
EPS = 1e-06
MESH = pl.DeviceIdType.MESH
F32 = jnp.float32
BF16 = jnp.bfloat16
NX = 4
NZ = 8
NY = 4
NCHIP = NX * NZ


STEPS = (2, 1)
WRAPS = (5, 6, 7)
GREETED = STEPS + WRAPS


def dot(a, b):
    return jnp.dot(a, b, preferred_element_type=F32)


def dot_nt(a, b):
    return lax.dot_general(a, b, (((1,), (1,)), ((), ())), preferred_element_type=F32)


def sigmoid(v):
    return jax.nn.sigmoid(v)


(C_K0, C_V0, C_Q0, C_A, C_B, C_GA, C_GC, C_CO, C_AO, C_K1, C_V1, C_Q1) = range(12)
SHARED = {C_K1: C_K0, C_V1: C_V0, C_Q1: C_Q0}


def kernel(
    hidden_hbm, pre_gain_hbm, w_query, w_key, w_value, offset_hbm, w_a, w_b, w_ga, w_gc,
    taps_hbm, bias_hbm, ngain_hbm, nshift_hbm, w_ao, w_co, post_gain_hbm,
    out,
    offset, hidden, pre_gain, taps, bias, ngain, nshift, post_gain, hbuf, wk, wv, wq, wa, wb, wga, wgc, wco, wo,
    kbuf, vbuf, kst, vst, qbuf, qst, obuf, stk, tbl, tblr, wbuf, own, ps, pr, tri,
    gst, halo, gbuf, cst, crx, stx, srx, convb, gateb, att, abuf, ssx, ssr,
    lsem, ssem, h_s, h_r, p_s, p_r, z_s, z_r, q_s, q_r, t_s, t_r, o_s, o_r, ready, halo_s, halo_r,
    w_s, w_r, v_s, v_r, st_s, st_r, c_s, c_r, a_s, a_r, ss_s, ss_r,
):
    z = lax.axis_index("z")
    x = lax.axis_index("x")
    c = lax.axis_index("c")
    y = lax.axis_index("y")
    chip = z * NX + x
    oc = 1 - c

    def dev(zz=z, xx=x, cc=c, yy=y):
        return (zz, xx, cc, yy)

    def ypeer(d):
        return lax.rem(y + d, NY)

    def xpeer(d):
        return lax.rem(x + d, NX)

    def zpeer(d):
        return lax.rem(z + d + NZ, NZ)

    def rc(src, dst, ss, rs, to):
        return pltpu.make_async_remote_copy(
            src_ref=src, dst_ref=dst, send_sem=ss, recv_sem=rs, device_id=to, device_id_type=MESH
        )

    half = pl.ds(pl.multiple_of(c * HD, HD), HD)

    def whalf(yy, cc):
        return pl.ds(pl.multiple_of(yy * 256 + cc * HD, HD), HD)

    def start(copy):
        copy.start()

    def came(whole, group):
        rc(whole, whole, group[0], group[1], dev(cc=oc)).wait_recv()

    def gone(whole, group):
        rc(whole, whole, group[0], group[1], dev(cc=oc)).wait_send()

    all_h = hbuf.at[0:48, :], (h_s, h_r)
    all_p = qbuf.at[0:128, :], (p_s, p_r)
    all_q = qbuf.at[0:448, :], (q_s, q_r)
    all_t = tblr.at[0:3], (t_s, t_r)
    all_o = [(pr.at[0:3, i * 64 : (i + 1) * 64], (o_s.at[i], o_r.at[i])) for i in (0, 1)]
    all_w = wo.at[0:384, :], (w_s, w_r)
    all_v = wo.at[0:384, :], (v_s, v_r)
    all_st = srx.at[0:3], (st_s, st_r)
    all_c = crx.at[0:3], (c_s, c_r)
    all_a = abuf.at[:, 0:896], (a_s, a_r)
    all_ss = ssr.at[0:3], (ss_s, ss_r)

    own_cols = pl.ds(pl.multiple_of(c * HD, HD), HD)
    oth_cols = pl.ds(pl.multiple_of(oc * HD, HD), HD)
    lo, hi = pl.ds(0, HD), pl.ds(HD, HD)
    ycols = pl.ds(pl.multiple_of(y * 512, 512), 512)
    yrows = pl.ds(pl.multiple_of(y * 256, 256), 256)
    local = {
        C_K1: (w_key.at[:, oth_cols], wk.at[:, lo]),
        C_K0: (w_key.at[:, own_cols], wk.at[:, hi]),
        C_V1: (w_value.at[:, oth_cols], wv.at[:, lo]),
        C_V0: (w_value.at[:, own_cols], wv.at[:, hi]),
        C_Q1: (w_query.at[:, oth_cols], wq.at[:, hi]),
        C_Q0: (w_query.at[:, own_cols], wq.at[:, lo]),
        C_A: (w_a, wa),
        C_B: (w_b, wb),
        C_GA: (w_ga, wga),
        C_GC: (w_gc, wgc),
        C_CO: (w_co, wco),
        C_AO: (w_ao.at[:, ycols], wo.at[yrows, :]),
    }
    local = {k: pltpu.make_async_copy(s, d, lsem.at[SHARED.get(k, k)]) for k, (s, d) in local.items()}
    first_in = [(hidden_hbm, hidden), (pre_gain_hbm, pre_gain)]
    later_in = [
        (taps_hbm, taps), (bias_hbm, bias), (ngain_hbm, ngain), (nshift_hbm, nshift), (post_gain_hbm, post_gain),
        (offset_hbm, offset),
    ]
    small = [
        pltpu.make_async_copy(a, b, ssem.at[i]) for i, (a, b) in enumerate(first_in + later_in)
    ]
    for copy in small[:2]:
        copy.start()

    barrier = pltpu.get_barrier_semaphore()
    next_chip = lax.rem(chip + 1, NCHIP)
    prev_chip = lax.rem(chip + NCHIP - 1, NCHIP)
    pair_chip = c * next_chip + oc * prev_chip
    pz, px = pair_chip // NX, lax.rem(pair_chip, NX)
    greet = [dev(yy=ypeer(d)) for d in (1, 2, 3)]
    greet += [dev(cc=oc, yy=ypeer(d)) for d in (0, 1, 2, 3)]
    greet += [dev(xx=xpeer(d), cc=cc) for d in (1, 2, 3) for cc in (c, oc)]
    for peer in greet:
        pl.semaphore_signal(barrier, inc=1, device_id=peer, device_id_type=MESH)
    greeted = len(greet)
    for k in GREETED:
        @pl.when(z + k < NZ)
        def _():
            for cc in (c, oc) if k in STEPS else (c,):
                pl.semaphore_signal(barrier, inc=1, device_id=dev(zz=zpeer(k), cc=cc), device_id_type=MESH)

        greeted = greeted + jnp.where(z >= k, 2 if k in STEPS else 1, 0)
    next_core = (pz, px, oc, y)
    has_next = (c == 1) & (chip < NCHIP - 1)
    has_prev = (c == 0) & (chip > 0)

    @pl.when(has_next)
    def _():
        pl.semaphore_signal(barrier, inc=1, device_id=next_core, device_id_type=MESH)

    greeted = greeted + jnp.where(has_prev, 1, 0)

    for copy in small[:2]:
        copy.wait()

    hv = hidden[...].astype(F32)
    inv = lax.rsqrt(jnp.mean(hv * hv, axis=1, keepdims=True) + EPS)
    my16 = pl.ds(pl.multiple_of(y * 16, 16), 16)
    hbuf[my16, :] = (hv * inv * pre_gain[...]).astype(BF16)

    pl.semaphore_wait(barrier, greeted)
    for k in GREETED:
        @pl.when(z >= k)
        def _():
            for cc in (c, oc) if k in STEPS else (c,):
                pl.semaphore_signal(ready.at[k], inc=1, device_id=dev(zz=zpeer(-k), cc=cc), device_id_type=MESH)

    @pl.when(has_prev)
    def _():
        pl.semaphore_signal(ready.at[0], inc=1, device_id=next_core, device_id_type=MESH)


    for d in (2, 1, 3):
        start(rc(hbuf.at[my16, :], hbuf.at[my16, :], h_s, h_r, dev(yy=ypeer(d))))
    for copy in local.values():
        copy.start()
    for copy in small[2:]:
        copy.start()

    r2 = lax.broadcasted_iota(jnp.int32, (2 * HD, HD), 0) % HD
    c2 = lax.broadcasted_iota(jnp.int32, (2 * HD, HD), 1)
    tri[...] = jnp.where(r2 > c2, 1.0, 0.0).astype(BF16)
    obuf[...] = jnp.zeros(obuf.shape, F32)
    tbl[...] = jnp.zeros(tbl.shape, F32)
    came(*all_h)

    def send_shard(d):
        yy = ypeer(d)
        cols = pl.ds(pl.multiple_of(yy * 512, 512), 512)
        start(rc(w_ao.at[half, cols], wo.at[whalf(y, c), :], w_s, w_r, dev(yy=yy)))

    send_shard(1)
    send_shard(3)

    my64 = pl.ds(pl.multiple_of(c * 64, 64), 64)
    oth64 = pl.ds(pl.multiple_of(oc * 64, 64), 64)
    partner = dev(cc=oc)
    tables = (kbuf, vbuf)

    def z_own(h, i, cond=True):
        step = STEPS[i]

        @pl.when((z < NZ - step) & cond)
        def _():
            if h == 0:
                pl.semaphore_wait(ready.at[step], 2)
            mine, there = tables[h].at[z, my64, :], z_r.at[h * NZ + z]
            rc(mine, mine, z_s.at[i], there, dev(zz=zpeer(step))).start()
            rc((kst, vst)[h], mine, z_s.at[i], there, dev(zz=zpeer(step), cc=oc)).start()

    def z_copy(h, row, i, step):
        t = tables[h].at[row]
        return rc(t, t, z_s.at[i], z_r.at[h * NZ + row], dev(zz=zpeer(step)))

    def project(h):
        w, st, name = ((wk, kst, C_K0), (wv, vst, C_V0))[h]
        pltpu.make_async_copy(w, w, lsem.at[name]).wait()
        both = dot(hbuf[...], w[...]).astype(BF16)
        st[...] = both[:, :HD]
        start(rc(st, tables[h].at[z, my64, :], p_s, p_r, partner))
        tables[h][z, my64, :] = both[:, HD:]
        if h == 0:
            z_own(h, 0)
            z_own(h, 1)
        else:
            z_own(h, 0, c == 0)

    project(0)
    pltpu.make_async_copy(wq, wq, lsem.at[C_Q0]).wait()
    qv = dot(hbuf[...], wq[...]).astype(BF16)
    qst[...] = qv[:, HD:]

    def qrows(xx, cc):
        return pl.ds(pl.multiple_of(xx * HD + cc * 64, 64), 64)

    mine = qbuf.at[qrows(x, c), :]
    qbuf[qrows(x, c), :] = qv[:, :HD]
    for d in range(NX):
        start(rc(qst, mine, q_s, q_r, dev(xx=xpeer(d), cc=oc)))
        if d > 0:
            start(rc(mine, mine, q_s, q_r, dev(xx=xpeer(d))))

    project(1)
    local[C_A].wait()
    local[C_B].wait()
    left = dot(hbuf[...], wa[...]).astype(BF16).astype(F32)
    right = dot(hbuf[...], wb[...]).astype(BF16).astype(F32)
    gated = (left * sigmoid(right)).astype(BF16)
    gst[...] = gated[32:, :]
    gbuf[32:, :] = gated.astype(F32)
    halo_to = ((next_chip // NX) * c + z * oc, lax.rem(next_chip, NX) * c + x * oc, oc, y)

    @pl.when(has_next)
    def _():
        pl.semaphore_wait(ready.at[0], 1)

    has_halo = (c == 1) | (chip > 0)
    sends_halo = (c == 0) | (chip < NCHIP - 1)

    @pl.when(sends_halo)
    def _():
        rc(gst, halo, halo_s, halo_r, halo_to).start()

    came(*all_p)

    def wrap(h):
        for i, k in enumerate(WRAPS):
            @pl.when(z + k < NZ)
            def _():
                if h == 0:
                    pl.semaphore_wait(ready.at[k], 1)
                z_copy(h, z, 4 + i, k).start()

    wrap(0)

    def arrived(h, k):
        row = zpeer(-k)
        z_copy(h, row, 0, 1).wait_recv()

    def relay(h, low=2, high=NZ - 1):
        @pl.when((z >= low) & (z < high))
        def _():
            arrived(h, 2)
            for i, step in enumerate(STEPS):
                @pl.when(z < NZ - step)
                def _():
                    z_copy(h, zpeer(-2), 2 + i, step).start()

    relay(0)
    z_own(1, 0, c == 1)
    z_own(1, 1)
    small[7].wait()
    off = offset[c]
    scale = 1.0 / math.sqrt(HD)

    def come(h, k):
        if k == 2:
            pl.when(z == NZ - 1)(functools.partial(arrived, h, k))
        elif k > 0:
            arrived(h, k)

    def some_blocks(ks):
        for k in ks:
            come(0, k)
        fronts = []
        for k in ks:
            row = zpeer(-k)
            for b in range(NX):
                s = dot_nt(qbuf[b * HD : (b + 1) * HD, :], kbuf[row]) * scale + off
                u = jnp.exp(-jnp.abs(s))
                one = 1.0 + u
                tail = jnp.log(one) + (u - (one - 1.0))
                soft = jnp.maximum(s, 0.0) + tail
                logit = s - soft
                if k == 0:
                    rows = lax.broadcasted_iota(jnp.int32, (HD, HD), 0) + b * HD
                    cols = lax.broadcasted_iota(jnp.int32, (HD, HD), 1) + x * HD
                    soft = jnp.where(cols < rows, soft, 0.0)
                    logit = jnp.where(cols < rows, logit, -jnp.inf)
                top = soft.astype(BF16)
                rest = (soft - top.astype(F32)).astype(BF16)
                fronts.append((k, row, b, logit, jnp.concatenate([top, rest], axis=1)))
        sums = [dot(f[4], tri[...]) for f in fronts]
        ones = jnp.ones((NZ, 2 * HD), BF16)
        for k, row, b, _, pair in fronts:
            here = lax.broadcasted_iota(jnp.int32, (NZ, HD), 0) == row
            cols = slice(b * HD, (b + 1) * HD)
            tbl[:, cols] = jnp.where(here, dot_nt(ones, pair), tbl[:, cols])
        for (k, row, b, logit, _), t in zip(fronts, sums):
            stk[k, b * HD : (b + 1) * HD, :] = jnp.exp(logit - t).astype(BF16)

    def blocks(low, high):
        pl.when(z >= high)(functools.partial(some_blocks, (low, high)))
        pl.when((z >= low) & (z < high))(functools.partial(some_blocks, (low,)))

    @pl.when(has_halo)
    def _():
        rc(gst, halo, halo_s, halo_r, halo_to).wait_recv()
        gbuf[0:32, :] = halo[...].astype(F32)

    @pl.when(jnp.logical_not(has_halo))
    def _():
        gbuf[0:32, :] = jnp.zeros((32, 256), F32)

    for copy in small[2:7]:
        copy.wait()
    conv = jnp.broadcast_to(bias[...], (64, 256))
    for i in range(WIDTH):
        conv = conv + taps[i : i + 1, :] * gbuf[2 + i : 66 + i, :]
    local_mean = jnp.mean(conv, axis=1, keepdims=True)
    dev_local = conv - local_mean
    local_m2 = jnp.sum(dev_local * dev_local, axis=1, keepdims=True)
    lane = lax.broadcasted_iota(jnp.int32, (64, HD), 1)
    stx[...] = jnp.where(lane < 64, local_mean, local_m2)
    for d in (2, 1, 3):
        start(rc(stx, srx.at[y], st_s, st_r, dev(yy=ypeer(d))))
    convb[...] = conv

    send_shard(2)
    wrap(1)
    came(*all_q)

    blocks(0, 1)
    @pl.when((z >= 2) & (z < 5))
    def _():
        some_blocks((2,))

    @pl.when(z >= 5)
    def _():
        some_blocks((2, 5))

    relay(1, high=6)
    blocks(6, 7)
    blocks(3, 4)

    for d in (2, 1, 3):
        start(rc(tbl, tblr.at[x], t_s, t_r, dev(xx=xpeer(d))))
    tblr[x] = tbl[...]

    relay(1, low=6)
    srx[y] = stx[...]
    came(*all_st)
    stats = [srx[i] for i in range(NY)]
    means = [t[:, 0:1] for t in stats]
    mean = (means[0] + means[1] + means[2] + means[3]) * 0.25
    m2 = stats[0][:, 64:65] + stats[1][:, 64:65] + stats[2][:, 64:65] + stats[3][:, 64:65]
    for t in means:
        m2 = m2 + 256.0 * (t - mean) * (t - mean)
    cn = (convb[...] - mean) * lax.rsqrt(m2 / CONV_CH + EPS) * ngain[...] + nshift[...]
    cn = (cn * sigmoid(cn)).astype(BF16)
    local[C_CO].wait()
    for i in range(NY):
        cst[i] = dot(cn, wco[:, i * 512 : (i + 1) * 512]).astype(BF16)
    for d in (2, 1, 3):
        yy = ypeer(d)
        start(rc(cst.at[yy], crx.at[y], c_s, c_r, dev(yy=yy)))

    def values(ks):
        for k in ks:
            @pl.when(z >= k)
            def _():
                come(1, k)
                row = zpeer(-k)
                obuf[row] = dot(stk[k], vbuf[row])

    values((0, 1, 2, 7, 6, 5))

    came(*all_t)

    totals = [tblr[i] for i in range(NX)]
    row_sum = totals[0] + totals[1] + totals[2] + totals[3]
    at = lax.broadcasted_iota(jnp.int32, (NZ, NX * HD), 0)
    outside = jnp.zeros((NZ, NX * HD), F32)
    for j in range(1, NZ):
        outside = outside + jnp.where(at < j, row_sum[j : j + 1, :], 0.0)
    for i in range(1, NX):
        outside = outside + jnp.where(x < i, 1.0, 0.0) * totals[i]
    weight = jnp.exp(-outside)
    per_row = weight.T
    for b in range(NX):
        wbuf[b] = per_row[b * HD : (b + 1) * HD, :]
    values((3, 4))
    halves = [slice(i * 64, (i + 1) * 64) for i in (0, 1)]
    for i in (0, 1):
        for d in (2, 1, 3, 0):
            b = xpeer(d)
            per_row = wbuf[b, halves[i], :]
            rows = pl.ds(pl.multiple_of(b * HD + i * 64, 64), 64)
            acc = obuf[0, rows, :] * per_row[:, 0:1]
            for j in range(1, NZ):
                acc = acc + obuf[j, rows, :] * per_row[:, j : j + 1]
            if d > 0:
                ps[d, halves[i], :] = acc.astype(BF16)
            else:
                own[halves[i], :] = acc
        for d in (2, 1, 3):
            start(rc(ps.at[d, halves[i]], pr.at[x, halves[i]], o_s.at[i], o_r.at[i], dev(xx=xpeer(d))))

    came(*all_w)
    for d in (2, 1, 3):
        got = wo.at[whalf(ypeer(d), c), :]
        start(rc(got, got, v_s, v_r, partner))

    local[C_GA].wait()
    local[C_GC].wait()
    gateb[0] = sigmoid(dot(hbuf[...], wga[...]).astype(BF16).astype(F32))
    gateb[1] = sigmoid(dot(hbuf[...], wgc[...]).astype(BF16).astype(F32))

    head = pl.ds(pl.multiple_of((y * 2 + c) * HD, HD), HD)
    for i, rows in enumerate(halves):
        came(*all_o[i])
        acc = own[rows, :]
        for d in (2, 1, 3):
            acc = acc + pr[xpeer(d), rows, :].astype(F32)
        att[rows, :] = acc.astype(BF16)
        for d in (2, 1, 3):
            start(rc(att.at[rows, :], abuf.at[:, head], a_s, a_r, dev(cc=i, yy=ypeer(d))))

        @pl.when(c == i)
        def _():
            abuf[:, head] = att[rows, :]

        @pl.when(c != i)
        def _():
            rc(att.at[rows, :], abuf.at[:, head], a_s, a_r, dev(cc=i)).start()

    local[C_AO].wait()
    came(*all_v)

    csum = cst[y].astype(F32)
    came(*all_c)
    for d in (2, 1, 3):
        yy = ypeer(d)
        csum = csum + crx[yy].astype(F32)
    gateb[1] = gateb[1] * csum.astype(BF16).astype(F32)

    came(*all_a)
    branch = dot(abuf[...], wo[...]).astype(BF16).astype(F32)
    merged = gateb[0] * branch + gateb[1]
    sq = merged * merged
    part = sq[:, 0:128] + sq[:, 128:256] + sq[:, 256:384] + sq[:, 384:512]
    part = jnp.concatenate([part, jnp.zeros((64, HD), F32)], axis=0).T
    ssx[...] = jnp.sum(part.reshape(16, 8, HD), axis=0)
    for d in (2, 1, 3):
        start(rc(ssx, ssr.at[y], ss_s, ss_r, dev(yy=ypeer(d))))
    total = ssx[...]
    came(*all_ss)
    for d in (2, 1, 3):
        total = total + ssr[ypeer(d)]
    total = jnp.broadcast_to(jnp.sum(total, axis=0, keepdims=True), (HD, HD)).T[:64, 0:1]
    out[...] = (merged * lax.rsqrt(total / D + EPS) * post_gain[...]).astype(BF16)

    for group in (all_h, all_p, all_q, all_t, *all_o, all_w, all_v, all_st, all_c, all_a, all_ss):
        gone(*group)
    def z_sent(i, cond):
        @pl.when(cond)
        def _():
            two = kbuf.at[0:2]
            rc(two, two, z_s.at[i], z_r.at[0], partner).wait_send()

    for i, step in enumerate(STEPS):
        z_sent(i, z < NZ - step)
        z_sent(2 + i, (z >= 2) & (z < NZ - step))
    for i, k in enumerate(WRAPS):
        z_sent(4 + i, z + k < NZ)

    @pl.when(sends_halo)
    def _():
        rc(gst, halo, halo_s, halo_r, halo_to).wait_send()


def on_device(
    hidden_in, pre_gain, w_query, w_key, w_value, stick_offset, w_glu_a, w_glu_b, w_gate_attn,
    w_gate_conv, conv_taps, conv_bias, norm_gain, norm_shift, w_attn_out, w_conv_out, post_gain,
):
    args = (
        hidden_in, pre_gain.reshape(1, -1), w_query, w_key, w_value, stick_offset, w_glu_a,
        w_glu_b, w_gate_attn, w_gate_conv, conv_taps, conv_bias.reshape(1, -1),
        norm_gain.reshape(1, -1), norm_shift.reshape(1, -1), w_attn_out, w_conv_out,
        post_gain.reshape(1, -1),
    )
    hb = pl.BlockSpec(memory_space=pl.ANY)
    dma = pltpu.SemaphoreType.DMA
    return pl.pallas_call(
        kernel,
        out_shape=jax.ShapeDtypeStruct((64, 512), BF16),
        in_specs=[hb] * 17,
        out_specs=pl.BlockSpec(memory_space=pltpu.VMEM),
        scratch_shapes=[
            pltpu.SMEM((2,), F32),
            pltpu.VMEM((16, D), BF16),
            pltpu.VMEM((1, D), F32),
            pltpu.VMEM((WIDTH, 256), F32),
            pltpu.VMEM((1, 256), F32),
            pltpu.VMEM((1, 256), F32),
            pltpu.VMEM((1, 256), F32),
            pltpu.VMEM((1, 512), F32),
            pltpu.VMEM((64, D), BF16),
            pltpu.VMEM((D, 256), BF16),
            pltpu.VMEM((D, 256), BF16),
            pltpu.VMEM((D, 256), BF16),
            pltpu.VMEM((D, 256), BF16),
            pltpu.VMEM((D, 256), BF16),
            pltpu.VMEM((D, 512), BF16),
            pltpu.VMEM((D, 512), BF16),
            pltpu.VMEM((256, D), BF16),
            pltpu.VMEM((1024, 512), BF16),
            pltpu.VMEM((NZ, 128, 128), BF16),
            pltpu.VMEM((NZ, 128, 128), BF16),
            pltpu.VMEM((64, 128), BF16),
            pltpu.VMEM((64, 128), BF16),
            pltpu.VMEM((NX * 128, 128), BF16),
            pltpu.VMEM((64, 128), BF16),
            pltpu.VMEM((NZ, NX * 128, 128), F32),
            pltpu.VMEM((NZ, NX * 128, 128), BF16),
            pltpu.VMEM((NZ, NX * 128), F32),
            pltpu.VMEM((NX, NZ, NX * 128), F32),
            pltpu.VMEM((NX, 128, NZ), F32),
            pltpu.VMEM((128, 128), F32),
            pltpu.VMEM((NX, 128, 128), BF16),
            pltpu.VMEM((NX, 128, 128), BF16),
            pltpu.VMEM((256, 128), BF16),
            pltpu.VMEM((32, 256), BF16),
            pltpu.VMEM((32, 256), BF16),
            pltpu.VMEM((96, 256), F32),
            pltpu.VMEM((NY, 64, 512), BF16),
            pltpu.VMEM((NY, 64, 512), BF16),
            pltpu.VMEM((64, 128), F32),
            pltpu.VMEM((NY, 64, 128), F32),
            pltpu.VMEM((64, 256), F32),
            pltpu.VMEM((2, 64, 512), F32),
            pltpu.VMEM((128, 128), BF16),
            pltpu.VMEM((64, 1024), BF16),
            pltpu.VMEM((8, 128), F32),
            pltpu.VMEM((NY, 8, 128), F32),
            dma((9,)), dma((8,)),
            dma, dma,
            dma, dma,
            dma((7,)), dma((16,)),
            dma, dma,
            dma, dma,
            dma((2,)), dma((2,)),
            pltpu.SemaphoreType.REGULAR((8,)),
            dma, dma,
            dma, dma, dma, dma,
            dma, dma,
            dma, dma,
            dma, dma,
            dma, dma,
        ],
        compiler_params=pltpu.CompilerParams(
            collective_id=0, has_side_effects=True, vmem_limit_bytes=40 * 1024 * 1024
        ),
    )(*(pltpu.with_memory_space_constraint(a, pltpu.HBM) for a in args))


def solution(mesh):
    torus = Mesh(mesh.devices.reshape(NZ, NX, 2, NY), ("z", "x", "c", "y"))
    every = ("z", "x", "c", "y")
    cols = P(None, "y")
    return jax.shard_map(
        on_device,
        mesh=torus,
        in_specs=(
            P(every, None), P(), cols, cols, cols, P("y"), cols, cols, cols, cols, cols,
            P("y"), P("y"), P("y"), P("y", None), P("y", None), P("y"),
        ),
        out_specs=P(("z", "x", "c"), "y"),
        check_vma=False,
    )
```

```python
import functools
import math

import jax
import jax.numpy as jnp
from jax import lax
from jax.experimental import pallas as pl
from jax.experimental.pallas import tpu as pltpu
from jax.sharding import Mesh
from jax.sharding import PartitionSpec as P

D = 2048
HD = 128
CONV_CH = 1024
WIDTH = 31
EPS = 1e-06
MESH = pl.DeviceIdType.MESH
F32 = jnp.float32
BF16 = jnp.bfloat16
NX = 4
NZ = 8
NY = 4
NCHIP = NX * NZ


STEPS = (2, 1)
WRAPS = (5, 6, 7)
GREETED = STEPS + WRAPS


def dot(a, b):
    return jnp.dot(a, b, preferred_element_type=F32)


def dot_nt(a, b):
    return lax.dot_general(a, b, (((1,), (1,)), ((), ())), preferred_element_type=F32)


def sigmoid(v):
    return jax.nn.sigmoid(v)


(C_K0, C_V0, C_Q0, C_A, C_B, C_GA, C_GC, C_CO, C_AO, C_K1, C_V1, C_Q1) = range(12)
SHARED = {C_K1: C_K0, C_V1: C_V0, C_Q1: C_Q0}


def kernel(
    hidden_hbm, pre_gain_hbm, w_query, w_key, w_value, offset_hbm, w_a, w_b, w_ga, w_gc,
    taps_hbm, bias_hbm, ngain_hbm, nshift_hbm, w_ao, w_co, post_gain_hbm,
    out,
    offset, hidden, pre_gain, taps, bias, ngain, nshift, post_gain, hbuf, wk, wv, wq, wa, wb, wga, wgc, wco, wo,
    kbuf, vbuf, kst, vst, qbuf, qst, obuf, stk, tbl, tblr, wbuf, own, ps, pr, tri,
    gst, halo, gbuf, cst, crx, stx, srx, convb, gateb, att, abuf, ssx, ssr,
    lsem, ssem, h_s, h_r, p_s, p_r, z_s, z_r, q_s, q_r, t_s, t_r, o_s, o_r, ready, halo_s, halo_r,
    w_s, w_r, v_s, v_r, st_s, st_r, c_s, c_r, a_s, a_r, ss_s, ss_r,
):
    z = lax.axis_index("z")
    x = lax.axis_index("x")
    c = lax.axis_index("c")
    y = lax.axis_index("y")
    chip = z * NX + x
    oc = 1 - c

    def dev(zz=z, xx=x, cc=c, yy=y):
        return (zz, xx, cc, yy)

    def ypeer(d):
        return lax.rem(y + d, NY)

    def xpeer(d):
        return lax.rem(x + d, NX)

    def zpeer(d):
        return lax.rem(z + d + NZ, NZ)

    def rc(src, dst, ss, rs, to):
        return pltpu.make_async_remote_copy(
            src_ref=src, dst_ref=dst, send_sem=ss, recv_sem=rs, device_id=to, device_id_type=MESH
        )

    half = pl.ds(pl.multiple_of(c * HD, HD), HD)

    def whalf(yy, cc):
        return pl.ds(pl.multiple_of(yy * 256 + cc * HD, HD), HD)

    def start(copy):
        copy.start()

    def came(whole, group):
        rc(whole, whole, group[0], group[1], dev(cc=oc)).wait_recv()

    def gone(whole, group):
        rc(whole, whole, group[0], group[1], dev(cc=oc)).wait_send()

    all_h = hbuf.at[0:48, :], (h_s, h_r)
    all_p = qbuf.at[0:128, :], (p_s, p_r)
    all_q = qbuf.at[0:448, :], (q_s, q_r)
    all_t = tblr.at[0:3], (t_s, t_r)
    all_o = [(pr.at[0:3, i * 64 : (i + 1) * 64], (o_s.at[i], o_r.at[i])) for i in (0, 1)]
    all_w = wo.at[0:384, :], (w_s, w_r)
    all_v = wo.at[0:384, :], (v_s, v_r)
    all_st = srx.at[0:3], (st_s, st_r)
    all_c = crx.at[0:3], (c_s, c_r)
    all_a = abuf.at[:, 0:896], (a_s, a_r)
    all_ss = ssr.at[0:3], (ss_s, ss_r)

    own_cols = pl.ds(pl.multiple_of(c * HD, HD), HD)
    oth_cols = pl.ds(pl.multiple_of(oc * HD, HD), HD)
    lo, hi = pl.ds(0, HD), pl.ds(HD, HD)
    ycols = pl.ds(pl.multiple_of(y * 512, 512), 512)
    yrows = pl.ds(pl.multiple_of(y * 256, 256), 256)
    local = {
        C_K1: (w_key.at[:, oth_cols], wk.at[:, lo]),
        C_K0: (w_key.at[:, own_cols], wk.at[:, hi]),
        C_V1: (w_value.at[:, oth_cols], wv.at[:, lo]),
        C_V0: (w_value.at[:, own_cols], wv.at[:, hi]),
        C_Q1: (w_query.at[:, oth_cols], wq.at[:, hi]),
        C_Q0: (w_query.at[:, own_cols], wq.at[:, lo]),
        C_A: (w_a, wa),
        C_B: (w_b, wb),
        C_GA: (w_ga, wga),
        C_GC: (w_gc, wgc),
        C_CO: (w_co, wco),
        C_AO: (w_ao.at[:, ycols], wo.at[yrows, :]),
    }
    local = {k: pltpu.make_async_copy(s, d, lsem.at[SHARED.get(k, k)]) for k, (s, d) in local.items()}
    first_in = [(hidden_hbm, hidden), (pre_gain_hbm, pre_gain)]
    later_in = [
        (taps_hbm, taps), (bias_hbm, bias), (ngain_hbm, ngain), (nshift_hbm, nshift), (post_gain_hbm, post_gain),
        (offset_hbm, offset),
    ]
    small = [
        pltpu.make_async_copy(a, b, ssem.at[i]) for i, (a, b) in enumerate(first_in + later_in)
    ]
    for copy in small[:2]:
        copy.start()

    barrier = pltpu.get_barrier_semaphore()
    next_chip = lax.rem(chip + 1, NCHIP)
    prev_chip = lax.rem(chip + NCHIP - 1, NCHIP)
    pair_chip = c * next_chip + oc * prev_chip
    pz, px = pair_chip // NX, lax.rem(pair_chip, NX)
    greet = [dev(yy=ypeer(d)) for d in (1, 2, 3)]
    greet += [dev(cc=oc, yy=ypeer(d)) for d in (0, 1, 2, 3)]
    greet += [dev(xx=xpeer(d), cc=cc) for d in (1, 2, 3) for cc in (c, oc)]
    for peer in greet:
        pl.semaphore_signal(barrier, inc=1, device_id=peer, device_id_type=MESH)
    greeted = len(greet)
    for k in GREETED:
        @pl.when(z + k < NZ)
        def _():
            for cc in (c, oc) if k in STEPS else (c,):
                pl.semaphore_signal(barrier, inc=1, device_id=dev(zz=zpeer(k), cc=cc), device_id_type=MESH)

        greeted = greeted + jnp.where(z >= k, 2 if k in STEPS else 1, 0)
    next_core = (pz, px, oc, y)
    has_next = (c == 1) & (chip < NCHIP - 1)
    has_prev = (c == 0) & (chip > 0)

    @pl.when(has_next)
    def _():
        pl.semaphore_signal(barrier, inc=1, device_id=next_core, device_id_type=MESH)

    greeted = greeted + jnp.where(has_prev, 1, 0)

    for copy in small[:2]:
        copy.wait()

    hv = hidden[...].astype(F32)
    inv = lax.rsqrt(jnp.mean(hv * hv, axis=1, keepdims=True) + EPS)
    my16 = pl.ds(pl.multiple_of(y * 16, 16), 16)
    hbuf[my16, :] = (hv * inv * pre_gain[...]).astype(BF16)

    pl.semaphore_wait(barrier, greeted)
    for k in GREETED:
        @pl.when(z >= k)
        def _():
            for cc in (c, oc) if k in STEPS else (c,):
                pl.semaphore_signal(ready.at[k], inc=1, device_id=dev(zz=zpeer(-k), cc=cc), device_id_type=MESH)

    @pl.when(has_prev)
    def _():
        pl.semaphore_signal(ready.at[0], inc=1, device_id=next_core, device_id_type=MESH)


    for d in (2, 1, 3):
        start(rc(hbuf.at[my16, :], hbuf.at[my16, :], h_s, h_r, dev(yy=ypeer(d))))
    for copy in local.values():
        copy.start()
    for copy in small[2:]:
        copy.start()

    r2 = lax.broadcasted_iota(jnp.int32, (2 * HD, HD), 0) % HD
    c2 = lax.broadcasted_iota(jnp.int32, (2 * HD, HD), 1)
    tri[...] = jnp.where(r2 > c2, 1.0, 0.0).astype(BF16)
    obuf[...] = jnp.zeros(obuf.shape, F32)
    tbl[...] = jnp.zeros(tbl.shape, F32)
    came(*all_h)

    def send_shard(d):
        yy = ypeer(d)
        cols = pl.ds(pl.multiple_of(yy * 512, 512), 512)
        start(rc(w_ao.at[half, cols], wo.at[whalf(y, c), :], w_s, w_r, dev(yy=yy)))

    send_shard(1)
    send_shard(3)

    my64 = pl.ds(pl.multiple_of(c * 64, 64), 64)
    oth64 = pl.ds(pl.multiple_of(oc * 64, 64), 64)
    partner = dev(cc=oc)
    tables = (kbuf, vbuf)

    def z_own(h, i, cond=True):
        step = STEPS[i]

        @pl.when((z < NZ - step) & cond)
        def _():
            if h == 0:
                pl.semaphore_wait(ready.at[step], 2)
            mine, there = tables[h].at[z, my64, :], z_r.at[h * NZ + z]
            rc(mine, mine, z_s.at[i], there, dev(zz=zpeer(step))).start()
            rc((kst, vst)[h], mine, z_s.at[i], there, dev(zz=zpeer(step), cc=oc)).start()

    def z_copy(h, row, i, step):
        t = tables[h].at[row]
        return rc(t, t, z_s.at[i], z_r.at[h * NZ + row], dev(zz=zpeer(step)))

    def project(h):
        w, st, name = ((wk, kst, C_K0), (wv, vst, C_V0))[h]
        pltpu.make_async_copy(w, w, lsem.at[name]).wait()
        both = dot(hbuf[...], w[...]).astype(BF16)
        st[...] = both[:, :HD]
        start(rc(st, tables[h].at[z, my64, :], p_s, p_r, partner))
        tables[h][z, my64, :] = both[:, HD:]
        if h == 0:
            z_own(h, 0)
            z_own(h, 1, c == 0)
        else:
            z_own(h, 0, c == 0)

    project(0)
    pltpu.make_async_copy(wq, wq, lsem.at[C_Q0]).wait()
    qv = dot(hbuf[...], wq[...]).astype(BF16)
    qst[...] = qv[:, HD:]

    def qrows(xx, cc):
        return pl.ds(pl.multiple_of(xx * HD + cc * 64, 64), 64)

    mine = qbuf.at[qrows(x, c), :]
    qbuf[qrows(x, c), :] = qv[:, :HD]
    for d in range(NX):
        start(rc(qst, mine, q_s, q_r, dev(xx=xpeer(d), cc=oc)))
        if d > 0:
            start(rc(mine, mine, q_s, q_r, dev(xx=xpeer(d))))

    z_own(0, 1, c == 1)
    project(1)
    local[C_A].wait()
    local[C_B].wait()
    left = dot(hbuf[...], wa[...]).astype(BF16).astype(F32)
    right = dot(hbuf[...], wb[...]).astype(BF16).astype(F32)
    gated = (left * sigmoid(right)).astype(BF16)
    gst[...] = gated[32:, :]
    gbuf[32:, :] = gated.astype(F32)
    halo_to = ((next_chip // NX) * c + z * oc, lax.rem(next_chip, NX) * c + x * oc, oc, y)

    @pl.when(has_next)
    def _():
        pl.semaphore_wait(ready.at[0], 1)

    has_halo = (c == 1) | (chip > 0)
    sends_halo = (c == 0) | (chip < NCHIP - 1)

    @pl.when(sends_halo)
    def _():
        rc(gst, halo, halo_s, halo_r, halo_to).start()

    came(*all_p)

    def wrap(h):
        for i, k in enumerate(WRAPS):
            @pl.when(z + k < NZ)
            def _():
                if h == 0:
                    pl.semaphore_wait(ready.at[k], 1)
                z_copy(h, z, 4 + i, k).start()

    wrap(0)

    def arrived(h, k):
        row = zpeer(-k)
        z_copy(h, row, 0, 1).wait_recv()

    def relay(h, low=2, high=NZ - 1):
        @pl.when((z >= low) & (z < high))
        def _():
            arrived(h, 2)
            for i, step in enumerate(STEPS):
                @pl.when(z < NZ - step)
                def _():
                    z_copy(h, zpeer(-2), 2 + i, step).start()

    relay(0)
    z_own(1, 0, c == 1)
    z_own(1, 1)
    small[7].wait()
    off = offset[c]
    scale = 1.0 / math.sqrt(HD)

    def come(h, k):
        if k == 2:
            pl.when(z == NZ - 1)(functools.partial(arrived, h, k))
        elif k > 0:
            arrived(h, k)

    def some_blocks(ks):
        for k in ks:
            come(0, k)
        fronts = []
        for k in ks:
            row = zpeer(-k)
            for b in range(NX):
                s = dot_nt(qbuf[b * HD : (b + 1) * HD, :], kbuf[row]) * scale + off
                u = jnp.exp(-jnp.abs(s))
                one = 1.0 + u
                tail = jnp.log(one) + (u - (one - 1.0))
                soft = jnp.maximum(s, 0.0) + tail
                logit = s - soft
                if k == 0:
                    rows = lax.broadcasted_iota(jnp.int32, (HD, HD), 0) + b * HD
                    cols = lax.broadcasted_iota(jnp.int32, (HD, HD), 1) + x * HD
                    soft = jnp.where(cols < rows, soft, 0.0)
                    logit = jnp.where(cols < rows, logit, -jnp.inf)
                top = soft.astype(BF16)
                rest = (soft - top.astype(F32)).astype(BF16)
                fronts.append((k, row, b, logit, jnp.concatenate([top, rest], axis=1)))
        sums = [dot(f[4], tri[...]) for f in fronts]
        ones = jnp.ones((NZ, 2 * HD), BF16)
        for k, row, b, _, pair in fronts:
            here = lax.broadcasted_iota(jnp.int32, (NZ, HD), 0) == row
            cols = slice(b * HD, (b + 1) * HD)
            tbl[:, cols] = jnp.where(here, dot_nt(ones, pair), tbl[:, cols])
        for (k, row, b, logit, _), t in zip(fronts, sums):
            stk[k, b * HD : (b + 1) * HD, :] = jnp.exp(logit - t).astype(BF16)

    def blocks(low, high):
        pl.when(z >= high)(functools.partial(some_blocks, (low, high)))
        pl.when((z >= low) & (z < high))(functools.partial(some_blocks, (low,)))

    @pl.when(has_halo)
    def _():
        rc(gst, halo, halo_s, halo_r, halo_to).wait_recv()
        gbuf[0:32, :] = halo[...].astype(F32)

    @pl.when(jnp.logical_not(has_halo))
    def _():
        gbuf[0:32, :] = jnp.zeros((32, 256), F32)

    for copy in small[2:7]:
        copy.wait()
    conv = jnp.broadcast_to(bias[...], (64, 256))
    for i in range(WIDTH):
        conv = conv + taps[i : i + 1, :] * gbuf[2 + i : 66 + i, :]
    local_mean = jnp.mean(conv, axis=1, keepdims=True)
    dev_local = conv - local_mean
    local_m2 = jnp.sum(dev_local * dev_local, axis=1, keepdims=True)
    lane = lax.broadcasted_iota(jnp.int32, (64, HD), 1)
    stx[...] = jnp.where(lane < 64, local_mean, local_m2)
    for d in (2, 1, 3):
        start(rc(stx, srx.at[y], st_s, st_r, dev(yy=ypeer(d))))
    convb[...] = conv

    send_shard(2)
    wrap(1)
    came(*all_q)

    blocks(0, 1)
    @pl.when((z >= 2) & (z < 5))
    def _():
        some_blocks((2,))

    @pl.when(z >= 5)
    def _():
        some_blocks((2, 5))

    relay(1, high=6)
    blocks(6, 7)
    blocks(3, 4)

    for d in (2, 1, 3):
        start(rc(tbl, tblr.at[x], t_s, t_r, dev(xx=xpeer(d))))
    tblr[x] = tbl[...]

    relay(1, low=6)
    srx[y] = stx[...]
    came(*all_st)
    stats = [srx[i] for i in range(NY)]
    means = [t[:, 0:1] for t in stats]
    mean = (means[0] + means[1] + means[2] + means[3]) * 0.25
    m2 = stats[0][:, 64:65] + stats[1][:, 64:65] + stats[2][:, 64:65] + stats[3][:, 64:65]
    for t in means:
        m2 = m2 + 256.0 * (t - mean) * (t - mean)
    cn = (convb[...] - mean) * lax.rsqrt(m2 / CONV_CH + EPS) * ngain[...] + nshift[...]
    cn = (cn * sigmoid(cn)).astype(BF16)
    local[C_CO].wait()
    for i in range(NY):
        cst[i] = dot(cn, wco[:, i * 512 : (i + 1) * 512]).astype(BF16)
    for d in (2, 1, 3):
        yy = ypeer(d)
        start(rc(cst.at[yy], crx.at[y], c_s, c_r, dev(yy=yy)))

    def values(ks):
        for k in ks:
            @pl.when(z >= k)
            def _():
                come(1, k)
                row = zpeer(-k)
                obuf[row] = dot(stk[k], vbuf[row])

    values((0, 1, 2, 7, 6, 5))

    came(*all_t)

    totals = [tblr[i] for i in range(NX)]
    row_sum = totals[0] + totals[1] + totals[2] + totals[3]
    at = lax.broadcasted_iota(jnp.int32, (NZ, NX * HD), 0)
    outside = jnp.zeros((NZ, NX * HD), F32)
    for j in range(1, NZ):
        outside = outside + jnp.where(at < j, row_sum[j : j + 1, :], 0.0)
    for i in range(1, NX):
        outside = outside + jnp.where(x < i, 1.0, 0.0) * totals[i]
    weight = jnp.exp(-outside)
    per_row = weight.T
    for b in range(NX):
        wbuf[b] = per_row[b * HD : (b + 1) * HD, :]
    values((3, 4))
    halves = [slice(i * 64, (i + 1) * 64) for i in (0, 1)]
    for i in (0, 1):
        for d in (2, 1, 3, 0):
            b = xpeer(d)
            per_row = wbuf[b, halves[i], :]
            rows = pl.ds(pl.multiple_of(b * HD + i * 64, 64), 64)
            acc = obuf[0, rows, :] * per_row[:, 0:1]
            for j in range(1, NZ):
                acc = acc + obuf[j, rows, :] * per_row[:, j : j + 1]
            if d > 0:
                ps[d, halves[i], :] = acc.astype(BF16)
            else:
                own[halves[i], :] = acc
        for d in (2, 1, 3):
            start(rc(ps.at[d, halves[i]], pr.at[x, halves[i]], o_s.at[i], o_r.at[i], dev(xx=xpeer(d))))

    came(*all_w)
    for d in (2, 1, 3):
        got = wo.at[whalf(ypeer(d), c), :]
        start(rc(got, got, v_s, v_r, partner))

    local[C_GA].wait()
    local[C_GC].wait()
    gateb[0] = sigmoid(dot(hbuf[...], wga[...]).astype(BF16).astype(F32))
    gateb[1] = sigmoid(dot(hbuf[...], wgc[...]).astype(BF16).astype(F32))

    head = pl.ds(pl.multiple_of((y * 2 + c) * HD, HD), HD)
    for i, rows in enumerate(halves):
        came(*all_o[i])
        acc = own[rows, :]
        for d in (2, 1, 3):
            acc = acc + pr[xpeer(d), rows, :].astype(F32)
        att[rows, :] = acc.astype(BF16)
        for d in (2, 1, 3):
            start(rc(att.at[rows, :], abuf.at[:, head], a_s, a_r, dev(cc=i, yy=ypeer(d))))

        @pl.when(c == i)
        def _():
            abuf[:, head] = att[rows, :]

        @pl.when(c != i)
        def _():
            rc(att.at[rows, :], abuf.at[:, head], a_s, a_r, dev(cc=i)).start()

    local[C_AO].wait()
    came(*all_v)

    csum = cst[y].astype(F32)
    came(*all_c)
    for d in (2, 1, 3):
        yy = ypeer(d)
        csum = csum + crx[yy].astype(F32)
    gateb[1] = gateb[1] * csum.astype(BF16).astype(F32)

    came(*all_a)
    branch = dot(abuf[...], wo[...]).astype(BF16).astype(F32)
    merged = gateb[0] * branch + gateb[1]
    sq = merged * merged
    part = sq[:, 0:128] + sq[:, 128:256] + sq[:, 256:384] + sq[:, 384:512]
    part = jnp.concatenate([part, jnp.zeros((64, HD), F32)], axis=0).T
    ssx[...] = jnp.sum(part.reshape(16, 8, HD), axis=0)
    for d in (2, 1, 3):
        start(rc(ssx, ssr.at[y], ss_s, ss_r, dev(yy=ypeer(d))))
    total = ssx[...]
    came(*all_ss)
    for d in (2, 1, 3):
        total = total + ssr[ypeer(d)]
    total = jnp.broadcast_to(jnp.sum(total, axis=0, keepdims=True), (HD, HD)).T[:64, 0:1]
    out[...] = (merged * lax.rsqrt(total / D + EPS) * post_gain[...]).astype(BF16)

    for group in (all_h, all_p, all_q, all_t, *all_o, all_w, all_v, all_st, all_c, all_a, all_ss):
        gone(*group)
    def z_sent(i, cond):
        @pl.when(cond)
        def _():
            two = kbuf.at[0:2]
            rc(two, two, z_s.at[i], z_r.at[0], partner).wait_send()

    for i, step in enumerate(STEPS):
        z_sent(i, z < NZ - step)
        z_sent(2 + i, (z >= 2) & (z < NZ - step))
    for i, k in enumerate(WRAPS):
        z_sent(4 + i, z + k < NZ)

    @pl.when(sends_halo)
    def _():
        rc(gst, halo, halo_s, halo_r, halo_to).wait_send()


def on_device(
    hidden_in, pre_gain, w_query, w_key, w_value, stick_offset, w_glu_a, w_glu_b, w_gate_attn,
    w_gate_conv, conv_taps, conv_bias, norm_gain, norm_shift, w_attn_out, w_conv_out, post_gain,
):
    args = (
        hidden_in, pre_gain.reshape(1, -1), w_query, w_key, w_value, stick_offset, w_glu_a,
        w_glu_b, w_gate_attn, w_gate_conv, conv_taps, conv_bias.reshape(1, -1),
        norm_gain.reshape(1, -1), norm_shift.reshape(1, -1), w_attn_out, w_conv_out,
        post_gain.reshape(1, -1),
    )
    hb = pl.BlockSpec(memory_space=pl.ANY)
    dma = pltpu.SemaphoreType.DMA
    return pl.pallas_call(
        kernel,
        out_shape=jax.ShapeDtypeStruct((64, 512), BF16),
        in_specs=[hb] * 17,
        out_specs=pl.BlockSpec(memory_space=pltpu.VMEM),
        scratch_shapes=[
            pltpu.SMEM((2,), F32),
            pltpu.VMEM((16, D), BF16),
            pltpu.VMEM((1, D), F32),
            pltpu.VMEM((WIDTH, 256), F32),
            pltpu.VMEM((1, 256), F32),
            pltpu.VMEM((1, 256), F32),
            pltpu.VMEM((1, 256), F32),
            pltpu.VMEM((1, 512), F32),
            pltpu.VMEM((64, D), BF16),
            pltpu.VMEM((D, 256), BF16),
            pltpu.VMEM((D, 256), BF16),
            pltpu.VMEM((D, 256), BF16),
            pltpu.VMEM((D, 256), BF16),
            pltpu.VMEM((D, 256), BF16),
            pltpu.VMEM((D, 512), BF16),
            pltpu.VMEM((D, 512), BF16),
            pltpu.VMEM((256, D), BF16),
            pltpu.VMEM((1024, 512), BF16),
            pltpu.VMEM((NZ, 128, 128), BF16),
            pltpu.VMEM((NZ, 128, 128), BF16),
            pltpu.VMEM((64, 128), BF16),
            pltpu.VMEM((64, 128), BF16),
            pltpu.VMEM((NX * 128, 128), BF16),
            pltpu.VMEM((64, 128), BF16),
            pltpu.VMEM((NZ, NX * 128, 128), F32),
            pltpu.VMEM((NZ, NX * 128, 128), BF16),
            pltpu.VMEM((NZ, NX * 128), F32),
            pltpu.VMEM((NX, NZ, NX * 128), F32),
            pltpu.VMEM((NX, 128, NZ), F32),
            pltpu.VMEM((128, 128), F32),
            pltpu.VMEM((NX, 128, 128), BF16),
            pltpu.VMEM((NX, 128, 128), BF16),
            pltpu.VMEM((256, 128), BF16),
            pltpu.VMEM((32, 256), BF16),
            pltpu.VMEM((32, 256), BF16),
            pltpu.VMEM((96, 256), F32),
            pltpu.VMEM((NY, 64, 512), BF16),
            pltpu.VMEM((NY, 64, 512), BF16),
            pltpu.VMEM((64, 128), F32),
            pltpu.VMEM((NY, 64, 128), F32),
            pltpu.VMEM((64, 256), F32),
            pltpu.VMEM((2, 64, 512), F32),
            pltpu.VMEM((128, 128), BF16),
            pltpu.VMEM((64, 1024), BF16),
            pltpu.VMEM((8, 128), F32),
            pltpu.VMEM((NY, 8, 128), F32),
            dma((9,)), dma((8,)),
            dma, dma,
            dma, dma,
            dma((7,)), dma((16,)),
            dma, dma,
            dma, dma,
            dma((2,)), dma((2,)),
            pltpu.SemaphoreType.REGULAR((8,)),
            dma, dma,
            dma, dma, dma, dma,
            dma, dma,
            dma, dma,
            dma, dma,
            dma, dma,
        ],
        compiler_params=pltpu.CompilerParams(
            collective_id=0, has_side_effects=True, vmem_limit_bytes=40 * 1024 * 1024
        ),
    )(*(pltpu.with_memory_space_constraint(a, pltpu.HBM) for a in args))


def solution(mesh):
    torus = Mesh(mesh.devices.reshape(NZ, NX, 2, NY), ("z", "x", "c", "y"))
    every = ("z", "x", "c", "y")
    cols = P(None, "y")
    return jax.shard_map(
        on_device,
        mesh=torus,
        in_specs=(
            P(every, None), P(), cols, cols, cols, P("y"), cols, cols, cols, cols, cols,
            P("y"), P("y"), P("y"), P("y", None), P("y", None), P("y"),
        ),
        out_specs=P(("z", "x", "c"), "y"),
        check_vma=False,
    )
```
